128 devices in a mesh: ep: 128 (over z, y, x, core).
Axes of the slice: x: 4, y: 4, z: 4, core: 2. Of those that a mesh axis runs over, the one named last changes fastest.
Arguments:
- tokens: bfloat16 [2048, 2048], P('ep'), may hold values from -6 to 6
- cache_keys: bfloat16 [2048, 1024, 128], P('ep'), may hold values from -6 to 6
- cache_values: bfloat16 [2048, 1024, 128], P('ep'), may hold values from -6 to 6
- cache_len: int32 [2048], P('ep'), may hold values from 1 to 1024
- norm_gain_first: float32 [2048], replicated, may hold values from 0.1 to 1.9
- w_query: bfloat16 [2048, 2048], P(None, 'ep'), may hold values from -0.125 to 0.125
- w_key: bfloat16 [2048, 128], replicated, may hold values from -0.125 to 0.125
- w_value: bfloat16 [2048, 128], replicated, may hold values from -0.125 to 0.125
- head_bias: float32 [32], replicated, may hold values from -8.5 to -3
- w_output: bfloat16 [2048, 2048], P(None, 'ep'), may hold values from -0.125 to 0.125
- norm_gain_second: float32 [2048], replicated, may hold values from 0.1 to 1.9
- group_id: int32 [2048], P('ep'), may hold values from 0 to 7, as said below
- member: int32 [2048, 6], P('ep'), may hold values from 0 to 15, as said below
- group_gate: float32 [2048], P('ep'), may hold values from 0.3 to 1
- member_weight: float32 [2048, 6], P('ep'), may hold values from 0.05 to 0.5
- expert_gate_w: bfloat16 [128, 2048, 512], P('ep'), may hold values from -0.125 to 0.125
- expert_up_w: bfloat16 [128, 2048, 512], P('ep'), may hold values from -0.125 to 0.125
- expert_down_w: bfloat16 [128, 512, 2048], P('ep'), may hold values from -0.25 to 0.25
- dense_gate_w: bfloat16 [2048, 2048], P(None, 'ep'), may hold values from -0.125 to 0.125
- dense_up_w: bfloat16 [2048, 2048], P(None, 'ep'), may hold values from -1 to 1
- hidden_gain: float32 [2048], replicated, may hold values from 0.1 to 1.9
- dense_down_w: bfloat16 [2048, 2048], P(None, 'ep'), may hold values from -0.125 to 0.125
- branch_logit: float32 [2048], replicated, may hold values from -8 to 8
Outputs:
- mixed_out: bfloat16 [2048, 2048], P('ep')
- new_keys: bfloat16 [2048, 128], P('ep')
- new_values: bfloat16 [2048, 128], P('ep')
The draws below stay inside these ranges and needn't reach their ends.
Inputs may be any that keep to these rules, and one draw needn't show every extreme that they name: `group_id`: each group number is named by exactly 2 of the tokens of one device. `member`: each row names 6 different members; with group_id, no expert is named by more than 2 tokens of one device, and some expert is named by 2 tokens of every device.
All inputs are finite; a program needn't handle non-finite values.
Results may differ from the reference program's by a relative error of at most 0.0085.
Values may be sent and summed in bfloat16 or wider, within the bound.
A program may use at most 128 MiB of HBM per device.

```python
import math
import jax
import jax.numpy as jnp
from jax import lax

D = 2048
HEADS = 32
HEAD_DIM = 64
KV_HEADS = 2
FD = 2048
FE = 512
PER_GROUP = 16
TOP_K = 6
SEQ_DEV = 16
CACHE = 1024
TOKENS = 2048
EXPERTS = 128
GROUPS = 8
N_EP = 128


def group_table(key):
    block_count = TOKENS // SEQ_DEV
    block_keys = jax.random.split(jax.random.fold_in(key, 11), block_count)

    def shuffle_block(block_key):
        return jax.random.permutation(block_key, SEQ_DEV)
    shuffled = jax.vmap(shuffle_block)(block_keys)
    return (shuffled % GROUPS).reshape(TOKENS).astype(jnp.int32)


def draw_group_id(key, part):
    return group_table(key)


def draw_member(key, part):
    groups_of = group_table(key)
    common = jax.random.randint(jax.random.fold_in(key, 12), (GROUPS,), 0, PER_GROUP)
    common_token = jnp.take(common, groups_of)
    columns = jnp.arange(PER_GROUP, dtype=jnp.int32)[None, :]
    scores = jax.random.randint(jax.random.fold_in(key, 13), (TOKENS, PER_GROUP), 0, 1 << 20) * PER_GROUP + columns
    scores = jnp.where(columns == common_token[:, None], 1 << 26, scores)
    unused, chosen = lax.top_k(scores, TOP_K)
    order_scores = jax.random.randint(jax.random.fold_in(key, 14), (TOKENS, TOP_K), 0, 1 << 20) * TOP_K
    order_scores = order_scores + jnp.arange(TOP_K, dtype=jnp.int32)[None, :]
    reorder = jnp.argsort(order_scores, axis=1)
    return jnp.take_along_axis(chosen, reorder, axis=1).astype(jnp.int32)


def draw_head_bias(key, part):
    return jax.random.uniform(key, (HEADS,), jnp.float32, -7.5, -3.0)


def draw_dense_up_w(key, part):
    base = jax.random.normal(jax.random.fold_in(key, 21), (D, FD), jnp.float32) * D ** (-0.5)
    ramp = jnp.arange(FD, dtype=jnp.float32) / FD
    rising = jnp.exp(ramp * math.log(4.0))
    rough = jnp.exp(jax.random.uniform(jax.random.fold_in(key, 22), (FD,), jnp.float32, -0.7, 0.7))
    scaled = jnp.clip(base * (rising * rough)[None, :], -1.0, 1.0)
    return scaled.astype(jnp.bfloat16)


def place_ends(array, rng, low, top_value):
    place = [jax.random.randint(jax.random.fold_in(rng, axis), (), 0, length) for axis, length in enumerate(array.shape)]
    main_axis = array.shape.index(max(array.shape))
    neighbour = place[:main_axis] + [(place[main_axis] + 1) % array.shape[main_axis]] + place[main_axis + 1:]
    return array.at[tuple(place)].set(low).at[tuple(neighbour)].set(top_value)


def block_levels(own_key, extent, shards, least, high):
    gain = 1.0
    for axis_at, parts in shards:
        steps = jax.random.uniform(jax.random.fold_in(jax.random.fold_in(own_key, 6), axis_at), (parts,), jnp.float32, least / len(shards), high / len(shards))
        gain = gain * jnp.repeat(jnp.exp(steps), extent[axis_at] // parts).reshape((-1,) + (1,) * (len(extent) - 1 - axis_at))
    return gain


def bell_draw(key, dims, scale, most, pieces=(), kind=jnp.bfloat16):
    loudness = block_levels(key, dims, pieces, -0.22, 0.18) if pieces else 1.0
    values = jax.random.normal(key, dims, jnp.float32) * scale * loudness
    return jnp.minimum(jnp.maximum(values, -most), most).astype(kind)


def setup_inputs(seed: int = 0) -> dict:
    seeds = jax.random.split(jax.random.key(seed), 24)
    tokens = bell_draw(seeds[0], (TOKENS, D), 1.0, 6.0, ((0, 128),))
    cache_keys = bell_draw(seeds[1], (TOKENS, CACHE, KV_HEADS * HEAD_DIM), 1.0, 6.0, ((0, 128),))
    cache_values = bell_draw(seeds[2], (TOKENS, CACHE, KV_HEADS * HEAD_DIM), 1.0, 6.0, ((0, 128),))
    cache_len = place_ends(jax.random.randint(seeds[3], (TOKENS,), 1, CACHE + 1), jax.random.fold_in(seeds[3], 1), 1, CACHE).astype(jnp.int32)
    norm_gain_first = jnp.clip(1.0 + 0.18 * jax.random.normal(seeds[4], (D,), jnp.float32), 0.1, 1.9)
    w_query = bell_draw(seeds[5], (D, HEADS * HEAD_DIM), D ** -0.5, 0.125, ((1, 128),))
    w_key = bell_draw(seeds[6], (D, KV_HEADS * HEAD_DIM), D ** -0.5, 0.125)
    w_value = bell_draw(seeds[7], (D, KV_HEADS * HEAD_DIM), D ** -0.5, 0.125)
    head_bias = draw_head_bias(jax.random.fold_in(seeds[23], 71), 0)
    w_output = bell_draw(seeds[9], (HEADS * HEAD_DIM, D), (HEADS * HEAD_DIM) ** -0.5, 0.125, ((1, 128),))
    norm_gain_second = jnp.clip(1.0 + 0.18 * jax.random.normal(seeds[10], (D,), jnp.float32), 0.1, 1.9)
    group_id = draw_group_id(jax.random.fold_in(seeds[23], 71), 0)
    member = draw_member(jax.random.fold_in(seeds[23], 71), 0)
    group_gate = jnp.clip(jnp.exp(math.log(1.0) - 1.2039728 * jax.random.uniform(seeds[13], (TOKENS,), jnp.float32) ** block_levels(seeds[13], (TOKENS,), ((0, 128),), -0.2, 0.2)), 0.3, 1.0)
    member_weight = jnp.clip(jnp.exp(math.log(0.5) - 2.3025851 * jax.random.uniform(seeds[14], (TOKENS, TOP_K), jnp.float32) ** block_levels(seeds[14], (TOKENS, TOP_K), ((0, 128),), -0.2, 0.2)), 0.05, 0.5)
    expert_gate_w = bell_draw(seeds[15], (EXPERTS, D, FE), D ** -0.5, 0.125, ((0, 128),))
    expert_up_w = bell_draw(seeds[16], (EXPERTS, D, FE), D ** -0.5, 0.125, ((0, 128),))
    expert_down_w = bell_draw(seeds[17], (EXPERTS, FE, D), FE ** -0.5, 0.25, ((0, 128),))
    dense_gate_w = bell_draw(seeds[18], (D, FD), D ** -0.5, 0.125, ((1, 128),))
    dense_up_w = draw_dense_up_w(jax.random.fold_in(seeds[23], 71), 0)
    hidden_gain = jnp.clip(1.0 + 0.18 * jax.random.normal(seeds[20], (FD,), jnp.float32), 0.1, 1.9)
    dense_down_w = bell_draw(seeds[21], (FD, D), FD ** -0.5, 0.125, ((1, 128),))
    branch_logit = bell_draw(seeds[22], (D,), 1.5, 8.0, (), jnp.float32)
    return {"tokens": tokens, "cache_keys": cache_keys, "cache_values": cache_values, "cache_len": cache_len, "norm_gain_first": norm_gain_first, "w_query": w_query, "w_key": w_key, "w_value": w_value, "head_bias": head_bias, "w_output": w_output, "norm_gain_second": norm_gain_second, "group_id": group_id, "member": member, "group_gate": group_gate, "member_weight": member_weight, "expert_gate_w": expert_gate_w, "expert_up_w": expert_up_w, "expert_down_w": expert_down_w, "dense_gate_w": dense_gate_w, "dense_up_w": dense_up_w, "hidden_gain": hidden_gain, "dense_down_w": dense_down_w, "branch_logit": branch_logit}


epsilon = 1e-06
pair_block = 32

def rms_scale(values):
    return lax.rsqrt(lax.optimization_barrier(jnp.mean(values * values, axis=-1, keepdims=True)) + epsilon)

def stick_read(queries, key_cache, value_cache, lengths, head_bias):
    batch_size = queries.shape[0]
    span_len = key_cache.shape[1]
    group_size = HEADS // KV_HEADS
    query_heads = queries.reshape(batch_size, KV_HEADS, group_size, HEAD_DIM).astype(jnp.float32)
    key_heads = key_cache.reshape(batch_size, span_len, KV_HEADS, HEAD_DIM).astype(jnp.float32)
    value_heads = value_cache.reshape(batch_size, span_len, KV_HEADS, HEAD_DIM).astype(jnp.float32)
    scores = jnp.einsum('bkgd,bskd->bkgs', query_heads, key_heads) * HEAD_DIM ** (-0.5)
    scores = scores + head_bias.reshape(KV_HEADS, group_size)[None, :, :, None]
    live_mask = (jnp.arange(span_len, dtype=jnp.int32)[None, :] < lengths[:, None])[:, None, None, :]
    log_remain = jnp.where(live_mask, jax.nn.log_sigmoid(-scores), 0.0)
    remain_after = lax.cumsum(log_remain, axis=3, reverse=True) - log_remain
    weights = jnp.where(live_mask, jnp.exp(jax.nn.log_sigmoid(scores) + remain_after), 0.0).astype(jnp.bfloat16)
    mixed_heads = jnp.einsum('bkgs,bskd->bkgd', weights.astype(jnp.float32), value_heads)
    return mixed_heads.reshape(batch_size, HEADS * HEAD_DIM).astype(jnp.bfloat16)

def expert_apply(expert, pair_rows, expert_gate_w, expert_up_w, expert_down_w):
    gate_w = lax.dynamic_index_in_dim(expert_gate_w, expert, 0, keepdims=False)
    up_w = lax.dynamic_index_in_dim(expert_up_w, expert, 0, keepdims=False)
    down_w = lax.dynamic_index_in_dim(expert_down_w, expert, 0, keepdims=False)
    gate_pre = jnp.dot(pair_rows, gate_w, preferred_element_type=jnp.float32)
    upper_pre = jnp.dot(pair_rows, up_w, preferred_element_type=jnp.float32)
    hidden = (jax.nn.silu(gate_pre) * upper_pre).astype(jnp.bfloat16)
    return jnp.dot(hidden, down_w, preferred_element_type=jnp.float32).astype(jnp.bfloat16)

def reference(tokens, cache_keys, cache_values, cache_len, norm_gain_first, w_query, w_key, w_value, head_bias, w_output, norm_gain_second, group_id, member, group_gate, member_weight, expert_gate_w, expert_up_w, expert_down_w, dense_gate_w, dense_up_w, hidden_gain, dense_down_w, branch_logit):
    stream = tokens.astype(jnp.float32)
    normed_first = (stream * rms_scale(stream) * norm_gain_first).astype(jnp.bfloat16)
    queries = jnp.dot(normed_first, w_query, preferred_element_type=jnp.float32).astype(jnp.bfloat16)
    new_keys = jnp.dot(normed_first, w_key, preferred_element_type=jnp.float32).astype(jnp.bfloat16)
    new_values = jnp.dot(normed_first, w_value, preferred_element_type=jnp.float32).astype(jnp.bfloat16)

    def attend_block(block_args):
        block_queries, block_keys, block_values, block_lens = block_args
        return stick_read(block_queries, block_keys, block_values, block_lens, head_bias)
    attended = lax.map(attend_block, (queries.reshape(N_EP, SEQ_DEV, HEADS * HEAD_DIM), cache_keys.reshape(N_EP, SEQ_DEV, CACHE, KV_HEADS * HEAD_DIM), cache_values.reshape(N_EP, SEQ_DEV, CACHE, KV_HEADS * HEAD_DIM), cache_len.reshape(N_EP, SEQ_DEV))).reshape(TOKENS, HEADS * HEAD_DIM)
    projected = jnp.dot(attended, w_output, preferred_element_type=jnp.float32).astype(jnp.bfloat16)
    second_stream = stream + projected.astype(jnp.float32)
    normed_second = (second_stream * rms_scale(second_stream) * norm_gain_second).astype(jnp.bfloat16)
    pair_expert = (group_id[:, None] * PER_GROUP + member).reshape(-1).astype(jnp.int32)
    pair_total = pair_expert.shape[0]
    sort_order = jnp.argsort(pair_expert, stable=True).astype(jnp.int32)
    sorted_expert = pair_expert[sort_order]
    pair_rows = normed_second[sort_order // TOP_K]

    def run_block(block_index):
        block_rows = lax.dynamic_slice_in_dim(pair_rows, block_index * pair_block, pair_block, 0)
        block_expert = lax.dynamic_slice_in_dim(sorted_expert, block_index * pair_block, pair_block, 0)

        def visit(expert, accum):
            result_rows = expert_apply(expert, block_rows, expert_gate_w, expert_up_w, expert_down_w)
            return jnp.where((block_expert == expert)[:, None], result_rows.astype(jnp.float32), accum)
        return lax.fori_loop(block_expert[0], block_expert[pair_block - 1] + 1, visit, jnp.zeros((pair_block, D), jnp.float32))
    sorted_out = lax.map(run_block, jnp.arange(pair_total // pair_block, dtype=jnp.int32)).reshape(pair_total, D)
    expert_out = jnp.zeros((pair_total, D), jnp.float32).at[sort_order].set(sorted_out)
    combine = group_gate[:, None] * member_weight
    routed = lax.optimization_barrier(jnp.sum(expert_out.reshape(TOKENS, TOP_K, D) * combine[:, :, None], axis=1))
    dense_gate = jnp.dot(normed_second, dense_gate_w, preferred_element_type=jnp.float32)
    dense_upper = jnp.dot(normed_second, dense_up_w, preferred_element_type=jnp.float32)
    dense_hidden = jax.nn.silu(dense_gate) * dense_upper
    dense_normed = (dense_hidden * rms_scale(dense_hidden) * hidden_gain).astype(jnp.bfloat16)
    dense_out = jnp.dot(dense_normed, dense_down_w, preferred_element_type=jnp.float32).astype(jnp.bfloat16)
    mixed_out = second_stream + routed + jax.nn.sigmoid(branch_logit) * dense_out.astype(jnp.float32)
    return (mixed_out.astype(jnp.bfloat16), new_keys, new_values)
```

```python
import functools

import jax
import jax.numpy as jnp
from jax import lax
from jax.experimental import pallas as pl
from jax.experimental.pallas import tpu as pltpu
from jax.sharding import PartitionSpec as P

D = 2048
HEADS = 32
HEAD_DIM = 64
SEQ = 16
CACHE = 1024
BLK = 256
EPS = 1e-06
F32 = jnp.float32
BF = jnp.bfloat16
MESH = pl.DeviceIdType.MESH
NT = (((1,), (1,)), ((), ()))
HI = lax.Precision.HIGHEST


def iota(shape, dim):
    return lax.broadcasted_iota(jnp.int32, shape, dim)


def one_hot(mask):
    return jnp.where(mask, 1.0, 0.0)


def dot(a, b):
    return jnp.dot(a, b, preferred_element_type=F32)


def dot_nt(a, b):
    return lax.dot_general(a, b, NT, preferred_element_type=F32)


def split2(v):
    high = v.astype(BF)
    return high, (v - high.astype(F32)).astype(BF)


def remote(src, dst, sems, target):
    return pltpu.make_async_remote_copy(
        src_ref=src,
        dst_ref=dst,
        send_sem=sems.at[0],
        recv_sem=sems.at[1],
        device_id=(target,),
        device_id_type=MESH,
    )


def take(ref, sem):
    pltpu.make_async_copy(ref, ref, sem).wait()


def lanes(k):
    return pl.ds(pl.multiple_of(k * BLK, BLK), BLK)


def kernel(
    tok, ck, cv, clen, g1, wq, wk, wv, hb, wo, g2, gid, mem, gg, mw, eg, eu, ed, wg, wu, hg, wd, bl,
    out, nk, nv,
    kb, vb, egb, eub, edb, wkb, wvb,
    wqb, wob, wgb, wub, wdb,
    xa, xc, xd, qs, qr, ts, tb, cs0, cb, cs, cd, pq, po, qstack, qb, ob, ps, pr, ys,
    sq, sqr, zb, zs, zr, hbuf,
    lsem, s_wq, s_wo, s_wg, s_wu, s_wd, s_pair, s_ex, s_xa, s_xc, s_ts, s_cb, s_cd, s_q, s_pr, s_y, s_sq, s_z,
):
    me = lax.axis_index("ep")
    chip = me // 2
    core = me % 2
    group = me // 16
    place = chip % 8
    pair = chip * 2 + (1 - core)

    local = [
        pltpu.make_async_copy(ck, kb, lsem.at[0]),
        pltpu.make_async_copy(cv, vb, lsem.at[1]),
        pltpu.make_async_copy(wk, wkb, lsem.at[2]),
        pltpu.make_async_copy(wv, wvb, lsem.at[3]),
        pltpu.make_async_copy(eg.at[0], egb.at[0], lsem.at[4]),
        pltpu.make_async_copy(eu.at[0], eub.at[0], lsem.at[5]),
        pltpu.make_async_copy(ed.at[0], edb.at[0], lsem.at[6]),
    ]

    barrier = pltpu.get_barrier_semaphore()

    def greet(k, carry):
        other = (chip + k) % 64 * 2 + core
        pl.semaphore_signal(barrier, inc=1, device_id=(other,), device_id_type=MESH)
        return carry

    pl.semaphore_signal(barrier, inc=1, device_id=(pair,), device_id_type=MESH)
    lax.fori_loop(1, 64, greet, 0)
    for c in local:
        c.start()

    x = tok[...].astype(F32)
    normed = (x * lax.rsqrt(jnp.mean(x * x, axis=-1, keepdims=True) + EPS) * g1[...]).astype(BF)
    xa[place] = normed
    gids = gid[...]
    hits = one_hot(iota((8, SEQ), 0) == gids)
    before = dot(hits, one_hot(iota((SEQ, SEQ), 0) < iota((SEQ, SEQ), 1)))
    rank = jnp.sum(hits * before, axis=0, keepdims=True).astype(jnp.int32)
    spot = gids * 2 + rank
    order = one_hot(iota((SEQ, SEQ), 0) == spot)
    eye16 = iota((SEQ, SEQ), 0) == iota((SEQ, SEQ), 1)
    spot_col = jnp.sum(jnp.where(eye16, jnp.broadcast_to(spot, (SEQ, SEQ)), 0), axis=1, keepdims=True)
    back = one_hot(iota((SEQ, SEQ), 1) == spot_col).astype(BF)
    order_bf = order.astype(BF)
    sorted_tok = dot(order_bf, tok[...]).astype(BF)
    for k in range(8):
        ts[k] = sorted_tok[:, k * BLK : (k + 1) * BLK]
    share = jnp.zeros((128, SEQ), F32)
    for k in range(6):
        share = share + jnp.where(iota((128, SEQ), 0) == mem[k : k + 1, :], mw[k : k + 1, :], 0.0)
    share = share * gg[...]
    shared = lax.dot_general(order, share, NT, precision=HI, preferred_element_type=F32)
    cs0[...] = shared
    tb[place] = ts[place]
    cb[place] = shared

    pl.semaphore_wait(barrier, 64)

    def spread_strip(strip, buf, sems):
        slot = buf.at[place, core]

        def send(k, carry):
            g = (group + k) % 8
            remote(strip, slot, sems, (g * 8 + group) * 2 + core).start()
            return carry

        @pl.when(place == group)
        def _():
            pltpu.make_async_copy(strip, slot, sems.at[1]).start()

        @pl.when(place != group)
        def _():
            send(0, 0)

        lax.fori_loop(1, 8, send, 0)

    def strip_sent(strip, buf, sems):
        take(buf.at[pl.ds(0, 7), core], sems.at[0])

        @pl.when(place != group)
        def _():
            take(buf.at[0, core], sems.at[0])

    def pass_on(buf, sems, k):
        take(buf.at[:, core], sems.at[1])
        remote(buf.at[:, core], buf.at[:, core], s_pair.at[k], pair).start()

    def in_group(src_of, dst, sems):
        def send(k, carry):
            p = (place + k) % 8
            remote(src_of(p), dst, sems, (group * 8 + p) * 2 + core).start()
            return carry

        lax.fori_loop(1, 8, send, 0)

    def over_plane(src_of, dst_of, sems):
        def send(k, carry):
            other = (chip + k) % 64
            remote(src_of(other), dst_of(other), sems, other * 2 + core).start()
            return carry

        lax.fori_loop(1, 64, send, 0)

    spread_strip(wq, wqb, s_wq)
    in_group(lambda p: xa.at[place], xa.at[place], s_xa)
    in_group(lambda p: ts.at[p], tb.at[place], s_ts)
    in_group(lambda p: cs0, cb.at[place], s_cb)

    local[2].wait()
    local[3].wait()
    nk[...] = dot(normed, wkb[...]).astype(BF)
    nv[...] = dot(normed, wvb[...]).astype(BF)
    rows, cols = iota((512, 512), 0), iota((512, 512), 1)
    pq[...] = one_hot(cols == rows % 32 * 16 + rows // 32).astype(BF)
    po[...] = one_hot(cols == rows % 16 * 32 + rows // 16).astype(BF)
    r, c = iota((128, 128), 0), iota((128, 128), 1)
    regroup = one_hot(c == r % 16 // 2 * 16 + r // 16 * 2 + r % 2)
    fold = one_hot(c == r % 8 * 16 + r // 16 * 2 + r % 16 // 8).astype(BF)
    eye = r == c
    eye32 = iota((32, 32), 0) == iota((32, 32), 1)
    bias = jnp.sum(jnp.where(eye32, jnp.broadcast_to(hb[...], (32, 32)), 0.0), axis=1, keepdims=True)
    tri = one_hot(iota((BLK, BLK), 0) >= iota((BLK, BLK), 1)).astype(BF)

    pass_on(wqb, s_wq, 0)
    take(xa.at[pl.ds(0, 7)], s_xa.at[1])
    take(wqb.at[:, core], s_pair.at[0, 1])
    q = dot_nt(xa[...].reshape(128, D), wqb[...].reshape(BLK, D)).astype(BF)
    qs[...] = q.reshape(8, SEQ, BLK)
    qr[:, lanes(place)] = qs[place]
    in_group(lambda p: qs.at[p], qr.at[:, lanes(place)], s_q)

    spread_strip(wo, wob, s_wo)
    remote(eg.at[0], egb.at[1], s_ex.at[0], pair).start()
    remote(eu.at[0], eub.at[1], s_ex.at[1], pair).start()
    remote(ed.at[0], edb.at[1], s_ex.at[2], pair).start()

    take(tb.at[pl.ds(0, 7)], s_ts.at[1])
    take(cb.at[pl.ds(0, 7)], s_cb.at[1])
    combs = jnp.dot(regroup, cb[...].reshape(128, 128), precision=HI, preferred_element_type=F32)
    cs[...] = combs.reshape(8, SEQ, 128)
    cd[group] = cs[group]

    def send_comb(k, carry):
        g = (group + k) % 8
        remote(cs.at[g], cd.at[group], s_cd, (g * 8 + place) * 2 + core).start()
        return carry

    lax.fori_loop(1, 8, send_comb, 0)

    take(qr.at[:, pl.ds(0, 7 * BLK)], s_q.at[1])
    left = iota((SEQ, 128), 1) < HEAD_DIM
    for t in range(16):
        v = qr[:, t * 128 : (t + 1) * 128].astype(F32) * HEAD_DIM**-0.5
        w = pltpu.roll(v, HEAD_DIM, 1)
        first, second = (v, w) if t < 8 else (w, v)
        keep = left if t < 8 else jnp.logical_not(left)
        qstack[32 * t : 32 * t + 16, :] = jnp.where(keep, first, 0.0).astype(BF)
        qstack[32 * t + 16 : 32 * t + 32, :] = jnp.where(keep, second, 0.0).astype(BF)
    qb[...] = dot(pq[...], qstack[...]).astype(BF).reshape(SEQ, HEADS, 128)
    local[0].wait()
    local[1].wait()
    spread_strip(wg, wgb, s_wg)
    spread_strip(wu, wub, s_wu)

    def attend(b, carry):
        s = dot_nt(qb[b], kb[b]) + bias
        live = iota((HEADS, CACHE), 1) < clen[b]
        rest = jnp.where(live, -(jnp.maximum(s, 0.0) + jnp.log(1.0 + jnp.exp(-jnp.abs(s)))), 0.0)
        high, low = split2(rest)
        parts = [v[:, n * BLK : (n + 1) * BLK] for v in (high, low) for n in range(4)]
        sums = dot(jnp.concatenate(parts, axis=0), tri)
        run = jnp.zeros((HEADS, 1), F32)
        later = []
        for n in (3, 2, 1, 0):
            within = sums[n * 32 : n * 32 + 32] + sums[128 + n * 32 : 160 + n * 32]
            later.append(within + run)
            run = run + within[:, 0:1]
        later = jnp.concatenate(later[::-1], axis=1)
        weights = jnp.where(live, jnp.exp(s + later), 0.0).astype(BF)
        ob[b] = dot(weights, vb[b]).astype(BF)
        return carry

    lax.fori_loop(0, 8, attend, 0)
    pass_on(wob, s_wo, 1)
    lax.fori_loop(8, 16, attend, 0)

    heads = dot(po[...], ob[...].reshape(512, 128))
    for t in range(16):
        a = heads[32 * t : 32 * t + 16, :]
        b = heads[32 * t + 16 : 32 * t + 32, :]
        if t < 8:
            joined = jnp.where(left, a, pltpu.roll(b, HEAD_DIM, 1))
        else:
            joined = jnp.where(left, pltpu.roll(a, HEAD_DIM, 1), b)
        xc[place, :, t * 128 : (t + 1) * 128] = dot(order_bf, joined.astype(BF)).astype(BF)
    in_group(lambda p: xc.at[place], xc.at[place], s_xc)

    over_plane(lambda o: wd.at[:, lanes(o % 8)], lambda o: wdb.at[chip, core], s_wd)
    own_wd = pltpu.make_async_copy(wd.at[:, lanes(place)], wdb.at[chip, core], lsem.at[7])
    own_wd.start()

    take(wob.at[:, core], s_pair.at[1, 1])
    take(xc.at[pl.ds(0, 7)], s_xc.at[1])
    proj = dot_nt(xc[...].reshape(128, D), wob[...].reshape(BLK, D)).astype(BF)
    stream = tb[...].reshape(128, BLK).astype(F32) + proj.astype(F32)
    y = (stream * g2[:, lanes(place)]).astype(BF)
    ys[...] = dot(regroup.astype(BF), y).astype(BF).reshape(8, SEQ, BLK)
    xd[group, :, lanes(place)] = ys[group]
    over_plane(lambda o: ys.at[o // 8], lambda o: xd.at[group, :, lanes(place)], s_y)
    ps[...] = proj.reshape(8, SEQ, BLK)
    pr[:, lanes(place)] = ps[place]
    in_group(lambda p: ps.at[p], pr.at[:, lanes(place)], s_pr)

    pass_on(wgb, s_wg, 2)
    pass_on(wub, s_wu, 3)
    own_wd.wait()
    take(wdb.at[pl.ds(0, 63), core], s_wd.at[1])
    remote(wdb.at[:, core], wdb.at[:, core], s_pair.at[4], pair).start()
    take(cd.at[pl.ds(0, 7)], s_cd.at[1])
    lane = iota((128, 128), 1)
    comb = cd[...].reshape(128, 128)
    member0 = place * 2 + core
    member1 = place * 2 + 1 - core
    comb0 = jnp.sum(jnp.where(lane == member0, comb, 0.0), axis=1, keepdims=True)
    comb1 = jnp.sum(jnp.where(lane == member1, comb, 0.0), axis=1, keepdims=True)

    take(zr.at[pl.ds(0, 63)], s_y.at[1])
    rows_in = xd[...].reshape(128, D)
    plain = rows_in.astype(F32) * (1.0 / g2[...])
    scale = lax.rsqrt(jnp.mean(plain * plain, axis=1, keepdims=True) + EPS)
    take(wgb.at[:, core], s_pair.at[2, 1])
    take(wub.at[:, core], s_pair.at[3, 1])
    gate = dot_nt(rows_in, wgb[...].reshape(BLK, D)) * scale
    upper = dot_nt(rows_in, wub[...].reshape(BLK, D)) * scale
    hidden = gate * jax.nn.sigmoid(gate) * upper
    part = jnp.sum(hidden * hidden, axis=1, keepdims=True)
    part_row = jnp.sum(jnp.where(eye, jnp.broadcast_to(part, (128, 128)), 0.0), axis=0, keepdims=True)
    sq[...] = jnp.broadcast_to(part_row, (8, 128))
    sqr[place] = sq[...]
    in_group(lambda p: sq, sqr.at[place], s_sq)

    for e, comb_e in ((0, comb0), (1, comb1)):
        if e == 0:
            for k in (4, 5, 6):
                local[k].wait()
        else:
            take(egb.at[1], s_ex.at[0, 1])
            take(eub.at[1], s_ex.at[1, 1])
            take(edb.at[1], s_ex.at[2, 1])
        gate_e = dot(rows_in, egb[e]) * scale
        upper_e = dot(rows_in, eub[e]) * scale
        hbuf[:, e * 512 : (e + 1) * 512] = (gate_e * jax.nn.sigmoid(gate_e) * upper_e * comb_e).astype(BF)

    take(sqr.at[pl.ds(0, 7)], s_sq.at[1])
    total = jnp.sum(sqr[...], axis=0)[0:1, :]
    total_col = jnp.sum(jnp.where(eye, jnp.broadcast_to(total, (128, 128)), 0.0), axis=1, keepdims=True)
    dense_scale = lax.rsqrt(total_col * (1.0 / D) + EPS)
    dense = (hidden * dense_scale * hg[:, lanes(place)]).astype(BF)
    take(wdb.at[:, core], s_pair.at[4, 1])

    def produce(k, carry):
        routed = dot(hbuf[...], edb[:, :, lanes(k)].reshape(1024, BLK))
        down = dot_nt(dense, wdb[pl.ds(k * 8, 8)].reshape(BLK, BLK))
        z = routed + jax.nn.sigmoid(bl[:, lanes(k)]) * down
        zb[k] = z.astype(BF).reshape(8, SEQ, BLK)
        return carry

    lax.fori_loop(0, 8, produce, 0)

    def give(k, carry):
        g = (group + k) % 8
        zs[g] = dot(fold, zb[:, g].reshape(128, BLK)).astype(BF).reshape(8, SEQ, BLK)

        def send(j, carry):
            p = (place + j) % 8
            remote(zs.at[g, p], zr.at[chip], s_z, (g * 8 + p) * 2 + core).start()
            return carry

        @pl.when(g == group)
        def _():
            zr[chip] = zs[g, place]

        @pl.when(g != group)
        def _():
            send(0, 0)

        lax.fori_loop(1, 8, send, 0)
        return carry

    lax.fori_loop(0, 8, give, 0)

    spots = dot_nt(one_hot(iota((128, SEQ), 0) % 16 == iota((128, SEQ), 1)), order)
    unfold = dot(spots, one_hot(iota((SEQ, 128), 1) // 8 == iota((SEQ, 128), 0)))
    unfold = jnp.where(r // 16 == c % 8, unfold, 0.0).astype(BF)
    take(pr.at[:, pl.ds(0, 7 * BLK)], s_pr.at[1])
    second = tok[...].astype(F32) + dot(back, pr[...])
    take(zr.at[pl.ds(0, 63)], s_z.at[1])
    sums = jnp.sum(zr[...].reshape(8, 8, SEQ, BLK).astype(F32), axis=1).reshape(128, BLK)
    high, low = split2(sums)
    branch = dot(unfold, high) + dot(unfold, low)
    for k in range(8):
        s = slice(k * BLK, (k + 1) * BLK)
        out[:, s] = (second[:, s] + branch[k * 16 : k * 16 + 16]).astype(BF)

    strip_sent(wq, wqb, s_wq)
    strip_sent(wo, wob, s_wo)
    strip_sent(wg, wgb, s_wg)
    strip_sent(wu, wub, s_wu)
    take(wdb.at[pl.ds(0, 63), core], s_wd.at[0])
    for k, buf in enumerate((wqb, wob, wgb, wub, wdb)):
        take(buf.at[:, core], s_pair.at[k, 0])
    take(egb.at[1], s_ex.at[0, 0])
    take(eub.at[1], s_ex.at[1, 0])
    take(edb.at[1], s_ex.at[2, 0])
    take(xa.at[pl.ds(0, 7)], s_xa.at[0])
    take(xc.at[pl.ds(0, 7)], s_xc.at[0])
    take(tb.at[pl.ds(0, 7)], s_ts.at[0])
    take(cb.at[pl.ds(0, 7)], s_cb.at[0])
    take(cd.at[pl.ds(0, 7)], s_cd.at[0])
    take(qr.at[:, pl.ds(0, 7 * BLK)], s_q.at[0])
    take(pr.at[:, pl.ds(0, 7 * BLK)], s_pr.at[0])
    take(zr.at[pl.ds(0, 63)], s_y.at[0])
    take(sqr.at[pl.ds(0, 7)], s_sq.at[0])
    take(zr.at[pl.ds(0, 63)], s_z.at[0])


def shards(
    tokens, cache_keys, cache_values, cache_len, norm_gain_first, w_query, w_key, w_value, head_bias,
    w_output, norm_gain_second, group_id, member, group_gate, member_weight, expert_gate_w, expert_up_w,
    expert_down_w, dense_gate_w, dense_up_w, hidden_gain, dense_down_w, branch_logit,
):
    vmem = pl.BlockSpec(memory_space=pltpu.VMEM)
    hbm = pl.BlockSpec(memory_space=pl.ANY)
    smem = pl.BlockSpec(memory_space=pltpu.SMEM)
    V = pltpu.VMEM
    strips = (8, 2, SEQ, D)
    pair_sem = pltpu.SemaphoreType.DMA((2,))
    args = (
        (tokens, vmem),
        (cache_keys, hbm),
        (cache_values, hbm),
        (cache_len, smem),
        (norm_gain_first.reshape(1, D), vmem),
        (w_query.T, vmem),
        (w_key, hbm),
        (w_value, hbm),
        (head_bias.reshape(1, HEADS), vmem),
        (w_output.T, vmem),
        (norm_gain_second.reshape(1, D), vmem),
        (group_id.reshape(1, SEQ), vmem),
        (member.T, vmem),
        (group_gate.reshape(1, SEQ), vmem),
        (member_weight.T, vmem),
        (expert_gate_w, hbm),
        (expert_up_w, hbm),
        (expert_down_w, hbm),
        (dense_gate_w.T, vmem),
        (dense_up_w.T, vmem),
        (hidden_gain.reshape(1, D), vmem),
        (dense_down_w.T, vmem),
        (branch_logit.reshape(1, D), vmem),
    )
    scratch = [
        V((SEQ, CACHE, 128), BF),
        V((SEQ, CACHE, 128), BF),
        V((2, D, 512), BF),
        V((2, D, 512), BF),
        V((2, 512, D), BF),
        V((D, 128), BF),
        V((D, 128), BF),
        V(strips, BF),
        V(strips, BF),
        V(strips, BF),
        V(strips, BF),
        V((64, 2, SEQ, BLK), BF),
        V((8, SEQ, D), BF),
        V((8, SEQ, D), BF),
        V((8, SEQ, D), BF),
        V((8, SEQ, BLK), BF),
        V((SEQ, D), BF),
        V((8, SEQ, BLK), BF),
        V((8, SEQ, BLK), BF),
        V((SEQ, 128), F32),
        V((8, SEQ, 128), F32),
        V((8, SEQ, 128), F32),
        V((8, SEQ, 128), F32),
        V((512, 512), BF),
        V((512, 512), BF),
        V((512, 128), BF),
        V((SEQ, HEADS, 128), BF),
        V((SEQ, HEADS, 128), BF),
        V((8, SEQ, BLK), BF),
        V((SEQ, D), BF),
        V((8, SEQ, BLK), BF),
        V((8, 128), F32),
        V((8, 8, 128), F32),
        V((8, 8, SEQ, BLK), BF),
        V((8, 8, SEQ, BLK), BF),
        V((64, SEQ, BLK), BF),
        V((128, 1024), BF),
        pltpu.SemaphoreType.DMA((8,)),
        pair_sem,
        pair_sem,
        pair_sem,
        pair_sem,
        pair_sem,
        pltpu.SemaphoreType.DMA((5, 2)),
        pltpu.SemaphoreType.DMA((3, 2)),
    ] + [pair_sem] * 10
    return pl.pallas_call(
        kernel,
        out_shape=(
            jax.ShapeDtypeStruct((SEQ, D), BF),
            jax.ShapeDtypeStruct((SEQ, 128), BF),
            jax.ShapeDtypeStruct((SEQ, 128), BF),
        ),
        in_specs=[spec for _, spec in args],
        out_specs=(vmem, vmem, vmem),
        scratch_shapes=scratch,
        compiler_params=pltpu.CompilerParams(
            collective_id=0, has_side_effects=True, vmem_limit_bytes=62_000_000
        ),
    )(*[a for a, _ in args])


def solution(mesh):
    in_specs = (
        P("ep", None),
        P("ep", None, None),
        P("ep", None, None),
        P("ep"),
        P(),
        P(None, "ep"),
        P(),
        P(),
        P(),
        P(None, "ep"),
        P(),
        P("ep"),
        P("ep", None),
        P("ep"),
        P("ep", None),
        P("ep", None, None),
        P("ep", None, None),
        P("ep", None, None),
        P(None, "ep"),
        P(None, "ep"),
        P(),
        P(None, "ep"),
        P(),
    )
    out_specs = (P("ep", None), P("ep", None), P("ep", None))
    return jax.shard_map(shards, mesh=mesh, in_specs=in_specs, out_specs=out_specs, check_vma=False)
```

```python
import functools

import jax
import jax.numpy as jnp
from jax import lax
from jax.experimental import pallas as pl
from jax.experimental.pallas import tpu as pltpu
from jax.sharding import PartitionSpec as P

D = 2048
HEADS = 32
HEAD_DIM = 64
SEQ = 16
CACHE = 1024
BLK = 256
EPS = 1e-06
F32 = jnp.float32
BF = jnp.bfloat16
MESH = pl.DeviceIdType.MESH
NT = (((1,), (1,)), ((), ()))
HI = lax.Precision.HIGHEST


def iota(shape, dim):
    return lax.broadcasted_iota(jnp.int32, shape, dim)


def one_hot(mask):
    return jnp.where(mask, 1.0, 0.0)


def dot(a, b):
    return jnp.dot(a, b, preferred_element_type=F32)


def dot_nt(a, b):
    return lax.dot_general(a, b, NT, preferred_element_type=F32)


def split2(v):
    high = v.astype(BF)
    return high, (v - high.astype(F32)).astype(BF)


def remote(src, dst, sems, target):
    return pltpu.make_async_remote_copy(
        src_ref=src,
        dst_ref=dst,
        send_sem=sems.at[0],
        recv_sem=sems.at[1],
        device_id=(target,),
        device_id_type=MESH,
    )


def take(ref, sem):
    pltpu.make_async_copy(ref, ref, sem).wait()


def chip_of(g, p):
    return g * 8 + (p // 4 + g) % 2 * 4 + p % 4


def gather_lanes(tiles, pieces):
    quarter = iota(tiles[0].shape, 1) // 32
    made = None
    for at, (tile, piece) in enumerate(pieces):
        shift = (at - piece) * 32 % 128
        v = pltpu.roll(tiles[tile], shift, 1) if shift else tiles[tile]
        made = v if made is None else jnp.where(quarter == at, v, made)
    return made


def tiles_of(v):
    return [v[:, t * 128 : (t + 1) * 128] for t in range(D // 128)]


def to_block_order(tiles):
    made = []
    for t in range(16):
        p, half = t // 2, t % 2
        chips = [chip_of(half * 4 + k, p) for k in range(4)]
        made.append(gather_lanes(tiles, [(c // 4, c % 4) for c in chips]))
    return made


def from_block_order(tiles):
    made = []
    for v in range(16):
        g, yl = v // 2, v % 2
        places = [(yl + g) % 2 * 4 + x for x in range(4)]
        made.append(gather_lanes(tiles, [(p * 2 + g // 4, g % 4) for p in places]))
    return made


def lanes(k):
    return pl.ds(pl.multiple_of(k * BLK, BLK), BLK)


def kernel(
    tok, ck, cv, clen, g1, wq, wk, wv, hb, wo, g2, gid, mem, gg, mw, eg, eu, ed, wg, wu, hg, wd, bl,
    out, nk, nv,
    kb, vb, egb, eub, edb, wkb, wvb,
    wqb, wob, wgb, wub, wdb,
    xa, xc, xd, qs, qr, ts, tb, cs0, cb, cs, cd, pq, po, qstack, qb, ob, ps, pr, ys,
    sq, sqr, zb, zs, zr, hbuf, g2b, hgb, wgp, wup, wdp,
    lsem, s_wq, s_wo, s_wg, s_wu, s_wd, s_pair, s_ex, s_xa, s_xc, s_ts, s_cb, s_cd, s_q, s_pr, s_y, s_sq, s_z,
):
    me = lax.axis_index("ep")
    chip = me // 2
    core = me % 2
    group = me // 16
    place = (chip % 8 // 4 + group) % 2 * 4 + chip % 4
    pair = chip * 2 + (1 - core)

    local = [
        pltpu.make_async_copy(ck, kb, lsem.at[0]),
        pltpu.make_async_copy(cv, vb, lsem.at[1]),
        pltpu.make_async_copy(wk, wkb, lsem.at[2]),
        pltpu.make_async_copy(wv, wvb, lsem.at[3]),
        pltpu.make_async_copy(ed.at[0], edb.at[0], lsem.at[4]),
    ]

    def load_experts(k, carry):
        src = pl.ds(pl.multiple_of(chip_of(k % 8, k // 8) * 32, 32), 32)
        dst = pl.ds(pl.multiple_of(k * 32, 32), 32)
        pltpu.make_async_copy(eg.at[0, src], egb.at[0, dst], lsem.at[5]).start()
        pltpu.make_async_copy(eu.at[0, src], eub.at[0, dst], lsem.at[6]).start()
        return carry

    barrier = pltpu.get_barrier_semaphore()

    def greet(k, carry):
        other = (chip + k) % 64 * 2 + core
        pl.semaphore_signal(barrier, inc=1, device_id=(other,), device_id_type=MESH)
        return carry

    pl.semaphore_signal(barrier, inc=1, device_id=(pair,), device_id_type=MESH)
    lax.fori_loop(1, 64, greet, 0)
    for c in local:
        c.start()
    lax.fori_loop(0, 64, load_experts, 0)

    x = tok[...].astype(F32)
    normed = (x * lax.rsqrt(jnp.mean(x * x, axis=-1, keepdims=True) + EPS) * g1[...]).astype(BF)
    xa[place] = normed
    gids = gid[...]
    hits = one_hot(iota((8, SEQ), 0) == gids)
    before = dot(hits, one_hot(iota((SEQ, SEQ), 0) < iota((SEQ, SEQ), 1)))
    rank = jnp.sum(hits * before, axis=0, keepdims=True).astype(jnp.int32)
    spot = gids * 2 + rank
    order = one_hot(iota((SEQ, SEQ), 0) == spot)
    eye16 = iota((SEQ, SEQ), 0) == iota((SEQ, SEQ), 1)
    spot_col = jnp.sum(jnp.where(eye16, jnp.broadcast_to(spot, (SEQ, SEQ)), 0), axis=1, keepdims=True)
    back = one_hot(iota((SEQ, SEQ), 1) == spot_col).astype(BF)
    order_bf = order.astype(BF)
    share = jnp.zeros((128, SEQ), F32)
    for k in range(6):
        share = share + jnp.where(iota((128, SEQ), 0) == mem[k : k + 1, :], mw[k : k + 1, :], 0.0)
    share = share * gg[...]
    shared = lax.dot_general(order, share, NT, precision=HI, preferred_element_type=F32)
    cs0[...] = shared
    cb[place] = shared

    pl.semaphore_wait(barrier, 64)

    def spread_strip(strip, buf, sems):
        slot = buf.at[group, core]

        def send(k, carry):
            g = (group + k) % 8
            remote(strip, slot, sems, chip_of(g, place) * 2 + core).start()
            return carry

        pltpu.make_async_copy(strip, slot, sems.at[1]).start()
        lax.fori_loop(1, 8, send, 0)

    def pass_on(buf, sems, k):
        take(buf.at[:, core], sems.at[1])
        remote(buf.at[:, core], buf.at[:, core], s_pair.at[k], pair).start()

    def in_group(src_of, dst, sems):
        def send(k, carry):
            p = (place + k) % 8
            remote(src_of(p), dst, sems, chip_of(group, p) * 2 + core).start()
            return carry

        lax.fori_loop(1, 8, send, 0)

    def over_plane(src_of, dst_of, sems):
        def send(k, carry):
            other = (chip + k) % 64
            remote(src_of(other), dst_of(other), sems, other * 2 + core).start()
            return carry

        lax.fori_loop(1, 64, send, 0)

    spread_strip(wq, wqb, s_wq)
    in_group(lambda p: xa.at[place], xa.at[place], s_xa)
    in_group(lambda p: cs0, cb.at[place], s_cb)

    moved = to_block_order(tiles_of(dot(order_bf, tok[...])))
    for k in range(8):
        ts[k] = jnp.concatenate(moved[2 * k : 2 * k + 2], axis=1).astype(BF)
    tb[place] = ts[place]
    in_group(lambda p: ts.at[p], tb.at[place], s_ts)
    for src, dst in ((g2, g2b), (hg, hgb), (wg, wgp), (wu, wup), (wd, wdp)):
        for k, tile in enumerate(to_block_order(tiles_of(src[...].astype(F32)))):
            dst[:, k * 128 : (k + 1) * 128] = tile.astype(dst.dtype)
    local[2].wait()
    local[3].wait()
    nk[...] = dot(normed, wkb[...]).astype(BF)
    nv[...] = dot(normed, wvb[...]).astype(BF)
    rows, cols = iota((512, 512), 0), iota((512, 512), 1)
    pq[...] = one_hot(cols == rows % 32 * 16 + rows // 32).astype(BF)
    po[...] = one_hot(cols == rows % 16 * 32 + rows // 16).astype(BF)
    r, c = iota((128, 128), 0), iota((128, 128), 1)
    regroup = one_hot(c == r % 16 // 2 * 16 + r // 16 * 2 + r % 2)
    fold = one_hot(c == r % 8 * 16 + r // 16 * 2 + r % 16 // 8).astype(BF)
    eye = r == c
    eye32 = iota((32, 32), 0) == iota((32, 32), 1)
    bias = jnp.sum(jnp.where(eye32, jnp.broadcast_to(hb[...], (32, 32)), 0.0), axis=1, keepdims=True)
    tri = one_hot(iota((BLK, BLK), 0) >= iota((BLK, BLK), 1)).astype(BF)

    pass_on(wqb, s_wq, 0)
    take(xa.at[pl.ds(0, 7)], s_xa.at[1])
    take(wqb.at[:, core], s_pair.at[0, 1])
    q = dot_nt(xa[...].reshape(128, D), wqb[...].reshape(BLK, D)).astype(BF)
    qs[...] = q.reshape(8, SEQ, BLK)
    qr[:, lanes(place)] = qs[place]
    in_group(lambda p: qs.at[p], qr.at[:, lanes(place)], s_q)

    spread_strip(wo, wob, s_wo)
    for k, buf in enumerate((edb, egb, eub)):
        take(buf.at[0], lsem.at[4 + k])
        remote(buf.at[0], buf.at[1], s_ex.at[k], pair).start()

    take(tb.at[pl.ds(0, 7)], s_ts.at[1])
    take(cb.at[pl.ds(0, 7)], s_cb.at[1])
    combs = jnp.dot(regroup, cb[...].reshape(128, 128), precision=HI, preferred_element_type=F32)
    cs[...] = combs.reshape(8, SEQ, 128)
    cd[group] = cs[group]

    def send_comb(k, carry):
        g = (group + k) % 8
        remote(cs.at[g], cd.at[group], s_cd, chip_of(g, place) * 2 + core).start()
        return carry

    lax.fori_loop(1, 8, send_comb, 0)

    take(qr.at[:, pl.ds(0, 7 * BLK)], s_q.at[1])
    left = iota((SEQ, 128), 1) < HEAD_DIM
    for t, v in enumerate(from_block_order(tiles_of(qr[...].astype(F32) * HEAD_DIM**-0.5))):
        w = pltpu.roll(v, HEAD_DIM, 1)
        first, second = (v, w) if t < 8 else (w, v)
        keep = left if t < 8 else jnp.logical_not(left)
        qstack[32 * t : 32 * t + 16, :] = jnp.where(keep, first, 0.0).astype(BF)
        qstack[32 * t + 16 : 32 * t + 32, :] = jnp.where(keep, second, 0.0).astype(BF)
    qb[...] = dot(pq[...], qstack[...]).astype(BF).reshape(SEQ, HEADS, 128)
    local[0].wait()
    local[1].wait()
    spread_strip(wgp, wgb, s_wg)
    spread_strip(wup, wub, s_wu)

    def attend(b, carry):
        s = dot_nt(qb[b], kb[b]) + bias
        live = iota((HEADS, CACHE), 1) < clen[b]
        rest = jnp.where(live, -(jnp.maximum(s, 0.0) + jnp.log(1.0 + jnp.exp(-jnp.abs(s)))), 0.0)
        high, low = split2(rest)
        parts = [v[:, n * BLK : (n + 1) * BLK] for v in (high, low) for n in range(4)]
        sums = dot(jnp.concatenate(parts, axis=0), tri)
        run = jnp.zeros((HEADS, 1), F32)
        later = []
        for n in (3, 2, 1, 0):
            within = sums[n * 32 : n * 32 + 32] + sums[128 + n * 32 : 160 + n * 32]
            later.append(within + run)
            run = run + within[:, 0:1]
        later = jnp.concatenate(later[::-1], axis=1)
        weights = jnp.where(live, jnp.exp(s + later), 0.0).astype(BF)
        ob[b] = dot(weights, vb[b]).astype(BF)
        return carry

    lax.fori_loop(0, 8, attend, 0)
    pass_on(wob, s_wo, 1)
    lax.fori_loop(8, 16, attend, 0)

    heads = dot(po[...], ob[...].reshape(512, 128))
    for t in range(16):
        a = heads[32 * t : 32 * t + 16, :]
        b = heads[32 * t + 16 : 32 * t + 32, :]
        if t < 8:
            joined = jnp.where(left, a, pltpu.roll(b, HEAD_DIM, 1))
        else:
            joined = jnp.where(left, pltpu.roll(a, HEAD_DIM, 1), b)
        xc[place, :, t * 128 : (t + 1) * 128] = dot(order_bf, joined.astype(BF)).astype(BF)
    in_group(lambda p: xc.at[place], xc.at[place], s_xc)

    over_plane(lambda o: wdp.at[:, lanes((o % 8 // 4 + o // 8) % 2 * 4 + o % 4)], lambda o: wdb.at[chip, core], s_wd)
    own_wd = pltpu.make_async_copy(wdp.at[:, lanes(place)], wdb.at[chip, core], lsem.at[7])
    own_wd.start()

    take(wob.at[:, core], s_pair.at[1, 1])
    take(xc.at[pl.ds(0, 7)], s_xc.at[1])
    proj = dot_nt(xc[...].reshape(128, D), wob[...].reshape(BLK, D)).astype(BF)
    stream = tb[...].reshape(128, BLK).astype(F32) + proj.astype(F32)
    y = (stream * g2b[:, lanes(place)]).astype(BF)
    ys[...] = dot(regroup.astype(BF), y).astype(BF).reshape(8, SEQ, BLK)
    xd[group, :, lanes(place)] = ys[group]
    over_plane(lambda o: ys.at[o // 8], lambda o: xd.at[group, :, lanes(place)], s_y)
    ps[...] = proj.reshape(8, SEQ, BLK)
    pr[:, lanes(place)] = ps[place]
    in_group(lambda p: ps.at[p], pr.at[:, lanes(place)], s_pr)

    pass_on(wgb, s_wg, 2)
    pass_on(wub, s_wu, 3)
    own_wd.wait()
    take(wdb.at[pl.ds(0, 63), core], s_wd.at[1])
    remote(wdb.at[:, core], wdb.at[:, core], s_pair.at[4], pair).start()
    take(cd.at[pl.ds(0, 7)], s_cd.at[1])
    lane = iota((128, 128), 1)
    comb = cd[...].reshape(128, 128)
    member0 = chip % 8 * 2 + core
    member1 = chip % 8 * 2 + 1 - core
    comb0 = jnp.sum(jnp.where(lane == member0, comb, 0.0), axis=1, keepdims=True)
    comb1 = jnp.sum(jnp.where(lane == member1, comb, 0.0), axis=1, keepdims=True)

    take(zr.at[pl.ds(0, 63)], s_y.at[1])
    rows_in = xd[...].reshape(128, D)
    plain = rows_in.astype(F32) * (1.0 / g2b[...])
    scale = lax.rsqrt(jnp.mean(plain * plain, axis=1, keepdims=True) + EPS)
    take(wgb.at[:, core], s_pair.at[2, 1])
    take(wub.at[:, core], s_pair.at[3, 1])
    gate = dot_nt(rows_in, wgb[...].reshape(BLK, D)) * scale
    upper = dot_nt(rows_in, wub[...].reshape(BLK, D)) * scale
    hidden = gate * jax.nn.sigmoid(gate) * upper
    part = jnp.sum(hidden * hidden, axis=1, keepdims=True)
    part_row = jnp.sum(jnp.where(eye, jnp.broadcast_to(part, (128, 128)), 0.0), axis=0, keepdims=True)
    sq[...] = jnp.broadcast_to(part_row, (8, 128))
    sqr[place] = sq[...]
    in_group(lambda p: sq, sqr.at[place], s_sq)

    for e, comb_e in ((0, comb0), (1, comb1)):
        if e == 1:
            take(edb.at[1], s_ex.at[0, 1])
            take(egb.at[1], s_ex.at[1, 1])
            take(eub.at[1], s_ex.at[2, 1])
        gate_e = dot(rows_in, egb[e]) * scale
        upper_e = dot(rows_in, eub[e]) * scale
        hbuf[:, e * 512 : (e + 1) * 512] = (gate_e * jax.nn.sigmoid(gate_e) * upper_e * comb_e).astype(BF)

    take(sqr.at[pl.ds(0, 7)], s_sq.at[1])
    total = jnp.sum(sqr[...], axis=0)[0:1, :]
    total_col = jnp.sum(jnp.where(eye, jnp.broadcast_to(total, (128, 128)), 0.0), axis=1, keepdims=True)
    dense_scale = lax.rsqrt(total_col * (1.0 / D) + EPS)
    dense = (hidden * dense_scale * hgb[:, lanes(place)]).astype(BF)
    take(wdb.at[:, core], s_pair.at[4, 1])

    def produce(k, carry):
        routed = dot(hbuf[...], edb[:, :, lanes(k)].reshape(1024, BLK))
        down = dot_nt(dense, wdb[pl.ds(k * 8, 8)].reshape(BLK, BLK))
        z = routed + jax.nn.sigmoid(bl[:, lanes(k)]) * down
        zb[k] = z.astype(BF).reshape(8, SEQ, BLK)
        return carry

    lax.fori_loop(0, 8, produce, 0)

    def give(k, carry):
        g = (group + k) % 8
        zs[g] = dot(fold, zb[:, g].reshape(128, BLK)).astype(BF).reshape(8, SEQ, BLK)

        def send(j, carry):
            p = (place + j) % 8
            remote(zs.at[g, p], zr.at[chip], s_z, chip_of(g, p) * 2 + core).start()
            return carry

        @pl.when(g == group)
        def _():
            zr[chip] = zs[g, place]

        @pl.when(g != group)
        def _():
            send(0, 0)

        lax.fori_loop(1, 8, send, 0)
        return carry

    lax.fori_loop(0, 8, give, 0)

    spots = dot_nt(one_hot(iota((128, SEQ), 0) % 16 == iota((128, SEQ), 1)), order)
    unfold = dot(spots, one_hot(iota((SEQ, 128), 1) // 8 == iota((SEQ, 128), 0)))
    unfold = jnp.where(r // 16 == c % 8, unfold, 0.0).astype(BF)
    take(pr.at[:, pl.ds(0, 7 * BLK)], s_pr.at[1])
    second = from_block_order(tiles_of(dot(back, pr[...])))
    take(zr.at[pl.ds(0, 63)], s_z.at[1])
    sums = jnp.sum(zr[...].reshape(8, 8, SEQ, BLK).astype(F32), axis=1).reshape(128, BLK)
    high, low = split2(sums)
    branch = dot(unfold, high) + dot(unfold, low)
    for k in range(8):
        s = slice(k * BLK, (k + 1) * BLK)
        own = tok[:, s].astype(F32) + jnp.concatenate(second[2 * k : 2 * k + 2], axis=1)
        out[:, s] = (own + branch[k * 16 : k * 16 + 16]).astype(BF)

    take(wqb.at[pl.ds(0, 7), core], s_wq.at[0])
    take(wob.at[pl.ds(0, 7), core], s_wo.at[0])
    take(wgb.at[pl.ds(0, 7), core], s_wg.at[0])
    take(wub.at[pl.ds(0, 7), core], s_wu.at[0])
    take(wdb.at[pl.ds(0, 63), core], s_wd.at[0])
    for k, buf in enumerate((wqb, wob, wgb, wub, wdb)):
        take(buf.at[:, core], s_pair.at[k, 0])
    take(edb.at[1], s_ex.at[0, 0])
    take(egb.at[1], s_ex.at[1, 0])
    take(eub.at[1], s_ex.at[2, 0])
    take(xa.at[pl.ds(0, 7)], s_xa.at[0])
    take(xc.at[pl.ds(0, 7)], s_xc.at[0])
    take(tb.at[pl.ds(0, 7)], s_ts.at[0])
    take(cb.at[pl.ds(0, 7)], s_cb.at[0])
    take(cd.at[pl.ds(0, 7)], s_cd.at[0])
    take(qr.at[:, pl.ds(0, 7 * BLK)], s_q.at[0])
    take(pr.at[:, pl.ds(0, 7 * BLK)], s_pr.at[0])
    take(zr.at[pl.ds(0, 63)], s_y.at[0])
    take(sqr.at[pl.ds(0, 7)], s_sq.at[0])
    take(zr.at[pl.ds(0, 63)], s_z.at[0])


def shards(
    tokens, cache_keys, cache_values, cache_len, norm_gain_first, w_query, w_key, w_value, head_bias,
    w_output, norm_gain_second, group_id, member, group_gate, member_weight, expert_gate_w, expert_up_w,
    expert_down_w, dense_gate_w, dense_up_w, hidden_gain, dense_down_w, branch_logit,
):
    vmem = pl.BlockSpec(memory_space=pltpu.VMEM)
    hbm = pl.BlockSpec(memory_space=pl.ANY)
    smem = pl.BlockSpec(memory_space=pltpu.SMEM)
    V = pltpu.VMEM
    strips = (8, 2, SEQ, D)
    pair_sem = pltpu.SemaphoreType.DMA((2,))
    args = (
        (tokens, vmem),
        (cache_keys, hbm),
        (cache_values, hbm),
        (cache_len, smem),
        (norm_gain_first.reshape(1, D), vmem),
        (w_query.T, vmem),
        (w_key, hbm),
        (w_value, hbm),
        (head_bias.reshape(1, HEADS), vmem),
        (w_output.T, vmem),
        (norm_gain_second.reshape(1, D), vmem),
        (group_id.reshape(1, SEQ), vmem),
        (member.T, vmem),
        (group_gate.reshape(1, SEQ), vmem),
        (member_weight.T, vmem),
        (expert_gate_w, hbm),
        (expert_up_w, hbm),
        (expert_down_w, hbm),
        (dense_gate_w.T, vmem),
        (dense_up_w.T, vmem),
        (hidden_gain.reshape(1, D), vmem),
        (dense_down_w.T, vmem),
        (branch_logit.reshape(1, D), vmem),
    )
    scratch = [
        V((SEQ, CACHE, 128), BF),
        V((SEQ, CACHE, 128), BF),
        V((2, D, 512), BF),
        V((2, D, 512), BF),
        V((2, 512, D), BF),
        V((D, 128), BF),
        V((D, 128), BF),
        V(strips, BF),
        V(strips, BF),
        V(strips, BF),
        V(strips, BF),
        V((64, 2, SEQ, BLK), BF),
        V((8, SEQ, D), BF),
        V((8, SEQ, D), BF),
        V((8, SEQ, D), BF),
        V((8, SEQ, BLK), BF),
        V((SEQ, D), BF),
        V((8, SEQ, BLK), BF),
        V((8, SEQ, BLK), BF),
        V((SEQ, 128), F32),
        V((8, SEQ, 128), F32),
        V((8, SEQ, 128), F32),
        V((8, SEQ, 128), F32),
        V((512, 512), BF),
        V((512, 512), BF),
        V((512, 128), BF),
        V((SEQ, HEADS, 128), BF),
        V((SEQ, HEADS, 128), BF),
        V((8, SEQ, BLK), BF),
        V((SEQ, D), BF),
        V((8, SEQ, BLK), BF),
        V((8, 128), F32),
        V((8, 8, 128), F32),
        V((8, 8, SEQ, BLK), BF),
        V((8, 8, SEQ, BLK), BF),
        V((64, SEQ, BLK), BF),
        V((128, 1024), BF),
        V((1, D), F32),
        V((1, D), F32),
        V((SEQ, D), BF),
        V((SEQ, D), BF),
        V((SEQ, D), BF),
        pltpu.SemaphoreType.DMA((8,)),
        pair_sem,
        pair_sem,
        pair_sem,
        pair_sem,
        pair_sem,
        pltpu.SemaphoreType.DMA((5, 2)),
        pltpu.SemaphoreType.DMA((3, 2)),
    ] + [pair_sem] * 10
    return pl.pallas_call(
        kernel,
        out_shape=(
            jax.ShapeDtypeStruct((SEQ, D), BF),
            jax.ShapeDtypeStruct((SEQ, 128), BF),
            jax.ShapeDtypeStruct((SEQ, 128), BF),
        ),
        in_specs=[spec for _, spec in args],
        out_specs=(vmem, vmem, vmem),
        scratch_shapes=scratch,
        compiler_params=pltpu.CompilerParams(
            collective_id=0, has_side_effects=True, vmem_limit_bytes=62_000_000
        ),
    )(*[a for a, _ in args])


def solution(mesh):
    in_specs = (
        P("ep", None),
        P("ep", None, None),
        P("ep", None, None),
        P("ep"),
        P(),
        P(None, "ep"),
        P(),
        P(),
        P(),
        P(None, "ep"),
        P(),
        P("ep"),
        P("ep", None),
        P("ep"),
        P("ep", None),
        P("ep", None, None),
        P("ep", None, None),
        P("ep", None, None),
        P(None, "ep"),
        P(None, "ep"),
        P(),
        P(None, "ep"),
        P(),
    )
    out_specs = (P("ep", None), P("ep", None), P("ep", None))
    return jax.shard_map(shards, mesh=mesh, in_specs=in_specs, out_specs=out_specs, check_vma=False)
```

```python
import functools

import jax
import jax.numpy as jnp
from jax import lax
from jax.experimental import pallas as pl
from jax.experimental.pallas import tpu as pltpu
from jax.sharding import PartitionSpec as P

D = 2048
HEADS = 32
HEAD_DIM = 64
SEQ = 16
CACHE = 1024
BLK = 256
EPS = 1e-06
F32 = jnp.float32
BF = jnp.bfloat16
MESH = pl.DeviceIdType.MESH
NT = (((1,), (1,)), ((), ()))
HI = lax.Precision.HIGHEST


def iota(shape, dim):
    return lax.broadcasted_iota(jnp.int32, shape, dim)


def one_hot(mask):
    return jnp.where(mask, 1.0, 0.0)


def dot(a, b):
    return jnp.dot(a, b, preferred_element_type=F32)


def dot_nt(a, b):
    return lax.dot_general(a, b, NT, preferred_element_type=F32)


def split2(v):
    high = v.astype(BF)
    return high, (v - high.astype(F32)).astype(BF)


def remote(src, dst, sems, target):
    return pltpu.make_async_remote_copy(
        src_ref=src,
        dst_ref=dst,
        send_sem=sems.at[0],
        recv_sem=sems.at[1],
        device_id=(target,),
        device_id_type=MESH,
    )


def take(ref, sem):
    pltpu.make_async_copy(ref, ref, sem).wait()


def chip_of(g, p):
    return g * 8 + (p // 4 + g) % 2 * 4 + p % 4


def gather_lanes(tiles, pieces):
    quarter = iota(tiles[0].shape, 1) // 32
    made = None
    for at, (tile, piece) in enumerate(pieces):
        shift = (at - piece) * 32 % 128
        v = pltpu.roll(tiles[tile], shift, 1) if shift else tiles[tile]
        made = v if made is None else jnp.where(quarter == at, v, made)
    return made


def tiles_of(v):
    return [v[:, t * 128 : (t + 1) * 128] for t in range(D // 128)]


def to_block_order(tiles):
    made = []
    for t in range(16):
        p, half = t // 2, t % 2
        chips = [chip_of(half * 4 + k, p) for k in range(4)]
        made.append(gather_lanes(tiles, [(c // 4, c % 4) for c in chips]))
    return made


def from_block_order(tiles):
    made = []
    for v in range(16):
        g, yl = v // 2, v % 2
        places = [(yl + g) % 2 * 4 + x for x in range(4)]
        made.append(gather_lanes(tiles, [(p * 2 + g // 4, g % 4) for p in places]))
    return made


def lanes(k):
    return pl.ds(pl.multiple_of(k * BLK, BLK), BLK)


def kernel(
    tok, ck, cv, clen, g1, wq, wk, wv, hb, wo, g2, gid, mem, gg, mw, eg, eu, ed, wg, wu, hg, wd, bl,
    out, nk, nv,
    kb, vb, egb, eub, edb, wkb, wvb,
    wqb, wob, wgb, wub, wdb,
    xa, xc, xd, qs, qr, ts, tb, cs0, cb, cs, cd, pq, po, qstack, qb, ob, ps, pr, ys,
    sq, sqr, zb, zs, zr, hbuf, zf, sc, wt, g2b, hgb, wgp, wup, wdp,
    lsem, s_wq, s_wo, s_wg, s_wu, s_wd, s_pair, s_ex, s_xa, s_xc, s_ts, s_cb, s_cd, s_q, s_pr, s_y, s_sq, s_z, s_wq2, s_xc2,
):
    me = lax.axis_index("ep")
    chip = me // 2
    core = me % 2
    group = me // 16
    place = (chip % 8 // 4 + group) % 2 * 4 + chip % 4
    pair = chip * 2 + (1 - core)

    local = [
        pltpu.make_async_copy(ck, kb, lsem.at[0]),
        pltpu.make_async_copy(cv, vb, lsem.at[1]),
        pltpu.make_async_copy(wk, wkb, lsem.at[2]),
        pltpu.make_async_copy(wv, wvb, lsem.at[3]),
        pltpu.make_async_copy(ed.at[0], edb.at[0], lsem.at[4]),
    ]

    def load_experts(k, carry):
        src = pl.ds(pl.multiple_of(chip_of(k % 8, k // 8) * 32, 32), 32)
        dst = pl.ds(pl.multiple_of(k * 32, 32), 32)
        pltpu.make_async_copy(eg.at[0, src], egb.at[0, dst], lsem.at[5]).start()
        pltpu.make_async_copy(eu.at[0, src], eub.at[0, dst], lsem.at[6]).start()
        return carry

    barrier = pltpu.get_barrier_semaphore()

    def greet(k, carry):
        other = (chip + k) % 64 * 2 + core
        pl.semaphore_signal(barrier, inc=1, device_id=(other,), device_id_type=MESH)
        return carry

    pl.semaphore_signal(barrier, inc=1, device_id=(pair,), device_id_type=MESH)
    lax.fori_loop(1, 64, greet, 0)
    for c in local:
        c.start()
    lax.fori_loop(0, 64, load_experts, 0)

    x = tok[...].astype(F32)
    normed = (x * lax.rsqrt(jnp.mean(x * x, axis=-1, keepdims=True) + EPS) * g1[...]).astype(BF)
    xa[place] = normed
    gids = gid[...]
    hits = one_hot(iota((8, SEQ), 0) == gids)
    before = dot(hits, one_hot(iota((SEQ, SEQ), 0) < iota((SEQ, SEQ), 1)))
    rank = jnp.sum(hits * before, axis=0, keepdims=True).astype(jnp.int32)
    spot = gids * 2 + rank
    order = one_hot(iota((SEQ, SEQ), 0) == spot)
    eye16 = iota((SEQ, SEQ), 0) == iota((SEQ, SEQ), 1)
    share = jnp.zeros((128, SEQ), F32)
    for k in range(6):
        share = share + jnp.where(iota((128, SEQ), 0) == mem[k : k + 1, :], mw[k : k + 1, :], 0.0)
    share = share * gg[...] + jnp.where(iota((128, SEQ), 0) == SEQ, spot.astype(F32), 0.0)
    shared = lax.dot_general(one_hot(eye16), share, NT, precision=HI, preferred_element_type=F32)
    cs0[...] = shared
    cb[place] = shared

    pl.semaphore_wait(barrier, 64)

    def spread_strip(strip, buf, sems):
        slot = buf.at[group, core]

        def send(k, carry):
            g = (group + k) % 8
            remote(strip, slot, sems, chip_of(g, place) * 2 + core).start()
            return carry

        pltpu.make_async_copy(strip, slot, sems.at[1]).start()
        lax.fori_loop(1, 8, send, 0)

    def pass_on(buf, sems, k):
        take(buf.at[:, core], sems.at[1])
        remote(buf.at[:, core], buf.at[:, core], s_pair.at[k], pair).start()

    def in_group(src_of, dst, sems):
        def send(k, carry):
            p = (place + k) % 8
            remote(src_of(p), dst, sems, chip_of(group, p) * 2 + core).start()
            return carry

        lax.fori_loop(1, 8, send, 0)

    def over_plane(src_of, dst_of, sems):
        def send(k, carry):
            other = (chip + k) % 64
            remote(src_of(other), dst_of(other), sems, other * 2 + core).start()
            return carry

        lax.fori_loop(1, 64, send, 0, unroll=7)

    near, far = pl.ds(0, D // 2), pl.ds(D // 2, D // 2)
    spread_strip(wq.at[:, near], wqb.at[:, :, :, near], s_wq)
    spread_strip(wq.at[:, far], wqb.at[:, :, :, far], s_wq2)
    in_group(lambda p: xa.at[place], xa.at[place], s_xa)
    in_group(lambda p: cs0, cb.at[place], s_cb)
    spread_strip(wo, wob, s_wo)

    moved = to_block_order(tiles_of(tok[...].astype(F32)))
    for k in range(8):
        ts[k] = jnp.concatenate(moved[2 * k : 2 * k + 2], axis=1).astype(BF)
    tb[place] = ts[place]
    in_group(lambda p: ts.at[p], tb.at[place], s_ts)
    for src, dst in ((g2, g2b), (hg, hgb), (wg, wgp), (wu, wup), (wd, wdp)):
        for k, tile in enumerate(to_block_order(tiles_of(src[...].astype(F32)))):
            dst[:, k * 128 : (k + 1) * 128] = tile.astype(dst.dtype)
    spread_strip(wgp, wgb, s_wg)
    spread_strip(wup, wub, s_wu)
    local[2].wait()
    local[3].wait()
    nk[...] = dot(normed, wkb[...]).astype(BF)
    nv[...] = dot(normed, wvb[...]).astype(BF)
    rows, cols = iota((512, 512), 0), iota((512, 512), 1)
    pq[...] = one_hot(cols == rows % 32 * 16 + rows // 32).astype(BF)
    rows, cols = iota((256, 256), 0), iota((256, 256), 1)
    po[...] = one_hot(cols == rows % 8 * 32 + rows // 8).astype(BF)
    r, c = iota((128, 128), 0), iota((128, 128), 1)
    fold = one_hot(c == r % 8 * 16 + r // 16 * 2 + r % 16 // 8).astype(BF)
    eye = r == c
    eye32 = iota((32, 32), 0) == iota((32, 32), 1)
    bias = jnp.sum(jnp.where(eye32, jnp.broadcast_to(hb[...], (32, 32)), 0.0), axis=1, keepdims=True)
    tri = one_hot(iota((BLK, BLK), 0) >= iota((BLK, BLK), 1)).astype(BF)

    pass_on(wqb.at[:, :, :, near], s_wq, 0)
    pass_on(wqb.at[:, :, :, far], s_wq2, 5)
    take(xa.at[pl.ds(0, 7)], s_xa.at[1])
    take(wqb.at[:, core, :, near], s_pair.at[0, 1])
    q = dot_nt(xa[:, :, : D // 2].reshape(128, D // 2), wqb[:, :, :, : D // 2].reshape(BLK, D // 2))
    take(wqb.at[:, core, :, far], s_pair.at[5, 1])
    q = q + dot_nt(xa[:, :, D // 2 :].reshape(128, D // 2), wqb[:, :, :, D // 2 :].reshape(BLK, D // 2))
    q = q.astype(BF)
    qs[...] = q.reshape(8, SEQ, BLK)
    qr[:, lanes(place)] = qs[place]
    in_group(lambda p: qs.at[p], qr.at[:, lanes(place)], s_q)

    for k, buf in enumerate((edb, egb, eub)):
        take(buf.at[0], lsem.at[4 + k])
        remote(buf.at[0], buf.at[1], s_ex.at[k], pair).start()

    take(tb.at[pl.ds(0, 7)], s_ts.at[1])
    take(cb.at[pl.ds(0, 7)], s_cb.at[1])
    sent = cb[...].reshape(128, 128)
    spot_row = jnp.sum(jnp.where(eye, jnp.broadcast_to(sent[:, SEQ : SEQ + 1], (128, 128)), 0.0), axis=0, keepdims=True)
    wanted = (r // 16 * 2 + r % 2).astype(F32)
    regroup = jnp.where(c // 16 == r % 16 // 2, one_hot(wanted == jnp.broadcast_to(spot_row, (128, 128))), 0.0)
    regroup_bf = regroup.astype(BF)
    combs = jnp.dot(regroup, sent, precision=HI, preferred_element_type=F32)
    cs[...] = combs.reshape(8, SEQ, 128)
    cd[group] = cs[group]

    def send_comb(k, carry):
        g = (group + k) % 8
        remote(cs.at[g], cd.at[group], s_cd, chip_of(g, place) * 2 + core).start()
        return carry

    lax.fori_loop(1, 8, send_comb, 0)

    over_plane(lambda o: wdp.at[:, lanes((o % 8 // 4 + o // 8) % 2 * 4 + o % 4)], lambda o: wdb.at[chip, core], s_wd)
    own_wd = pltpu.make_async_copy(wdp.at[:, lanes(place)], wdb.at[chip, core], lsem.at[7])
    own_wd.start()

    take(qr.at[:, pl.ds(0, 7 * BLK)], s_q.at[1])
    left = iota((SEQ, 128), 1) < HEAD_DIM
    for t, v in enumerate(from_block_order(tiles_of(qr[...].astype(F32) * HEAD_DIM**-0.5))):
        w = pltpu.roll(v, HEAD_DIM, 1)
        first, second = (v, w) if t < 8 else (w, v)
        keep = left if t < 8 else jnp.logical_not(left)
        qstack[32 * t : 32 * t + 16, :] = jnp.where(keep, first, 0.0).astype(BF)
        qstack[32 * t + 16 : 32 * t + 32, :] = jnp.where(keep, second, 0.0).astype(BF)
    qb[...] = dot(pq[...], qstack[...]).astype(BF).reshape(SEQ, HEADS, 128)
    local[0].wait()
    local[1].wait()

    def score(t):
        for k in range(2):
            sc[t % 2, k] = dot_nt(qb[2 * t + k], kb[2 * t + k]) + bias

    def weigh(t):
        parts = []
        for k in range(2):
            length = clen[2 * t + k]
            for n in range(4):
                v = sc[t % 2, k, :, n * BLK : (n + 1) * BLK]
                live = iota((HEADS, BLK), 1) < length - n * BLK
                rest = jnp.where(live, -(jnp.maximum(v, 0.0) + jnp.log(1.0 + jnp.exp(-jnp.abs(v)))), 0.0)
                parts.extend(split2(rest))
        sums = dot(jnp.concatenate(parts, axis=0), tri)
        for k in range(2):
            length = clen[2 * t + k]
            run = jnp.zeros((HEADS, 1), F32)
            for n in (3, 2, 1, 0):
                at = (k * 4 + n) * 64
                within = sums[at : at + 32] + sums[at + 32 : at + 64]
                live = iota((HEADS, BLK), 1) < length - n * BLK
                v = sc[t % 2, k, :, n * BLK : (n + 1) * BLK]
                wt[t % 2, k, :, n * BLK : (n + 1) * BLK] = jnp.where(live, jnp.exp(v + within + run), 0.0).astype(BF)
                run = run + within[:, 0:1]

    def mix(t):
        for k in range(2):
            ob[2 * t + k] = dot(wt[t % 2, k], vb[2 * t + k]).astype(BF)

    def hand_out(half):
        rows8 = slice(half * 8, half * 8 + 8)
        heads = dot(po[...], ob[rows8].reshape(256, 128))
        left8 = iota((8, 128), 1) < HEAD_DIM
        for t in range(16):
            a = heads[16 * t : 16 * t + 8, :]
            b = heads[16 * t + 8 : 16 * t + 16, :]
            if t < 8:
                joined = jnp.where(left8, a, pltpu.roll(b, HEAD_DIM, 1))
            else:
                joined = jnp.where(left8, pltpu.roll(a, HEAD_DIM, 1), b)
            xc[place, rows8, t * 128 : (t + 1) * 128] = joined.astype(BF)
        part = xc.at[place, pl.ds(half * 8, 8)]
        in_group(lambda p: part, part, s_xc if half == 0 else s_xc2)

    for t in range(10):
        if t < 8:
            score(t)
        if 1 <= t < 9:
            weigh(t - 1)
        if t >= 2:
            mix(t - 2)
        if t == 5:
            hand_out(0)
            pass_on(wob, s_wo, 1)
    hand_out(1)

    take(wob.at[:, core], s_pair.at[1, 1])
    take(xc.at[pl.ds(0, 7), pl.ds(0, 8)], s_xc.at[1])
    take(xc.at[pl.ds(0, 7), pl.ds(0, 8)], s_xc2.at[1])
    proj = dot_nt(xc[...].reshape(128, D), wob[...].reshape(BLK, D)).astype(BF)
    stream = tb[...].reshape(128, BLK).astype(F32) + proj.astype(F32)
    y = (stream * g2b[:, lanes(place)]).astype(BF)
    ys[...] = dot(regroup_bf, y).astype(BF).reshape(8, SEQ, BLK)
    xd[group, :, lanes(place)] = ys[group]
    over_plane(lambda o: ys.at[o // 8], lambda o: xd.at[group, :, lanes(place)], s_y)
    ps[...] = proj.reshape(8, SEQ, BLK)
    pr[:, lanes(place)] = ps[place]
    in_group(lambda p: ps.at[p], pr.at[:, lanes(place)], s_pr)

    pass_on(wgb, s_wg, 2)
    pass_on(wub, s_wu, 3)
    own_wd.wait()
    take(wdb.at[pl.ds(0, 63), core], s_wd.at[1])
    remote(wdb.at[:, core], wdb.at[:, core], s_pair.at[4], pair).start()
    take(cd.at[pl.ds(0, 7)], s_cd.at[1])
    lane = iota((128, 128), 1)
    comb = cd[...].reshape(128, 128)
    member0 = chip % 8 * 2 + core
    member1 = chip % 8 * 2 + 1 - core
    comb0 = jnp.sum(jnp.where(lane == member0, comb, 0.0), axis=1, keepdims=True)
    comb1 = jnp.sum(jnp.where(lane == member1, comb, 0.0), axis=1, keepdims=True)

    take(zr.at[pl.ds(0, 63)], s_y.at[1])
    rows_in = xd[...].reshape(128, D)
    plain = rows_in.astype(F32) * (1.0 / g2b[...])
    scale = lax.rsqrt(jnp.mean(plain * plain, axis=1, keepdims=True) + EPS)
    take(wgb.at[:, core], s_pair.at[2, 1])
    take(wub.at[:, core], s_pair.at[3, 1])
    gate = dot_nt(rows_in, wgb[...].reshape(BLK, D)) * scale
    upper = dot_nt(rows_in, wub[...].reshape(BLK, D)) * scale
    hidden = gate * jax.nn.sigmoid(gate) * upper
    part = jnp.sum(hidden * hidden, axis=1, keepdims=True)
    part_row = jnp.sum(jnp.where(eye, jnp.broadcast_to(part, (128, 128)), 0.0), axis=0, keepdims=True)
    sq[...] = jnp.broadcast_to(part_row, (8, 128))
    sqr[place] = sq[...]
    in_group(lambda p: sq, sqr.at[place], s_sq)

    for e, comb_e in ((0, comb0), (1, comb1)):
        if e == 1:
            take(edb.at[1], s_ex.at[0, 1])
            take(egb.at[1], s_ex.at[1, 1])
            take(eub.at[1], s_ex.at[2, 1])
        gate_e = dot(rows_in, egb[e]) * scale
        upper_e = dot(rows_in, eub[e]) * scale
        hbuf[:, e * 512 : (e + 1) * 512] = (gate_e * jax.nn.sigmoid(gate_e) * upper_e * comb_e).astype(BF)

    def route(k, carry):
        zf[:, lanes(k)] = dot(hbuf[...], edb[:, :, lanes(k)].reshape(1024, BLK))
        return carry

    lax.fori_loop(0, 8, route, 0, unroll=2)
    take(sqr.at[pl.ds(0, 7)], s_sq.at[1])
    total = jnp.sum(sqr[...], axis=0)[0:1, :]
    total_col = jnp.sum(jnp.where(eye, jnp.broadcast_to(total, (128, 128)), 0.0), axis=1, keepdims=True)
    dense_scale = lax.rsqrt(total_col * (1.0 / D) + EPS)
    dense = (hidden * dense_scale * hgb[:, lanes(place)]).astype(BF)
    take(wdb.at[:, core], s_pair.at[4, 1])

    def produce(k, carry):
        down = dot_nt(dense, wdb[pl.ds(k * 8, 8)].reshape(BLK, BLK))
        z = zf[:, lanes(k)] + jax.nn.sigmoid(bl[:, lanes(k)]) * down
        zb[k] = z.astype(BF).reshape(8, SEQ, BLK)
        return carry

    lax.fori_loop(0, 8, produce, 0, unroll=2)

    def give(k, carry):
        g = (group + k) % 8
        zs[g] = dot(fold, zb[:, g].reshape(128, BLK)).astype(BF).reshape(8, SEQ, BLK)

        def send(j, carry):
            p = (place + j) % 8
            remote(zs.at[g, p], zr.at[chip], s_z, chip_of(g, p) * 2 + core).start()
            return carry

        @pl.when(g == group)
        def _():
            zr[chip] = zs[g, place]

        @pl.when(g != group)
        def _():
            send(0, 0)

        lax.fori_loop(1, 8, send, 0)
        return carry

    lax.fori_loop(0, 8, give, 0)

    spots = dot_nt(one_hot(iota((128, SEQ), 0) % 16 == iota((128, SEQ), 1)), order)
    unfold = dot(spots, one_hot(iota((SEQ, 128), 1) // 8 == iota((SEQ, 128), 0)))
    unfold = jnp.where(r // 16 == c % 8, unfold, 0.0).astype(BF)
    take(pr.at[:, pl.ds(0, 7 * BLK)], s_pr.at[1])
    second = from_block_order(tiles_of(pr[...].astype(F32)))
    take(zr.at[pl.ds(0, 63)], s_z.at[1])
    sums = jnp.sum(zr[...].reshape(8, 8, SEQ, BLK).astype(F32), axis=1).reshape(128, BLK)
    high, low = split2(sums)
    branch = dot(unfold, high) + dot(unfold, low)
    for k in range(8):
        s = slice(k * BLK, (k + 1) * BLK)
        own = tok[:, s].astype(F32) + jnp.concatenate(second[2 * k : 2 * k + 2], axis=1)
        out[:, s] = (own + branch[k * 16 : k * 16 + 16]).astype(BF)

    take(wqb.at[pl.ds(0, 7), core, :, near], s_wq.at[0])
    take(wqb.at[pl.ds(0, 7), core, :, far], s_wq2.at[0])
    take(wob.at[pl.ds(0, 7), core], s_wo.at[0])
    take(wgb.at[pl.ds(0, 7), core], s_wg.at[0])
    take(wub.at[pl.ds(0, 7), core], s_wu.at[0])
    take(wdb.at[pl.ds(0, 63), core], s_wd.at[0])
    for k, buf in enumerate((wqb.at[:, :, :, near], wob, wgb, wub, wdb, wqb.at[:, :, :, far])):
        take(buf.at[:, core], s_pair.at[k, 0])
    take(edb.at[1], s_ex.at[0, 0])
    take(egb.at[1], s_ex.at[1, 0])
    take(eub.at[1], s_ex.at[2, 0])
    take(xa.at[pl.ds(0, 7)], s_xa.at[0])
    take(xc.at[pl.ds(0, 7), pl.ds(0, 8)], s_xc.at[0])
    take(xc.at[pl.ds(0, 7), pl.ds(0, 8)], s_xc2.at[0])
    take(tb.at[pl.ds(0, 7)], s_ts.at[0])
    take(cb.at[pl.ds(0, 7)], s_cb.at[0])
    take(cd.at[pl.ds(0, 7)], s_cd.at[0])
    take(qr.at[:, pl.ds(0, 7 * BLK)], s_q.at[0])
    take(pr.at[:, pl.ds(0, 7 * BLK)], s_pr.at[0])
    take(zr.at[pl.ds(0, 63)], s_y.at[0])
    take(sqr.at[pl.ds(0, 7)], s_sq.at[0])
    take(zr.at[pl.ds(0, 63)], s_z.at[0])


def shards(
    tokens, cache_keys, cache_values, cache_len, norm_gain_first, w_query, w_key, w_value, head_bias,
    w_output, norm_gain_second, group_id, member, group_gate, member_weight, expert_gate_w, expert_up_w,
    expert_down_w, dense_gate_w, dense_up_w, hidden_gain, dense_down_w, branch_logit,
):
    vmem = pl.BlockSpec(memory_space=pltpu.VMEM)
    hbm = pl.BlockSpec(memory_space=pl.ANY)
    smem = pl.BlockSpec(memory_space=pltpu.SMEM)
    V = pltpu.VMEM
    strips = (8, 2, SEQ, D)
    pair_sem = pltpu.SemaphoreType.DMA((2,))
    args = (
        (tokens, vmem),
        (cache_keys, hbm),
        (cache_values, hbm),
        (cache_len, smem),
        (norm_gain_first.reshape(1, D), vmem),
        (w_query.T, vmem),
        (w_key, hbm),
        (w_value, hbm),
        (head_bias.reshape(1, HEADS), vmem),
        (w_output.T, vmem),
        (norm_gain_second.reshape(1, D), vmem),
        (group_id.reshape(1, SEQ), vmem),
        (member.T, vmem),
        (group_gate.reshape(1, SEQ), vmem),
        (member_weight.T, vmem),
        (expert_gate_w, hbm),
        (expert_up_w, hbm),
        (expert_down_w, hbm),
        (dense_gate_w.T, vmem),
        (dense_up_w.T, vmem),
        (hidden_gain.reshape(1, D), vmem),
        (dense_down_w.T, vmem),
        (branch_logit.reshape(1, D), vmem),
    )
    scratch = [
        V((SEQ, CACHE, 128), BF),
        V((SEQ, CACHE, 128), BF),
        V((2, D, 512), BF),
        V((2, D, 512), BF),
        V((2, 512, D), BF),
        V((D, 128), BF),
        V((D, 128), BF),
        V(strips, BF),
        V(strips, BF),
        V(strips, BF),
        V(strips, BF),
        V((64, 2, SEQ, BLK), BF),
        V((8, SEQ, D), BF),
        V((8, SEQ, D), BF),
        V((8, SEQ, D), BF),
        V((8, SEQ, BLK), BF),
        V((SEQ, D), BF),
        V((8, SEQ, BLK), BF),
        V((8, SEQ, BLK), BF),
        V((SEQ, 128), F32),
        V((8, SEQ, 128), F32),
        V((8, SEQ, 128), F32),
        V((8, SEQ, 128), F32),
        V((512, 512), BF),
        V((256, 256), BF),
        V((512, 128), BF),
        V((SEQ, HEADS, 128), BF),
        V((SEQ, HEADS, 128), BF),
        V((8, SEQ, BLK), BF),
        V((SEQ, D), BF),
        V((8, SEQ, BLK), BF),
        V((8, 128), F32),
        V((8, 8, 128), F32),
        V((8, 8, SEQ, BLK), BF),
        V((8, 8, SEQ, BLK), BF),
        V((64, SEQ, BLK), BF),
        V((128, 1024), BF),
        V((128, D), F32),
        V((2, 2, HEADS, CACHE), F32),
        V((2, 2, HEADS, CACHE), BF),
        V((1, D), F32),
        V((1, D), F32),
        V((SEQ, D), BF),
        V((SEQ, D), BF),
        V((SEQ, D), BF),
        pltpu.SemaphoreType.DMA((8,)),
        pair_sem,
        pair_sem,
        pair_sem,
        pair_sem,
        pair_sem,
        pltpu.SemaphoreType.DMA((6, 2)),
        pltpu.SemaphoreType.DMA((3, 2)),
    ] + [pair_sem] * 12
    return pl.pallas_call(
        kernel,
        out_shape=(
            jax.ShapeDtypeStruct((SEQ, D), BF),
            jax.ShapeDtypeStruct((SEQ, 128), BF),
            jax.ShapeDtypeStruct((SEQ, 128), BF),
        ),
        in_specs=[spec for _, spec in args],
        out_specs=(vmem, vmem, vmem),
        scratch_shapes=scratch,
        compiler_params=pltpu.CompilerParams(
            collective_id=0, has_side_effects=True, vmem_limit_bytes=62_000_000
        ),
    )(*[a for a, _ in args])


def solution(mesh):
    in_specs = (
        P("ep", None),
        P("ep", None, None),
        P("ep", None, None),
        P("ep"),
        P(),
        P(None, "ep"),
        P(),
        P(),
        P(),
        P(None, "ep"),
        P(),
        P("ep"),
        P("ep", None),
        P("ep"),
        P("ep", None),
        P("ep", None, None),
        P("ep", None, None),
        P("ep", None, None),
        P(None, "ep"),
        P(None, "ep"),
        P(),
        P(None, "ep"),
        P(),
    )
    out_specs = (P("ep", None), P("ep", None), P("ep", None))
    return jax.shard_map(shards, mesh=mesh, in_specs=in_specs, out_specs=out_specs, check_vma=False)
```

```python
import functools

import jax
import jax.numpy as jnp
from jax import lax
from jax.experimental import pallas as pl
from jax.experimental.pallas import tpu as pltpu
from jax.sharding import PartitionSpec as P

D = 2048
HEADS = 32
HEAD_DIM = 64
SEQ = 16
CACHE = 1024
BLK = 256
EPS = 1e-06
F32 = jnp.float32
BF = jnp.bfloat16
MESH = pl.DeviceIdType.MESH
NT = (((1,), (1,)), ((), ()))
HI = lax.Precision.HIGHEST


def iota(shape, dim):
    return lax.broadcasted_iota(jnp.int32, shape, dim)


def one_hot(mask):
    return jnp.where(mask, 1.0, 0.0)


def dot(a, b):
    return jnp.dot(a, b, preferred_element_type=F32)


def dot_nt(a, b):
    return lax.dot_general(a, b, NT, preferred_element_type=F32)


def split2(v):
    high = v.astype(BF)
    return high, (v - high.astype(F32)).astype(BF)


def remote(src, dst, sems, target):
    return pltpu.make_async_remote_copy(
        src_ref=src,
        dst_ref=dst,
        send_sem=sems.at[0],
        recv_sem=sems.at[1],
        device_id=(target,),
        device_id_type=MESH,
    )


def take(ref, sem):
    pltpu.make_async_copy(ref, ref, sem).wait()


def chip_of(g, p):
    return g * 8 + (p // 4 + g) % 2 * 4 + p % 4


def gather_lanes(tiles, pieces):
    quarter = iota(tiles[0].shape, 1) // 32
    made = None
    for at, (tile, piece) in enumerate(pieces):
        shift = (at - piece) * 32 % 128
        v = pltpu.roll(tiles[tile], shift, 1) if shift else tiles[tile]
        made = v if made is None else jnp.where(quarter == at, v, made)
    return made


def tiles_of(v):
    return [v[:, t * 128 : (t + 1) * 128] for t in range(D // 128)]


def to_block_order(tiles):
    made = []
    for t in range(16):
        p, half = t // 2, t % 2
        chips = [chip_of(half * 4 + k, p) for k in range(4)]
        made.append(gather_lanes(tiles, [(c // 4, c % 4) for c in chips]))
    return made


def from_block_order(tiles):
    made = []
    for v in range(16):
        g, yl = v // 2, v % 2
        places = [(yl + g) % 2 * 4 + x for x in range(4)]
        made.append(gather_lanes(tiles, [(p * 2 + g // 4, g % 4) for p in places]))
    return made


def lanes(k):
    return pl.ds(pl.multiple_of(k * BLK, BLK), BLK)


def kernel(
    tok_h, ck, cv, clen_h, g1_h, wq_h, wk, wv, hb_h, wo_h, g2_h, gid_h, mem_h, gg_h, mw_h, eg, eu, ed, wg_h, wu_h, hg_h, wd_h, bl_h,
    out, nk, nv,
    kb, vb, egb, eub, edb, wkb, wvb,
    wqb, wob, wgb, wub, wdb,
    xa, xc, xd, qs, qr, ts, tb, cs0, cb, cs, cd, pq, po, qstack, qb, ob, ps, pr, ys,
    sq, sqr, zb, zs, zr, hbuf, zf, sc, wt, g2b, hgb, wgp, wup, wdp,
    lsem, s_wq, s_wo, s_wg, s_wu, s_wd, s_pair, s_ex, s_xa, s_xc, s_ts, s_cb, s_cd, s_q, s_pr, s_y, s_sq, s_z, s_wq2, s_xc2,
    tok, clen, g1, wq, hb, wo, g2, gid, mem, gg, mw, wg, wu, hg, wd, bl, fsem,
):
    me = lax.axis_index("ep")
    chip = me // 2
    core = me % 2
    group = me // 16
    place = (chip % 8 // 4 + group) % 2 * 4 + chip % 4
    pair = chip * 2 + (1 - core)

    fetch = [
        pltpu.make_async_copy(src, dst, fsem.at[k])
        for k, (src, dst) in enumerate(
            (
                (tok_h, tok), (g1_h, g1), (gid_h, gid), (mem_h, mem), (mw_h, mw), (gg_h, gg), (clen_h, clen), (hb_h, hb),
                (wq_h, wq), (wo_h, wo), (g2_h, g2), (hg_h, hg), (wg_h, wg), (wu_h, wu), (wd_h, wd), (bl_h, bl),
            )
        )
    ]
    local = [
        pltpu.make_async_copy(ck, kb, lsem.at[0]),
        pltpu.make_async_copy(cv, vb, lsem.at[1]),
        pltpu.make_async_copy(wk, wkb, lsem.at[2]),
        pltpu.make_async_copy(wv, wvb, lsem.at[3]),
        pltpu.make_async_copy(ed.at[0], edb.at[0], lsem.at[4]),
    ]

    def load_experts(k, carry):
        src = pl.ds(pl.multiple_of(chip_of(k % 8, k // 8) * 32, 32), 32)
        dst = pl.ds(pl.multiple_of(k * 32, 32), 32)
        pltpu.make_async_copy(eg.at[0, src], egb.at[0, dst], lsem.at[5]).start()
        pltpu.make_async_copy(eu.at[0, src], eub.at[0, dst], lsem.at[6]).start()
        return carry

    barrier = pltpu.get_barrier_semaphore()

    def greet(k, carry):
        mate = chip_of(group, (place + k) % 8) * 2 + core
        counterpart = chip_of((group + k) % 8, place) * 2 + core
        pl.semaphore_signal(barrier, inc=1, device_id=(mate,), device_id_type=MESH)
        pl.semaphore_signal(barrier, inc=1, device_id=(counterpart,), device_id_type=MESH)
        return carry

    for c in fetch:
        c.start()
    pl.semaphore_signal(barrier, inc=1, device_id=(pair,), device_id_type=MESH)
    lax.fori_loop(1, 8, greet, 0, unroll=7)
    for c in local:
        c.start()

    for c in fetch:
        c.wait()
    x = tok[...].astype(F32)
    normed = (x * lax.rsqrt(jnp.mean(x * x, axis=-1, keepdims=True) + EPS) * g1[...]).astype(BF)
    xa[place] = normed
    gids = gid[...]
    hits = one_hot(iota((8, SEQ), 0) == gids)
    before = dot(hits, one_hot(iota((SEQ, SEQ), 0) < iota((SEQ, SEQ), 1)))
    rank = jnp.sum(hits * before, axis=0, keepdims=True).astype(jnp.int32)
    spot = gids * 2 + rank
    order = one_hot(iota((SEQ, SEQ), 0) == spot)
    eye16 = iota((SEQ, SEQ), 0) == iota((SEQ, SEQ), 1)
    share = jnp.zeros((128, SEQ), F32)
    for k in range(6):
        share = share + jnp.where(iota((128, SEQ), 0) == mem[k : k + 1, :], mw[k : k + 1, :], 0.0)
    share = share * gg[...] + jnp.where(iota((128, SEQ), 0) == SEQ, spot.astype(F32), 0.0)
    shared = lax.dot_general(one_hot(eye16), share, NT, precision=HI, preferred_element_type=F32)
    cs0[...] = shared
    cb[place] = shared

    pl.semaphore_wait(barrier, 15)

    def spread_strip(strip, buf, sems):
        slot = buf.at[group, core]

        def send(k, carry):
            g = (group + k) % 8
            remote(strip, slot, sems, chip_of(g, place) * 2 + core).start()
            return carry

        pltpu.make_async_copy(strip, slot, sems.at[1]).start()
        lax.fori_loop(1, 8, send, 0)

    def pass_on(buf, sems, k):
        take(buf.at[:, core], sems.at[1])
        remote(buf.at[:, core], buf.at[:, core], s_pair.at[k], pair).start()

    def in_group(src_of, dst, sems):
        def send(k, carry):
            p = (place + k) % 8
            remote(src_of(p), dst, sems, chip_of(group, p) * 2 + core).start()
            return carry

        lax.fori_loop(1, 8, send, 0)

    def over_plane(src_of, dst_of, sems):
        def send(k, carry):
            other = (chip + k) % 64
            remote(src_of(other), dst_of(other), sems, other * 2 + core).start()
            return carry

        lax.fori_loop(1, 64, send, 0, unroll=7)

    near, far = pl.ds(0, D // 2), pl.ds(D // 2, D // 2)
    spread_strip(wq.at[:, near], wqb.at[:, :, :, near], s_wq)
    spread_strip(wq.at[:, far], wqb.at[:, :, :, far], s_wq2)
    in_group(lambda p: xa.at[place], xa.at[place], s_xa)
    in_group(lambda p: cs0, cb.at[place], s_cb)
    spread_strip(wo, wob, s_wo)

    lax.fori_loop(0, 64, load_experts, 0, unroll=4)
    moved = to_block_order(tiles_of(tok[...].astype(F32)))
    for k in range(8):
        ts[k] = jnp.concatenate(moved[2 * k : 2 * k + 2], axis=1).astype(BF)
    tb[place] = ts[place]
    in_group(lambda p: ts.at[p], tb.at[place], s_ts)
    for src, dst in ((g2, g2b), (hg, hgb), (wg, wgp), (wu, wup), (wd, wdp)):
        for k, tile in enumerate(to_block_order(tiles_of(src[...].astype(F32)))):
            dst[:, k * 128 : (k + 1) * 128] = tile.astype(dst.dtype)
    spread_strip(wgp, wgb, s_wg)
    spread_strip(wup, wub, s_wu)
    local[2].wait()
    local[3].wait()
    nk[...] = dot(normed, wkb[...]).astype(BF)
    nv[...] = dot(normed, wvb[...]).astype(BF)
    rows, cols = iota((512, 512), 0), iota((512, 512), 1)
    pq[...] = one_hot(cols == rows % 32 * 16 + rows // 32).astype(BF)
    rows, cols = iota((256, 256), 0), iota((256, 256), 1)
    po[...] = one_hot(cols == rows % 8 * 32 + rows // 8).astype(BF)
    r, c = iota((128, 128), 0), iota((128, 128), 1)
    fold = one_hot(c == r % 8 * 16 + r // 16 * 2 + r % 16 // 8).astype(BF)
    eye = r == c
    eye32 = iota((32, 32), 0) == iota((32, 32), 1)
    bias = jnp.sum(jnp.where(eye32, jnp.broadcast_to(hb[...], (32, 32)), 0.0), axis=1, keepdims=True)
    tri = one_hot(iota((BLK, BLK), 0) >= iota((BLK, BLK), 1)).astype(BF)

    pass_on(wqb.at[:, :, :, near], s_wq, 0)
    pass_on(wqb.at[:, :, :, far], s_wq2, 5)
    take(xa.at[pl.ds(0, 7)], s_xa.at[1])
    take(wqb.at[:, core, :, near], s_pair.at[0, 1])
    q = dot_nt(xa[:, :, : D // 2].reshape(128, D // 2), wqb[:, :, :, : D // 2].reshape(BLK, D // 2))
    take(wqb.at[:, core, :, far], s_pair.at[5, 1])
    q = q + dot_nt(xa[:, :, D // 2 :].reshape(128, D // 2), wqb[:, :, :, D // 2 :].reshape(BLK, D // 2))
    q = q.astype(BF)
    qs[...] = q.reshape(8, SEQ, BLK)
    qr[:, lanes(place)] = qs[place]
    in_group(lambda p: qs.at[p], qr.at[:, lanes(place)], s_q)

    for k, buf in enumerate((edb, egb, eub)):
        take(buf.at[0], lsem.at[4 + k])
        remote(buf.at[0], buf.at[1], s_ex.at[k], pair).start()

    take(tb.at[pl.ds(0, 7)], s_ts.at[1])
    take(cb.at[pl.ds(0, 7)], s_cb.at[1])
    sent = cb[...].reshape(128, 128)
    spot_row = jnp.sum(jnp.where(eye, jnp.broadcast_to(sent[:, SEQ : SEQ + 1], (128, 128)), 0.0), axis=0, keepdims=True)
    wanted = (r // 16 * 2 + r % 2).astype(F32)
    regroup = jnp.where(c // 16 == r % 16 // 2, one_hot(wanted == jnp.broadcast_to(spot_row, (128, 128))), 0.0)
    regroup_bf = regroup.astype(BF)
    combs = jnp.dot(regroup, sent, precision=HI, preferred_element_type=F32)
    cs[...] = combs.reshape(8, SEQ, 128)
    cd[group] = cs[group]

    def send_comb(k, carry):
        g = (group + k) % 8
        remote(cs.at[g], cd.at[group], s_cd, chip_of(g, place) * 2 + core).start()
        return carry

    lax.fori_loop(1, 8, send_comb, 0)

    over_plane(lambda o: wdp.at[:, lanes((o % 8 // 4 + o // 8) % 2 * 4 + o % 4)], lambda o: wdb.at[chip, core], s_wd)
    own_wd = pltpu.make_async_copy(wdp.at[:, lanes(place)], wdb.at[chip, core], lsem.at[7])
    own_wd.start()

    take(qr.at[:, pl.ds(0, 7 * BLK)], s_q.at[1])
    left = iota((SEQ, 128), 1) < HEAD_DIM
    for t, v in enumerate(from_block_order(tiles_of(qr[...].astype(F32) * HEAD_DIM**-0.5))):
        w = pltpu.roll(v, HEAD_DIM, 1)
        first, second = (v, w) if t < 8 else (w, v)
        keep = left if t < 8 else jnp.logical_not(left)
        qstack[32 * t : 32 * t + 16, :] = jnp.where(keep, first, 0.0).astype(BF)
        qstack[32 * t + 16 : 32 * t + 32, :] = jnp.where(keep, second, 0.0).astype(BF)
    qb[...] = dot(pq[...], qstack[...]).astype(BF).reshape(SEQ, HEADS, 128)
    local[0].wait()
    local[1].wait()

    def score(t):
        for k in range(2):
            sc[t % 2, k] = dot_nt(qb[2 * t + k], kb[2 * t + k]) + bias

    def weigh(t):
        parts = []
        for k in range(2):
            length = clen[2 * t + k]
            for n in range(4):
                v = sc[t % 2, k, :, n * BLK : (n + 1) * BLK]
                live = iota((HEADS, BLK), 1) < length - n * BLK
                rest = jnp.where(live, -(jnp.maximum(v, 0.0) + jnp.log(1.0 + jnp.exp(-jnp.abs(v)))), 0.0)
                parts.extend(split2(rest))
        sums = dot(jnp.concatenate(parts, axis=0), tri)
        for k in range(2):
            length = clen[2 * t + k]
            run = jnp.zeros((HEADS, 1), F32)
            for n in (3, 2, 1, 0):
                at = (k * 4 + n) * 64
                within = sums[at : at + 32] + sums[at + 32 : at + 64]
                live = iota((HEADS, BLK), 1) < length - n * BLK
                v = sc[t % 2, k, :, n * BLK : (n + 1) * BLK]
                wt[t % 2, k, :, n * BLK : (n + 1) * BLK] = jnp.where(live, jnp.exp(v + within + run), 0.0).astype(BF)
                run = run + within[:, 0:1]

    def mix(t):
        for k in range(2):
            ob[2 * t + k] = dot(wt[t % 2, k], vb[2 * t + k]).astype(BF)

    def hand_out(half):
        rows8 = slice(half * 8, half * 8 + 8)
        heads = dot(po[...], ob[rows8].reshape(256, 128))
        left8 = iota((8, 128), 1) < HEAD_DIM
        for t in range(16):
            a = heads[16 * t : 16 * t + 8, :]
            b = heads[16 * t + 8 : 16 * t + 16, :]
            if t < 8:
                joined = jnp.where(left8, a, pltpu.roll(b, HEAD_DIM, 1))
            else:
                joined = jnp.where(left8, pltpu.roll(a, HEAD_DIM, 1), b)
            xc[place, rows8, t * 128 : (t + 1) * 128] = joined.astype(BF)
        part = xc.at[place, pl.ds(half * 8, 8)]
        in_group(lambda p: part, part, s_xc if half == 0 else s_xc2)

    for t in range(10):
        if t < 8:
            score(t)
        if 1 <= t < 9:
            weigh(t - 1)
        if t >= 2:
            mix(t - 2)
        if t == 5:
            hand_out(0)
            pass_on(wob, s_wo, 1)
    hand_out(1)

    take(wob.at[:, core], s_pair.at[1, 1])
    take(xc.at[pl.ds(0, 7), pl.ds(0, 8)], s_xc.at[1])
    take(xc.at[pl.ds(0, 7), pl.ds(0, 8)], s_xc2.at[1])
    proj = dot_nt(xc[...].reshape(128, D), wob[...].reshape(BLK, D)).astype(BF)
    stream = tb[...].reshape(128, BLK).astype(F32) + proj.astype(F32)
    y = (stream * g2b[:, lanes(place)]).astype(BF)
    ys[...] = dot(regroup_bf, y).astype(BF).reshape(8, SEQ, BLK)
    xd[group, :, lanes(place)] = ys[group]
    over_plane(lambda o: ys.at[o // 8], lambda o: xd.at[group, :, lanes(place)], s_y)
    ps[...] = proj.reshape(8, SEQ, BLK)
    pr[:, lanes(place)] = ps[place]
    in_group(lambda p: ps.at[p], pr.at[:, lanes(place)], s_pr)

    pass_on(wgb, s_wg, 2)
    pass_on(wub, s_wu, 3)
    own_wd.wait()
    take(wdb.at[pl.ds(0, 63), core], s_wd.at[1])
    remote(wdb.at[:, core], wdb.at[:, core], s_pair.at[4], pair).start()
    take(cd.at[pl.ds(0, 7)], s_cd.at[1])
    lane = iota((128, 128), 1)
    comb = cd[...].reshape(128, 128)
    member0 = chip % 8 * 2 + core
    member1 = chip % 8 * 2 + 1 - core
    comb0 = jnp.sum(jnp.where(lane == member0, comb, 0.0), axis=1, keepdims=True)
    comb1 = jnp.sum(jnp.where(lane == member1, comb, 0.0), axis=1, keepdims=True)

    take(zr.at[pl.ds(0, 63)], s_y.at[1])
    rows_in = xd[...].reshape(128, D)
    plain = rows_in.astype(F32) * (1.0 / g2b[...])
    scale = lax.rsqrt(jnp.mean(plain * plain, axis=1, keepdims=True) + EPS)
    take(wgb.at[:, core], s_pair.at[2, 1])
    take(wub.at[:, core], s_pair.at[3, 1])
    gate = dot_nt(rows_in, wgb[...].reshape(BLK, D)) * scale
    upper = dot_nt(rows_in, wub[...].reshape(BLK, D)) * scale
    hidden = gate * jax.nn.sigmoid(gate) * upper
    part = jnp.sum(hidden * hidden, axis=1, keepdims=True)
    part_row = jnp.sum(jnp.where(eye, jnp.broadcast_to(part, (128, 128)), 0.0), axis=0, keepdims=True)
    sq[...] = jnp.broadcast_to(part_row, (8, 128))
    sqr[place] = sq[...]
    in_group(lambda p: sq, sqr.at[place], s_sq)

    for e, comb_e in ((0, comb0), (1, comb1)):
        if e == 1:
            take(edb.at[1], s_ex.at[0, 1])
            take(egb.at[1], s_ex.at[1, 1])
            take(eub.at[1], s_ex.at[2, 1])
        gate_e = dot(rows_in, egb[e]) * scale
        upper_e = dot(rows_in, eub[e]) * scale
        hbuf[:, e * 512 : (e + 1) * 512] = (gate_e * jax.nn.sigmoid(gate_e) * upper_e * comb_e).astype(BF)

    def route(k, carry):
        zf[:, lanes(k)] = dot(hbuf[...], edb[:, :, lanes(k)].reshape(1024, BLK))
        return carry

    lax.fori_loop(0, 8, route, 0, unroll=2)
    take(sqr.at[pl.ds(0, 7)], s_sq.at[1])
    total = jnp.sum(sqr[...], axis=0)[0:1, :]
    total_col = jnp.sum(jnp.where(eye, jnp.broadcast_to(total, (128, 128)), 0.0), axis=1, keepdims=True)
    dense_scale = lax.rsqrt(total_col * (1.0 / D) + EPS)
    dense = (hidden * dense_scale * hgb[:, lanes(place)]).astype(BF)
    take(wdb.at[:, core], s_pair.at[4, 1])

    def produce(k, carry):
        down = dot_nt(dense, wdb[pl.ds(k * 8, 8)].reshape(BLK, BLK))
        z = zf[:, lanes(k)] + jax.nn.sigmoid(bl[:, lanes(k)]) * down
        zb[k] = z.astype(BF).reshape(8, SEQ, BLK)
        return carry

    lax.fori_loop(0, 8, produce, 0, unroll=2)

    def give(k, carry):
        g = (group + k) % 8
        zs[g] = dot(fold, zb[:, g].reshape(128, BLK)).astype(BF).reshape(8, SEQ, BLK)

        def send(j, carry):
            p = (place + j) % 8
            remote(zs.at[g, p], zr.at[chip], s_z, chip_of(g, p) * 2 + core).start()
            return carry

        @pl.when(g == group)
        def _():
            zr[chip] = zs[g, place]

        @pl.when(g != group)
        def _():
            send(0, 0)

        lax.fori_loop(1, 8, send, 0)
        return carry

    lax.fori_loop(0, 8, give, 0)

    spots = dot_nt(one_hot(iota((128, SEQ), 0) % 16 == iota((128, SEQ), 1)), order)
    unfold = dot(spots, one_hot(iota((SEQ, 128), 1) // 8 == iota((SEQ, 128), 0)))
    unfold = jnp.where(r // 16 == c % 8, unfold, 0.0).astype(BF)
    take(pr.at[:, pl.ds(0, 7 * BLK)], s_pr.at[1])
    second = from_block_order(tiles_of(pr[...].astype(F32)))
    take(zr.at[pl.ds(0, 63)], s_z.at[1])
    sums = jnp.sum(zr[...].reshape(8, 8, SEQ, BLK).astype(F32), axis=1).reshape(128, BLK)
    high, low = split2(sums)
    branch = dot(unfold, high) + dot(unfold, low)
    for k in range(8):
        s = slice(k * BLK, (k + 1) * BLK)
        own = tok[:, s].astype(F32) + jnp.concatenate(second[2 * k : 2 * k + 2], axis=1)
        out[:, s] = (own + branch[k * 16 : k * 16 + 16]).astype(BF)

    take(wqb.at[pl.ds(0, 7), core, :, near], s_wq.at[0])
    take(wqb.at[pl.ds(0, 7), core, :, far], s_wq2.at[0])
    take(wob.at[pl.ds(0, 7), core], s_wo.at[0])
    take(wgb.at[pl.ds(0, 7), core], s_wg.at[0])
    take(wub.at[pl.ds(0, 7), core], s_wu.at[0])
    take(wdb.at[pl.ds(0, 63), core], s_wd.at[0])
    for k, buf in enumerate((wqb.at[:, :, :, near], wob, wgb, wub, wdb, wqb.at[:, :, :, far])):
        take(buf.at[:, core], s_pair.at[k, 0])
    take(edb.at[1], s_ex.at[0, 0])
    take(egb.at[1], s_ex.at[1, 0])
    take(eub.at[1], s_ex.at[2, 0])
    take(xa.at[pl.ds(0, 7)], s_xa.at[0])
    take(xc.at[pl.ds(0, 7), pl.ds(0, 8)], s_xc.at[0])
    take(xc.at[pl.ds(0, 7), pl.ds(0, 8)], s_xc2.at[0])
    take(tb.at[pl.ds(0, 7)], s_ts.at[0])
    take(cb.at[pl.ds(0, 7)], s_cb.at[0])
    take(cd.at[pl.ds(0, 7)], s_cd.at[0])
    take(qr.at[:, pl.ds(0, 7 * BLK)], s_q.at[0])
    take(pr.at[:, pl.ds(0, 7 * BLK)], s_pr.at[0])
    take(zr.at[pl.ds(0, 63)], s_y.at[0])
    take(sqr.at[pl.ds(0, 7)], s_sq.at[0])
    take(zr.at[pl.ds(0, 63)], s_z.at[0])


def write_out(a, b, c, a_out, b_out, c_out, sems):
    copies = [pltpu.make_async_copy(src, dst, sems.at[k]) for k, (src, dst) in enumerate(((a, a_out), (b, b_out), (c, c_out)))]
    for x in copies:
        x.start()
    for x in copies:
        x.wait()


def shards(
    tokens, cache_keys, cache_values, cache_len, norm_gain_first, w_query, w_key, w_value, head_bias,
    w_output, norm_gain_second, group_id, member, group_gate, member_weight, expert_gate_w, expert_up_w,
    expert_down_w, dense_gate_w, dense_up_w, hidden_gain, dense_down_w, branch_logit,
):
    vmem = pl.BlockSpec(memory_space=pltpu.VMEM)
    hbm = pl.BlockSpec(memory_space=pl.ANY)
    V = pltpu.VMEM
    strips = (8, 2, SEQ, D)
    pair_sem = pltpu.SemaphoreType.DMA((2,))
    args = (
        (tokens, hbm),
        (cache_keys, hbm),
        (cache_values, hbm),
        (cache_len, hbm),
        (norm_gain_first.reshape(1, D), hbm),
        (w_query.T, hbm),
        (w_key, hbm),
        (w_value, hbm),
        (head_bias.reshape(1, HEADS), hbm),
        (w_output.T, hbm),
        (norm_gain_second.reshape(1, D), hbm),
        (group_id.reshape(1, SEQ), hbm),
        (member.T, hbm),
        (group_gate.reshape(1, SEQ), hbm),
        (member_weight.T, hbm),
        (expert_gate_w, hbm),
        (expert_up_w, hbm),
        (expert_down_w, hbm),
        (dense_gate_w.T, hbm),
        (dense_up_w.T, hbm),
        (hidden_gain.reshape(1, D), hbm),
        (dense_down_w.T, hbm),
        (branch_logit.reshape(1, D), hbm),
    )
    scratch = [
        V((SEQ, CACHE, 128), BF),
        V((SEQ, CACHE, 128), BF),
        V((2, D, 512), BF),
        V((2, D, 512), BF),
        V((2, 512, D), BF),
        V((D, 128), BF),
        V((D, 128), BF),
        V(strips, BF),
        V(strips, BF),
        V(strips, BF),
        V(strips, BF),
        V((64, 2, SEQ, BLK), BF),
        V((8, SEQ, D), BF),
        V((8, SEQ, D), BF),
        V((8, SEQ, D), BF),
        V((8, SEQ, BLK), BF),
        V((SEQ, D), BF),
        V((8, SEQ, BLK), BF),
        V((8, SEQ, BLK), BF),
        V((SEQ, 128), F32),
        V((8, SEQ, 128), F32),
        V((8, SEQ, 128), F32),
        V((8, SEQ, 128), F32),
        V((512, 512), BF),
        V((256, 256), BF),
        V((512, 128), BF),
        V((SEQ, HEADS, 128), BF),
        V((SEQ, HEADS, 128), BF),
        V((8, SEQ, BLK), BF),
        V((SEQ, D), BF),
        V((8, SEQ, BLK), BF),
        V((8, 128), F32),
        V((8, 8, 128), F32),
        V((8, 8, SEQ, BLK), BF),
        V((8, 8, SEQ, BLK), BF),
        V((64, SEQ, BLK), BF),
        V((128, 1024), BF),
        V((128, D), F32),
        V((2, 2, HEADS, CACHE), F32),
        V((2, 2, HEADS, CACHE), BF),
        V((1, D), F32),
        V((1, D), F32),
        V((SEQ, D), BF),
        V((SEQ, D), BF),
        V((SEQ, D), BF),
        pltpu.SemaphoreType.DMA((8,)),
        pair_sem,
        pair_sem,
        pair_sem,
        pair_sem,
        pair_sem,
        pltpu.SemaphoreType.DMA((6, 2)),
        pltpu.SemaphoreType.DMA((3, 2)),
    ] + [pair_sem] * 12
    for a, space in (
        (0, V), (3, pltpu.SMEM), (4, V), (5, V), (8, V), (9, V), (10, V), (11, V),
        (12, V), (13, V), (14, V), (18, V), (19, V), (20, V), (21, V), (22, V),
    ):
        scratch.append(space(args[a][0].shape, args[a][0].dtype))
    scratch.append(pltpu.SemaphoreType.DMA((16,)))
    shapes = (
        jax.ShapeDtypeStruct((SEQ, D), BF),
        jax.ShapeDtypeStruct((SEQ, 128), BF),
        jax.ShapeDtypeStruct((SEQ, 128), BF),
    )
    made = pl.pallas_call(
        kernel,
        out_shape=tuple(pltpu.VMEM(x.shape, x.dtype) for x in shapes),
        in_specs=[spec for _, spec in args],
        out_specs=(vmem, vmem, vmem),
        scratch_shapes=scratch,
        compiler_params=pltpu.CompilerParams(
            collective_id=0, has_side_effects=True, vmem_limit_bytes=62_000_000
        ),
    )(*[a for a, _ in args])
    return pl.pallas_call(
        write_out, out_shape=shapes, in_specs=[vmem] * 3, out_specs=(hbm,) * 3,
        scratch_shapes=[pltpu.SemaphoreType.DMA((3,))],
    )(*[pltpu.with_memory_space_constraint(x, pltpu.VMEM) for x in made])


def solution(mesh):
    in_specs = (
        P("ep", None),
        P("ep", None, None),
        P("ep", None, None),
        P("ep"),
        P(),
        P(None, "ep"),
        P(),
        P(),
        P(),
        P(None, "ep"),
        P(),
        P("ep"),
        P("ep", None),
        P("ep"),
        P("ep", None),
        P("ep", None, None),
        P("ep", None, None),
        P("ep", None, None),
        P(None, "ep"),
        P(None, "ep"),
        P(),
        P(None, "ep"),
        P(),
    )
    out_specs = (P("ep", None), P("ep", None), P("ep", None))
    return jax.shard_map(shards, mesh=mesh, in_specs=in_specs, out_specs=out_specs, check_vma=False)
```

```python
import functools

import jax
import jax.numpy as jnp
from jax import lax
from jax.experimental import pallas as pl
from jax.experimental.pallas import tpu as pltpu
from jax.sharding import PartitionSpec as P

D = 2048
HEADS = 32
HEAD_DIM = 64
SEQ = 16
CACHE = 1024
BLK = 256
EPS = 1e-06
F32 = jnp.float32
BF = jnp.bfloat16
MESH = pl.DeviceIdType.MESH
NT = (((1,), (1,)), ((), ()))
HI = lax.Precision.HIGHEST


def iota(shape, dim):
    return lax.broadcasted_iota(jnp.int32, shape, dim)


def one_hot(mask):
    return jnp.where(mask, 1.0, 0.0)


def dot(a, b):
    return jnp.dot(a, b, preferred_element_type=F32)


def dot_nt(a, b):
    return lax.dot_general(a, b, NT, preferred_element_type=F32)


def split2(v):
    high = v.astype(BF)
    return high, (v - high.astype(F32)).astype(BF)


def remote(src, dst, sems, target):
    return pltpu.make_async_remote_copy(
        src_ref=src,
        dst_ref=dst,
        send_sem=sems.at[0],
        recv_sem=sems.at[1],
        device_id=(target,),
        device_id_type=MESH,
    )


def take(ref, sem):
    pltpu.make_async_copy(ref, ref, sem).wait()


def chip_of(g, p):
    return g * 8 + (p // 4 + g) % 2 * 4 + p % 4


def gather_lanes(tiles, pieces):
    quarter = iota(tiles[0].shape, 1) // 32
    made = None
    for at, (tile, piece) in enumerate(pieces):
        shift = (at - piece) * 32 % 128
        v = pltpu.roll(tiles[tile], shift, 1) if shift else tiles[tile]
        made = v if made is None else jnp.where(quarter == at, v, made)
    return made


def tiles_of(v):
    return [v[:, t * 128 : (t + 1) * 128] for t in range(D // 128)]


def to_block_order(tiles):
    made = []
    for t in range(16):
        p, half = t // 2, t % 2
        chips = [chip_of(half * 4 + k, p) for k in range(4)]
        made.append(gather_lanes(tiles, [(c // 4, c % 4) for c in chips]))
    return made


def from_block_order(tiles):
    made = []
    for v in range(16):
        g, yl = v // 2, v % 2
        places = [(yl + g) % 2 * 4 + x for x in range(4)]
        made.append(gather_lanes(tiles, [(p * 2 + g // 4, g % 4) for p in places]))
    return made


def lanes(k):
    return pl.ds(pl.multiple_of(k * BLK, BLK), BLK)


def kernel(
    tok_h, ck, cv, clen_h, g1_h, wq_h, wk, wv, hb_h, wo_h, g2_h, gid_h, mem_h, gg_h, mw_h, eg, eu, ed, wg_h, wu_h, hg_h, wd_h, bl_h,
    out, nk, nv,
    kb, vb, egb, eub, edb, wkb, wvb,
    wqb, wob, wgb, wub, wdb,
    xa, xc, xd, qs, qr, ts, tb, cs0, cb, cs, cd, pq, po, qstack, qb, ob, ps, pr, ys,
    sq, sqr, zb, zs, zr, hbuf, zf, zd, wot, sc, wt, g2b, hgb, wgp, wup, wdp,
    lsem, s_wq, s_wo, s_wg, s_wu, s_wd, s_pair, s_ex, s_xa, s_xc, s_ts, s_cb, s_cd, s_q, s_pr, s_y, s_sq, s_z, s_wq2, s_xc2,
    tok, clen, g1, wq, hb, wo, g2, gid, mem, gg, mw, wg, wu, hg, wd, bl, fsem,
):
    me = lax.axis_index("ep")
    chip = me // 2
    core = me % 2
    group = me // 16
    place = (chip % 8 // 4 + group) % 2 * 4 + chip % 4
    pair = chip * 2 + (1 - core)

    fetch = [
        pltpu.make_async_copy(src, dst, fsem.at[k])
        for k, (src, dst) in enumerate(
            (
                (tok_h, tok), (g1_h, g1), (gid_h, gid), (mem_h, mem), (mw_h, mw), (gg_h, gg), (clen_h, clen), (hb_h, hb),
                (wq_h, wq), (wo_h, wo), (g2_h, g2), (hg_h, hg), (wg_h, wg), (wu_h, wu), (wd_h, wd), (bl_h, bl),
            )
        )
    ]
    local = [
        pltpu.make_async_copy(ck, kb, lsem.at[0]),
        pltpu.make_async_copy(cv, vb, lsem.at[1]),
        pltpu.make_async_copy(wk, wkb, lsem.at[2]),
        pltpu.make_async_copy(wv, wvb, lsem.at[3]),
        pltpu.make_async_copy(ed.at[0], edb.at[0], lsem.at[4]),
    ]

    def load_experts(k, carry):
        src = pl.ds(pl.multiple_of(chip_of(k % 8, k // 8) * 32, 32), 32)
        dst = pl.ds(pl.multiple_of(k * 32, 32), 32)
        pltpu.make_async_copy(eg.at[0, src], egb.at[0, dst], lsem.at[5]).start()
        pltpu.make_async_copy(eu.at[0, src], eub.at[0, dst], lsem.at[6]).start()
        return carry

    barrier = pltpu.get_barrier_semaphore()

    def greet(k, carry):
        mate = chip_of(group, (place + k) % 8) * 2 + core
        counterpart = chip_of((group + k) % 8, place) * 2 + core
        pl.semaphore_signal(barrier, inc=1, device_id=(mate,), device_id_type=MESH)
        pl.semaphore_signal(barrier, inc=1, device_id=(counterpart,), device_id_type=MESH)
        return carry

    for c in fetch:
        c.start()
    pl.semaphore_signal(barrier, inc=1, device_id=(pair,), device_id_type=MESH)
    lax.fori_loop(1, 8, greet, 0, unroll=7)
    for c in local:
        c.start()

    for c in fetch:
        c.wait()
    x = tok[...].astype(F32)
    normed = (x * lax.rsqrt(jnp.mean(x * x, axis=-1, keepdims=True) + EPS) * g1[...]).astype(BF)
    xa[place] = normed
    gids = gid[...]
    hits = one_hot(iota((8, SEQ), 0) == gids)
    before = dot(hits, one_hot(iota((SEQ, SEQ), 0) < iota((SEQ, SEQ), 1)))
    rank = jnp.sum(hits * before, axis=0, keepdims=True).astype(jnp.int32)
    spot = gids * 2 + rank
    order = one_hot(iota((SEQ, SEQ), 0) == spot)
    eye16 = iota((SEQ, SEQ), 0) == iota((SEQ, SEQ), 1)
    share = jnp.zeros((128, SEQ), F32)
    for k in range(6):
        share = share + jnp.where(iota((128, SEQ), 0) == mem[k : k + 1, :], mw[k : k + 1, :], 0.0)
    share = share * gg[...] + jnp.where(iota((128, SEQ), 0) == SEQ, spot.astype(F32), 0.0)
    shared = lax.dot_general(one_hot(eye16), share, NT, precision=HI, preferred_element_type=F32)
    cs0[...] = shared
    cb[place] = shared

    pl.semaphore_wait(barrier, 15)

    near, far = pl.ds(0, D // 2), pl.ds(D // 2, D // 2)

    def spread_strip(strip, buf, sems):
        slot = buf.at[group, core]

        def send(k, carry):
            g = (group + k) % 8
            remote(strip, slot, sems, chip_of(g, place) * 2 + core).start()
            return carry

        pltpu.make_async_copy(strip, slot, sems.at[1]).start()
        lax.fori_loop(1, 8, send, 0)

    def pass_on(buf, sems, k):
        take(buf.at[:, core], sems.at[1])
        remote(buf.at[:, core], buf.at[:, core], s_pair.at[k], pair).start()

    depth, side = group // 2, group % 2
    mirror = chip_of(group + 1 - 2 * side, place) * 2 + core

    def along_z(src, dst, sem):
        def send(k, carry):
            remote(src, dst, sem, chip_of((depth + k) % 4 * 2 + side, place) * 2 + core).start()
            return carry

        lax.fori_loop(1, 4, send, 0)

    def plant(strip, buf, sems):
        slot = buf.at[depth, side, core]
        pltpu.make_async_copy(strip, slot, sems.at[5, 1]).start()
        along_z(strip.at[:, near], slot.at[:, near], sems.at[0])
        remote(strip.at[:, far], slot.at[:, far], sems.at[1], mirror).start()
        along_z(strip.at[:, far], slot.at[:, far], sems.at[2])

    def relay(buf, sems):
        take(buf.at[0, 0, core], sems.at[5, 1])
        take(buf.at[0, 0, core, :, far], sems.at[1, 1])
        ahead = buf.at[depth, 1 - side, core, :, far]
        along_z(ahead, ahead, sems.at[3])
        take(buf.at[pl.ds(0, 3), 0, core, :, near], sems.at[0, 1])
        across = buf.at[:, side, core, :, near]
        remote(across, across, sems.at[4], mirror).start()

    def finish(buf, sems, k):
        take(buf.at[pl.ds(0, 3), 0, core, :, far], sems.at[2, 1])
        take(buf.at[pl.ds(0, 3), 0, core, :, far], sems.at[3, 1])
        take(buf.at[:, 0, core, :, near], sems.at[4, 1])
        remote(buf.at[:, :, core], buf.at[:, :, core], s_pair.at[k], pair).start()

    def uproot(buf, sems):
        take(buf.at[pl.ds(0, 3), 0, core, :, near], sems.at[0, 0])
        take(buf.at[0, 0, core, :, far], sems.at[1, 0])
        take(buf.at[pl.ds(0, 3), 0, core, :, far], sems.at[2, 0])
        take(buf.at[pl.ds(0, 3), 0, core, :, far], sems.at[3, 0])
        take(buf.at[:, 0, core, :, near], sems.at[4, 0])

    def in_group(src_of, dst, sems):
        def send(k, carry):
            p = (place + k) % 8
            remote(src_of(p), dst, sems, chip_of(group, p) * 2 + core).start()
            return carry

        lax.fori_loop(1, 8, send, 0)

    def over_plane(src_of, dst_of, sems):
        def send(k, carry):
            other = (chip + k * 27) % 64
            remote(src_of(other), dst_of(other), sems, other * 2 + core).start()
            return carry

        lax.fori_loop(1, 64, send, 0, unroll=7)

    spread_strip(wq.at[:, near], wqb.at[:, :, :, near], s_wq)
    spread_strip(wq.at[:, far], wqb.at[:, :, :, far], s_wq2)
    in_group(lambda p: xa.at[place], xa.at[place], s_xa)
    in_group(lambda p: cs0, cb.at[place], s_cb)

    @pl.when(core == 0)
    def _():
        plant(wo, wob, s_wo)

    lax.fori_loop(0, 64, load_experts, 0, unroll=4)
    moved = to_block_order(tiles_of(tok[...].astype(F32)))
    for k in range(8):
        ts[k] = jnp.concatenate(moved[2 * k : 2 * k + 2], axis=1).astype(BF)
    tb[place] = ts[place]
    in_group(lambda p: ts.at[p], tb.at[place], s_ts)
    for src, dst in ((g2, g2b), (hg, hgb), (wg, wgp), (wu, wup), (wd, wdp)):
        for k, tile in enumerate(to_block_order(tiles_of(src[...].astype(F32)))):
            dst[:, k * 128 : (k + 1) * 128] = tile.astype(dst.dtype)

    @pl.when(core == 0)
    def _():
        plant(wgp, wgb, s_wg)
        plant(wup, wub, s_wu)

    local[2].wait()
    local[3].wait()
    nk[...] = dot(normed, wkb[...]).astype(BF)
    nv[...] = dot(normed, wvb[...]).astype(BF)
    rows, cols = iota((512, 512), 0), iota((512, 512), 1)
    pq[...] = one_hot(cols == rows % 32 * 16 + rows // 32).astype(BF)
    rows, cols = iota((256, 256), 0), iota((256, 256), 1)
    po[...] = one_hot(cols == rows % 8 * 32 + rows // 8).astype(BF)
    r, c = iota((128, 128), 0), iota((128, 128), 1)
    fold = one_hot(c == r % 8 * 16 + r // 16 * 2 + r % 16 // 8).astype(BF)
    eye = r == c
    eye32 = iota((32, 32), 0) == iota((32, 32), 1)
    bias = jnp.sum(jnp.where(eye32, jnp.broadcast_to(hb[...], (32, 32)), 0.0), axis=1, keepdims=True)
    tri = one_hot(iota((BLK, BLK), 0) >= iota((BLK, BLK), 1)).astype(BF)

    pass_on(wqb.at[:, :, :, near], s_wq, 0)
    pass_on(wqb.at[:, :, :, far], s_wq2, 5)

    @pl.when(core == 1)
    def _():
        plant(wo, wob, s_wo)
        plant(wgp, wgb, s_wg)
        plant(wup, wub, s_wu)

    take(xa.at[pl.ds(0, 7)], s_xa.at[1])
    take(wqb.at[:, core, :, near], s_pair.at[0, 1])
    q = dot_nt(xa[:, :, : D // 2].reshape(128, D // 2), wqb[:, :, :, : D // 2].reshape(BLK, D // 2))
    take(wqb.at[:, core, :, far], s_pair.at[5, 1])
    q = q + dot_nt(xa[:, :, D // 2 :].reshape(128, D // 2), wqb[:, :, :, D // 2 :].reshape(BLK, D // 2))
    q = q.astype(BF)
    qs[...] = q.reshape(8, SEQ, BLK)
    qr[:, lanes(place)] = qs[place]
    in_group(lambda p: qs.at[p], qr.at[:, lanes(place)], s_q)

    for k, buf in enumerate((edb, egb, eub)):
        take(buf.at[0], lsem.at[4 + k])
        remote(buf.at[0], buf.at[1], s_ex.at[k], pair).start()

    take(tb.at[pl.ds(0, 7)], s_ts.at[1])
    take(cb.at[pl.ds(0, 7)], s_cb.at[1])
    sent = cb[...].reshape(128, 128)
    spot_row = jnp.sum(jnp.where(eye, jnp.broadcast_to(sent[:, SEQ : SEQ + 1], (128, 128)), 0.0), axis=0, keepdims=True)
    wanted = (r // 16 * 2 + r % 2).astype(F32)
    regroup = jnp.where(c // 16 == r % 16 // 2, one_hot(wanted == jnp.broadcast_to(spot_row, (128, 128))), 0.0)
    regroup_bf = regroup.astype(BF)
    combs = jnp.dot(regroup, sent, precision=HI, preferred_element_type=F32)
    cs[...] = combs.reshape(8, SEQ, 128)
    cd[group] = cs[group]

    def send_comb(k, carry):
        g = (group + k) % 8
        remote(cs.at[g], cd.at[group], s_cd, chip_of(g, place) * 2 + core).start()
        return carry

    lax.fori_loop(1, 8, send_comb, 0)

    relay(wob, s_wo)
    over_plane(lambda o: wdp.at[:, lanes((o % 8 // 4 + o // 8) % 2 * 4 + o % 4)], lambda o: wdb.at[chip, core], s_wd)
    own_wd = pltpu.make_async_copy(wdp.at[:, lanes(place)], wdb.at[chip, core], lsem.at[7])
    own_wd.start()

    take(qr.at[:, pl.ds(0, 7 * BLK)], s_q.at[1])
    left = iota((SEQ, 128), 1) < HEAD_DIM
    for t, v in enumerate(from_block_order(tiles_of(qr[...].astype(F32) * HEAD_DIM**-0.5))):
        w = pltpu.roll(v, HEAD_DIM, 1)
        first, second = (v, w) if t < 8 else (w, v)
        keep = left if t < 8 else jnp.logical_not(left)
        qstack[32 * t : 32 * t + 16, :] = jnp.where(keep, first, 0.0).astype(BF)
        qstack[32 * t + 16 : 32 * t + 32, :] = jnp.where(keep, second, 0.0).astype(BF)
    qb[...] = dot(pq[...], qstack[...]).astype(BF).reshape(SEQ, HEADS, 128)
    local[0].wait()
    local[1].wait()

    def score(t):
        for k in range(2):
            sc[t % 2, k] = dot_nt(qb[2 * t + k], kb[2 * t + k]) + bias

    def weigh(t):
        parts = []
        for k in range(2):
            length = clen[2 * t + k]
            for n in range(4):
                v = sc[t % 2, k, :, n * BLK : (n + 1) * BLK]
                live = iota((HEADS, BLK), 1) < length - n * BLK
                rest = jnp.where(live, -(jnp.maximum(v, 0.0) + jnp.log(1.0 + jnp.exp(-jnp.abs(v)))), 0.0)
                parts.extend(split2(rest))
        sums = dot(jnp.concatenate(parts, axis=0), tri)
        for k in range(2):
            length = clen[2 * t + k]
            run = jnp.zeros((HEADS, 1), F32)
            for n in (3, 2, 1, 0):
                at = (k * 4 + n) * 64
                within = sums[at : at + 32] + sums[at + 32 : at + 64]
                live = iota((HEADS, BLK), 1) < length - n * BLK
                v = sc[t % 2, k, :, n * BLK : (n + 1) * BLK]
                wt[t % 2, k, :, n * BLK : (n + 1) * BLK] = jnp.where(live, jnp.exp(v + within + run), 0.0).astype(BF)
                run = run + within[:, 0:1]

    def mix(t):
        for k in range(2):
            ob[2 * t + k] = dot(wt[t % 2, k], vb[2 * t + k]).astype(BF)

    def hand_out(half):
        rows8 = slice(half * 8, half * 8 + 8)
        heads = dot(po[...], ob[rows8].reshape(256, 128))
        left8 = iota((8, 128), 1) < HEAD_DIM
        for t in range(16):
            a = heads[16 * t : 16 * t + 8, :]
            b = heads[16 * t + 8 : 16 * t + 16, :]
            if t < 8:
                joined = jnp.where(left8, a, pltpu.roll(b, HEAD_DIM, 1))
            else:
                joined = jnp.where(left8, pltpu.roll(a, HEAD_DIM, 1), b)
            xc[place, rows8, t * 128 : (t + 1) * 128] = joined.astype(BF)
        part = xc.at[place, pl.ds(half * 8, 8)]
        in_group(lambda p: part, part, s_xc if half == 0 else s_xc2)

    for t in range(10):
        if t < 8:
            score(t)
        if 1 <= t < 9:
            weigh(t - 1)
        if t >= 2:
            mix(t - 2)
        if t == 5:
            hand_out(0)
    hand_out(1)
    relay(wgb, s_wg)
    finish(wob, s_wo, 1)
    relay(wub, s_wu)

    take(wob.at[:, :, core], s_pair.at[1, 1])
    wot[...] = wob[...].reshape(BLK, D).T
    take(xc.at[pl.ds(0, 7), pl.ds(0, 8)], s_xc.at[1])
    take(xc.at[pl.ds(0, 7), pl.ds(0, 8)], s_xc2.at[1])
    proj = dot(xc[...].reshape(128, D), wot[...]).astype(BF)
    stream = tb[...].reshape(128, BLK).astype(F32) + proj.astype(F32)
    y = (stream * g2b[:, lanes(place)]).astype(BF)
    ys[...] = dot(regroup_bf, y).astype(BF).reshape(8, SEQ, BLK)
    xd[group, :, lanes(place)] = ys[group]
    over_plane(lambda o: ys.at[o // 8], lambda o: xd.at[group, :, lanes(place)], s_y)
    ps[...] = proj.reshape(8, SEQ, BLK)
    pr[:, lanes(place)] = ps[place]
    in_group(lambda p: ps.at[p], pr.at[:, lanes(place)], s_pr)

    finish(wgb, s_wg, 2)
    finish(wub, s_wu, 3)
    own_wd.wait()
    take(wdb.at[pl.ds(0, 63), core], s_wd.at[1])
    remote(wdb.at[:, core], wdb.at[:, core], s_pair.at[4], pair).start()
    take(cd.at[pl.ds(0, 7)], s_cd.at[1])
    lane = iota((128, 128), 1)
    comb = cd[...].reshape(128, 128)
    member0 = chip % 8 * 2 + core
    member1 = chip % 8 * 2 + 1 - core
    comb0 = jnp.sum(jnp.where(lane == member0, comb, 0.0), axis=1, keepdims=True)
    comb1 = jnp.sum(jnp.where(lane == member1, comb, 0.0), axis=1, keepdims=True)

    take(zr.at[pl.ds(0, 63)], s_y.at[1])
    rows_in = xd[...].reshape(128, D)
    plain = rows_in.astype(F32) * (1.0 / g2b[...])
    scale = lax.rsqrt(jnp.mean(plain * plain, axis=1, keepdims=True) + EPS)
    take(wgb.at[:, :, core], s_pair.at[2, 1])
    take(wub.at[:, :, core], s_pair.at[3, 1])
    gate = dot_nt(rows_in, wgb[...].reshape(BLK, D)) * scale
    upper = dot_nt(rows_in, wub[...].reshape(BLK, D)) * scale
    hidden = gate * jax.nn.sigmoid(gate) * upper
    part = jnp.sum(hidden * hidden, axis=1, keepdims=True)
    part_row = jnp.sum(jnp.where(eye, jnp.broadcast_to(part, (128, 128)), 0.0), axis=0, keepdims=True)
    sq[...] = jnp.broadcast_to(part_row, (8, 128))
    sqr[place] = sq[...]
    in_group(lambda p: sq, sqr.at[place], s_sq)

    for e, comb_e in ((0, comb0), (1, comb1)):
        if e == 1:
            take(edb.at[1], s_ex.at[0, 1])
            take(egb.at[1], s_ex.at[1, 1])
            take(eub.at[1], s_ex.at[2, 1])
        gate_e = dot(rows_in, egb[e]) * scale
        upper_e = dot(rows_in, eub[e]) * scale
        hbuf[:, e * 512 : (e + 1) * 512] = (gate_e * jax.nn.sigmoid(gate_e) * upper_e * comb_e).astype(BF)

    def route(k, carry):
        zf[:, lanes(k)] = dot(hbuf[...], edb[:, :, lanes(k)].reshape(1024, BLK))
        return carry

    lax.fori_loop(0, 8, route, 0, unroll=2)
    dense = (hidden * hgb[:, lanes(place)]).astype(BF)
    take(wdb.at[:, core], s_pair.at[4, 1])

    def down(k, carry):
        v = dot_nt(dense, wdb[pl.ds(k * 8, 8)].reshape(BLK, BLK))
        zd[:, lanes(k)] = jax.nn.sigmoid(bl[:, lanes(k)]) * v
        return carry

    lax.fori_loop(0, 8, down, 0, unroll=2)
    spots = dot_nt(one_hot(iota((128, SEQ), 0) % 16 == iota((128, SEQ), 1)), order)
    unfold = dot(spots, one_hot(iota((SEQ, 128), 1) // 8 == iota((SEQ, 128), 0)))
    unfold = jnp.where(r // 16 == c % 8, unfold, 0.0).astype(BF)
    take(pr.at[:, pl.ds(0, 7 * BLK)], s_pr.at[1])
    second = from_block_order(tiles_of(pr[...].astype(F32)))
    take(sqr.at[pl.ds(0, 7)], s_sq.at[1])
    total = jnp.sum(sqr[...], axis=0)[0:1, :]
    total_col = jnp.sum(jnp.where(eye, jnp.broadcast_to(total, (128, 128)), 0.0), axis=1, keepdims=True)
    dense_scale = lax.rsqrt(total_col * (1.0 / D) + EPS)

    def produce(k, carry):
        z = zf[:, lanes(k)] + dense_scale * zd[:, lanes(k)]
        zb[k] = z.astype(BF).reshape(8, SEQ, BLK)
        return carry

    lax.fori_loop(0, 8, produce, 0, unroll=2)

    def give(k, carry):
        g = (group + k) % 8
        zs[g] = dot(fold, zb[:, g].reshape(128, BLK)).astype(BF).reshape(8, SEQ, BLK)

        def send(j, carry):
            p = (place + j) % 8
            remote(zs.at[g, p], zr.at[chip], s_z, chip_of(g, p) * 2 + core).start()
            return carry

        @pl.when(g == group)
        def _():
            zr[chip] = zs[g, place]

        @pl.when(g != group)
        def _():
            send(0, 0)

        lax.fori_loop(1, 8, send, 0)
        return carry

    lax.fori_loop(0, 8, give, 0)

    take(zr.at[pl.ds(0, 63)], s_z.at[1])
    sums = jnp.sum(zr[...].reshape(8, 8, SEQ, BLK).astype(F32), axis=1).reshape(128, BLK)
    high, low = split2(sums)
    branch = dot(unfold, high) + dot(unfold, low)
    for k in range(8):
        s = slice(k * BLK, (k + 1) * BLK)
        own = tok[:, s].astype(F32) + jnp.concatenate(second[2 * k : 2 * k + 2], axis=1)
        out[:, s] = (own + branch[k * 16 : k * 16 + 16]).astype(BF)

    take(wqb.at[pl.ds(0, 7), core, :, near], s_wq.at[0])
    take(wqb.at[pl.ds(0, 7), core, :, far], s_wq2.at[0])
    uproot(wob, s_wo)
    uproot(wgb, s_wg)
    uproot(wub, s_wu)
    take(wdb.at[pl.ds(0, 63), core], s_wd.at[0])
    for k, buf in enumerate((wob, wgb, wub)):
        take(buf.at[:, :, core], s_pair.at[k + 1, 0])
    for k, buf in ((0, wqb.at[:, :, :, near]), (4, wdb), (5, wqb.at[:, :, :, far])):
        take(buf.at[:, core], s_pair.at[k, 0])
    take(edb.at[1], s_ex.at[0, 0])
    take(egb.at[1], s_ex.at[1, 0])
    take(eub.at[1], s_ex.at[2, 0])
    take(xa.at[pl.ds(0, 7)], s_xa.at[0])
    take(xc.at[pl.ds(0, 7), pl.ds(0, 8)], s_xc.at[0])
    take(xc.at[pl.ds(0, 7), pl.ds(0, 8)], s_xc2.at[0])
    take(tb.at[pl.ds(0, 7)], s_ts.at[0])
    take(cb.at[pl.ds(0, 7)], s_cb.at[0])
    take(cd.at[pl.ds(0, 7)], s_cd.at[0])
    take(qr.at[:, pl.ds(0, 7 * BLK)], s_q.at[0])
    take(pr.at[:, pl.ds(0, 7 * BLK)], s_pr.at[0])
    take(zr.at[pl.ds(0, 63)], s_y.at[0])
    take(sqr.at[pl.ds(0, 7)], s_sq.at[0])
    take(zr.at[pl.ds(0, 63)], s_z.at[0])


def write_out(a, b, c, a_out, b_out, c_out, sems):
    copies = [pltpu.make_async_copy(src, dst, sems.at[k]) for k, (src, dst) in enumerate(((a, a_out), (b, b_out), (c, c_out)))]
    for x in copies:
        x.start()
    for x in copies:
        x.wait()


def shards(
    tokens, cache_keys, cache_values, cache_len, norm_gain_first, w_query, w_key, w_value, head_bias,
    w_output, norm_gain_second, group_id, member, group_gate, member_weight, expert_gate_w, expert_up_w,
    expert_down_w, dense_gate_w, dense_up_w, hidden_gain, dense_down_w, branch_logit,
):
    vmem = pl.BlockSpec(memory_space=pltpu.VMEM)
    hbm = pl.BlockSpec(memory_space=pl.ANY)
    V = pltpu.VMEM
    strips = (8, 2, SEQ, D)
    pair_sem = pltpu.SemaphoreType.DMA((2,))
    tree_sem = pltpu.SemaphoreType.DMA((6, 2))
    args = (
        (tokens, hbm),
        (cache_keys, hbm),
        (cache_values, hbm),
        (cache_len, hbm),
        (norm_gain_first.reshape(1, D), hbm),
        (w_query.T, hbm),
        (w_key, hbm),
        (w_value, hbm),
        (head_bias.reshape(1, HEADS), hbm),
        (w_output.T, hbm),
        (norm_gain_second.reshape(1, D), hbm),
        (group_id.reshape(1, SEQ), hbm),
        (member.T, hbm),
        (group_gate.reshape(1, SEQ), hbm),
        (member_weight.T, hbm),
        (expert_gate_w, hbm),
        (expert_up_w, hbm),
        (expert_down_w, hbm),
        (dense_gate_w.T, hbm),
        (dense_up_w.T, hbm),
        (hidden_gain.reshape(1, D), hbm),
        (dense_down_w.T, hbm),
        (branch_logit.reshape(1, D), hbm),
    )
    scratch = [
        V((SEQ, CACHE, 128), BF),
        V((SEQ, CACHE, 128), BF),
        V((2, D, 512), BF),
        V((2, D, 512), BF),
        V((2, 512, D), BF),
        V((D, 128), BF),
        V((D, 128), BF),
        V(strips, BF),
        V((4, 2, 2, SEQ, D), BF),
        V((4, 2, 2, SEQ, D), BF),
        V((4, 2, 2, SEQ, D), BF),
        V((64, 2, SEQ, BLK), BF),
        V((8, SEQ, D), BF),
        V((8, SEQ, D), BF),
        V((8, SEQ, D), BF),
        V((8, SEQ, BLK), BF),
        V((SEQ, D), BF),
        V((8, SEQ, BLK), BF),
        V((8, SEQ, BLK), BF),
        V((SEQ, 128), F32),
        V((8, SEQ, 128), F32),
        V((8, SEQ, 128), F32),
        V((8, SEQ, 128), F32),
        V((512, 512), BF),
        V((256, 256), BF),
        V((512, 128), BF),
        V((SEQ, HEADS, 128), BF),
        V((SEQ, HEADS, 128), BF),
        V((8, SEQ, BLK), BF),
        V((SEQ, D), BF),
        V((8, SEQ, BLK), BF),
        V((8, 128), F32),
        V((8, 8, 128), F32),
        V((8, 8, SEQ, BLK), BF),
        V((8, 8, SEQ, BLK), BF),
        V((64, SEQ, BLK), BF),
        V((128, 1024), BF),
        V((128, D), F32),
        V((128, D), F32),
        V((D, BLK), BF),
        V((2, 2, HEADS, CACHE), F32),
        V((2, 2, HEADS, CACHE), BF),
        V((1, D), F32),
        V((1, D), F32),
        V((SEQ, D), BF),
        V((SEQ, D), BF),
        V((SEQ, D), BF),
        pltpu.SemaphoreType.DMA((8,)),
        pair_sem,
        tree_sem,
        tree_sem,
        tree_sem,
        pair_sem,
        pltpu.SemaphoreType.DMA((6, 2)),
        pltpu.SemaphoreType.DMA((3, 2)),
    ] + [pair_sem] * 12
    for a, space in (
        (0, V), (3, pltpu.SMEM), (4, V), (5, V), (8, V), (9, V), (10, V), (11, V),
        (12, V), (13, V), (14, V), (18, V), (19, V), (20, V), (21, V), (22, V),
    ):
        scratch.append(space(args[a][0].shape, args[a][0].dtype))
    scratch.append(pltpu.SemaphoreType.DMA((16,)))
    shapes = (
        jax.ShapeDtypeStruct((SEQ, D), BF),
        jax.ShapeDtypeStruct((SEQ, 128), BF),
        jax.ShapeDtypeStruct((SEQ, 128), BF),
    )
    made = pl.pallas_call(
        kernel,
        out_shape=tuple(pltpu.VMEM(x.shape, x.dtype) for x in shapes),
        in_specs=[spec for _, spec in args],
        out_specs=(vmem, vmem, vmem),
        scratch_shapes=scratch,
        compiler_params=pltpu.CompilerParams(
            collective_id=0, has_side_effects=True, vmem_limit_bytes=62_000_000
        ),
    )(*[a for a, _ in args])
    return pl.pallas_call(
        write_out, out_shape=shapes, in_specs=[vmem] * 3, out_specs=(hbm,) * 3,
        scratch_shapes=[pltpu.SemaphoreType.DMA((3,))],
    )(*[pltpu.with_memory_space_constraint(x, pltpu.VMEM) for x in made])


def solution(mesh):
    in_specs = (
        P("ep", None),
        P("ep", None, None),
        P("ep", None, None),
        P("ep"),
        P(),
        P(None, "ep"),
        P(),
        P(),
        P(),
        P(None, "ep"),
        P(),
        P("ep"),
        P("ep", None),
        P("ep"),
        P("ep", None),
        P("ep", None, None),
        P("ep", None, None),
        P("ep", None, None),
        P(None, "ep"),
        P(None, "ep"),
        P(),
        P(None, "ep"),
        P(),
    )
    out_specs = (P("ep", None), P("ep", None), P("ep", None))
    return jax.shard_map(shards, mesh=mesh, in_specs=in_specs, out_specs=out_specs, check_vma=False)
```

```python
import functools

import jax
import jax.numpy as jnp
from jax import lax
from jax.experimental import pallas as pl
from jax.experimental.pallas import tpu as pltpu
from jax.sharding import PartitionSpec as P

D = 2048
HEADS = 32
HEAD_DIM = 64
SEQ = 16
CACHE = 1024
BLK = 256
EPS = 1e-06
F32 = jnp.float32
BF = jnp.bfloat16
MESH = pl.DeviceIdType.MESH
NT = (((1,), (1,)), ((), ()))
HI = lax.Precision.HIGHEST


def iota(shape, dim):
    return lax.broadcasted_iota(jnp.int32, shape, dim)


def one_hot(mask):
    return jnp.where(mask, 1.0, 0.0)


def dot(a, b):
    return jnp.dot(a, b, preferred_element_type=F32)


def dot_nt(a, b):
    return lax.dot_general(a, b, NT, preferred_element_type=F32)


def split2(v):
    high = v.astype(BF)
    return high, (v - high.astype(F32)).astype(BF)


def remote(src, dst, sems, target):
    return pltpu.make_async_remote_copy(
        src_ref=src,
        dst_ref=dst,
        send_sem=sems.at[0],
        recv_sem=sems.at[1],
        device_id=(target,),
        device_id_type=MESH,
    )


def take(ref, sem):
    pltpu.make_async_copy(ref, ref, sem).wait()


def chip_of(g, p):
    return g * 8 + (p // 4 + g) % 2 * 4 + p % 4


def gather_lanes(tiles, pieces):
    quarter = iota(tiles[0].shape, 1) // 32
    made = None
    for at, (tile, piece) in enumerate(pieces):
        shift = (at - piece) * 32 % 128
        v = pltpu.roll(tiles[tile], shift, 1) if shift else tiles[tile]
        made = v if made is None else jnp.where(quarter == at, v, made)
    return made


def tiles_of(v):
    return [v[:, t * 128 : (t + 1) * 128] for t in range(D // 128)]


def to_block_order(tiles):
    made = []
    for t in range(16):
        p, half = t // 2, t % 2
        chips = [chip_of(half * 4 + k, p) for k in range(4)]
        made.append(gather_lanes(tiles, [(c // 4, c % 4) for c in chips]))
    return made


def from_block_order(tiles):
    made = []
    for v in range(16):
        g, yl = v // 2, v % 2
        places = [(yl + g) % 2 * 4 + x for x in range(4)]
        made.append(gather_lanes(tiles, [(p * 2 + g // 4, g % 4) for p in places]))
    return made


def lanes(k):
    return pl.ds(pl.multiple_of(k * BLK, BLK), BLK)


def kernel(
    tok_h, ck, cv, clen_h, g1_h, wq_h, wk, wv, hb_h, wo_h, g2_h, gid_h, mem_h, gg_h, mw_h, eg, eu, ed, wg_h, wu_h, hg_h, wd_h, bl_h,
    out, nk, nv,
    kb, vb, egb, eub, edb, wkb, wvb,
    wqb, wob, wgb, wub, wdb,
    xa, xc, xd, qs, qr, ts, tb, cs0, cb, cs, cd, pq, po, qstack, qb, ob, ps, pr, ys,
    sq, sqr, zb, zs, zr, hbuf, zf, zd, wot, wgt, wut, sc, wt, g2b, hgb, wgp, wup, wdp,
    lsem, s_wq, s_wo, s_wg, s_wu, s_wd, s_pair, s_ex, s_xa, s_xc, s_ts, s_cb, s_cd, s_q, s_pr, s_y, s_sq, s_z, s_wq2, s_xc2,
    tok, clen, g1, wq, hb, wo, g2, gid, mem, gg, mw, wg, wu, hg, wd, bl, fsem,
):
    me = lax.axis_index("ep")
    chip = me // 2
    core = me % 2
    group = me // 16
    place = (chip % 8 // 4 + group) % 2 * 4 + chip % 4
    pair = chip * 2 + (1 - core)

    fetch = [
        pltpu.make_async_copy(src, dst, fsem.at[k])
        for k, (src, dst) in enumerate(
            (
                (tok_h, tok), (g1_h, g1), (gid_h, gid), (mem_h, mem), (mw_h, mw), (gg_h, gg), (clen_h, clen), (hb_h, hb),
                (wq_h, wq), (wo_h, wo), (g2_h, g2), (hg_h, hg), (wg_h, wg), (wu_h, wu), (wd_h, wd), (bl_h, bl),
            )
        )
    ]
    local = [
        pltpu.make_async_copy(ck, kb, lsem.at[0]),
        pltpu.make_async_copy(cv, vb, lsem.at[1]),
        pltpu.make_async_copy(wk, wkb, lsem.at[2]),
        pltpu.make_async_copy(wv, wvb, lsem.at[3]),
        pltpu.make_async_copy(ed.at[0], edb.at[0], lsem.at[4]),
    ]

    def load_experts(k, carry):
        src = pl.ds(pl.multiple_of(chip_of(k % 8, k // 8) * 32, 32), 32)
        dst = pl.ds(pl.multiple_of(k * 32, 32), 32)
        pltpu.make_async_copy(eg.at[0, src], egb.at[0, dst], lsem.at[5]).start()
        pltpu.make_async_copy(eu.at[0, src], eub.at[0, dst], lsem.at[6]).start()
        return carry

    barrier = pltpu.get_barrier_semaphore()

    def greet(k, carry):
        mate = chip_of(group, (place + k) % 8) * 2 + core
        counterpart = chip_of((group + k) % 8, place) * 2 + core
        pl.semaphore_signal(barrier, inc=1, device_id=(mate,), device_id_type=MESH)
        pl.semaphore_signal(barrier, inc=1, device_id=(counterpart,), device_id_type=MESH)
        return carry

    for c in fetch:
        c.start()
    pl.semaphore_signal(barrier, inc=1, device_id=(pair,), device_id_type=MESH)
    lax.fori_loop(1, 8, greet, 0, unroll=7)
    for c in local:
        c.start()

    for c in fetch:
        c.wait()
    x = tok[...].astype(F32)
    normed = (x * lax.rsqrt(jnp.mean(x * x, axis=-1, keepdims=True) + EPS) * g1[...]).astype(BF)
    xa[place] = normed
    gids = gid[...]
    hits = one_hot(iota((8, SEQ), 0) == gids)
    before = dot(hits, one_hot(iota((SEQ, SEQ), 0) < iota((SEQ, SEQ), 1)))
    rank = jnp.sum(hits * before, axis=0, keepdims=True).astype(jnp.int32)
    spot = gids * 2 + rank
    order = one_hot(iota((SEQ, SEQ), 0) == spot)
    eye16 = iota((SEQ, SEQ), 0) == iota((SEQ, SEQ), 1)
    share = jnp.zeros((128, SEQ), F32)
    for k in range(6):
        share = share + jnp.where(iota((128, SEQ), 0) == mem[k : k + 1, :], mw[k : k + 1, :], 0.0)
    share = share * gg[...] + jnp.where(iota((128, SEQ), 0) == SEQ, spot.astype(F32), 0.0)
    shared = lax.dot_general(one_hot(eye16), share, NT, precision=HI, preferred_element_type=F32)
    cs0[...] = shared
    cb[place] = shared

    pl.semaphore_wait(barrier, 15)

    near, far = pl.ds(0, D // 2), pl.ds(D // 2, D // 2)

    def spread_strip(strip, buf, sems):
        slot = buf.at[group, core]

        def send(k, carry):
            g = (group + k) % 8
            remote(strip, slot, sems, chip_of(g, place) * 2 + core).start()
            return carry

        pltpu.make_async_copy(strip, slot, sems.at[1]).start()
        lax.fori_loop(1, 8, send, 0)

    def pass_on(buf, sems, k):
        take(buf.at[:, core], sems.at[1])
        remote(buf.at[:, core], buf.at[:, core], s_pair.at[k], pair).start()

    depth, side = group // 2, group % 2
    mirror = chip_of(group + 1 - 2 * side, place) * 2 + core

    def along_z(src, dst, sem):
        def send(k, carry):
            remote(src, dst, sem, chip_of((depth + k) % 4 * 2 + side, place) * 2 + core).start()
            return carry

        lax.fori_loop(1, 4, send, 0)

    def plant(strip, buf, sems):
        slot = buf.at[depth, side, core]
        pltpu.make_async_copy(strip, slot, sems.at[5, 1]).start()
        along_z(strip.at[:, near], slot.at[:, near], sems.at[0])
        remote(strip.at[:, far], slot.at[:, far], sems.at[1], mirror).start()
        along_z(strip.at[:, far], slot.at[:, far], sems.at[2])

    def relay(buf, sems):
        take(buf.at[0, 0, core], sems.at[5, 1])
        take(buf.at[0, 0, core, :, far], sems.at[1, 1])
        ahead = buf.at[depth, 1 - side, core, :, far]
        along_z(ahead, ahead, sems.at[3])
        take(buf.at[pl.ds(0, 3), 0, core, :, near], sems.at[0, 1])
        across = buf.at[:, side, core, :, near]
        remote(across, across, sems.at[4], mirror).start()

    def finish(buf, sems, k):
        take(buf.at[pl.ds(0, 3), 0, core, :, far], sems.at[2, 1])
        take(buf.at[pl.ds(0, 3), 0, core, :, far], sems.at[3, 1])
        take(buf.at[:, 0, core, :, near], sems.at[4, 1])
        remote(buf.at[:, :, core], buf.at[:, :, core], s_pair.at[k], pair).start()

    def uproot(buf, sems):
        take(buf.at[pl.ds(0, 3), 0, core, :, near], sems.at[0, 0])
        take(buf.at[0, 0, core, :, far], sems.at[1, 0])
        take(buf.at[pl.ds(0, 3), 0, core, :, far], sems.at[2, 0])
        take(buf.at[pl.ds(0, 3), 0, core, :, far], sems.at[3, 0])
        take(buf.at[:, 0, core, :, near], sems.at[4, 0])

    def in_group(src_of, dst, sems):
        def send(k, carry):
            p = (place + k) % 8
            remote(src_of(p), dst, sems, chip_of(group, p) * 2 + core).start()
            return carry

        lax.fori_loop(1, 8, send, 0)

    def over_plane(src_of, dst_of, sems):
        def send(k, carry):
            other = (chip + k * 27) % 64
            remote(src_of(other), dst_of(other), sems, other * 2 + core).start()
            return carry

        lax.fori_loop(1, 64, send, 0, unroll=7)

    spread_strip(wq.at[:, near], wqb.at[:, :, :, near], s_wq)
    spread_strip(wq.at[:, far], wqb.at[:, :, :, far], s_wq2)
    in_group(lambda p: xa.at[place], xa.at[place], s_xa)
    in_group(lambda p: cs0, cb.at[place], s_cb)

    @pl.when(core == 0)
    def _():
        plant(wo, wob, s_wo)

    lax.fori_loop(0, 64, load_experts, 0, unroll=4)
    moved = to_block_order(tiles_of(tok[...].astype(F32)))
    for k in range(8):
        ts[k] = jnp.concatenate(moved[2 * k : 2 * k + 2], axis=1).astype(BF)
    tb[place] = ts[place]
    in_group(lambda p: ts.at[p], tb.at[place], s_ts)
    for src, dst in ((g2, g2b), (hg, hgb), (wg, wgp), (wu, wup), (wd, wdp)):
        for k, tile in enumerate(to_block_order(tiles_of(src[...].astype(F32)))):
            dst[:, k * 128 : (k + 1) * 128] = tile.astype(dst.dtype)

    @pl.when(core == 0)
    def _():
        plant(wgp, wgb, s_wg)

    local[2].wait()
    local[3].wait()
    nk[...] = dot(normed, wkb[...]).astype(BF)
    nv[...] = dot(normed, wvb[...]).astype(BF)
    rows, cols = iota((512, 512), 0), iota((512, 512), 1)
    pq[...] = one_hot(cols == rows % 32 * 16 + rows // 32).astype(BF)
    rows, cols = iota((256, 256), 0), iota((256, 256), 1)
    po[...] = one_hot(cols == rows % 8 * 32 + rows // 8).astype(BF)
    r, c = iota((128, 128), 0), iota((128, 128), 1)
    fold = one_hot(c == r % 8 * 16 + r // 16 * 2 + r % 16 // 8).astype(BF)
    eye = r == c
    eye32 = iota((32, 32), 0) == iota((32, 32), 1)
    bias = jnp.sum(jnp.where(eye32, jnp.broadcast_to(hb[...], (32, 32)), 0.0), axis=1, keepdims=True)
    tri = one_hot(iota((BLK, BLK), 0) >= iota((BLK, BLK), 1)).astype(BF)

    pass_on(wqb.at[:, :, :, near], s_wq, 0)
    pass_on(wqb.at[:, :, :, far], s_wq2, 5)

    @pl.when(core == 1)
    def _():
        plant(wo, wob, s_wo)
        plant(wgp, wgb, s_wg)

    take(xa.at[pl.ds(0, 7)], s_xa.at[1])
    take(wqb.at[:, core, :, near], s_pair.at[0, 1])
    q = dot_nt(xa[:, :, : D // 2].reshape(128, D // 2), wqb[:, :, :, : D // 2].reshape(BLK, D // 2))
    take(wqb.at[:, core, :, far], s_pair.at[5, 1])
    q = q + dot_nt(xa[:, :, D // 2 :].reshape(128, D // 2), wqb[:, :, :, D // 2 :].reshape(BLK, D // 2))
    q = q.astype(BF)
    qs[...] = q.reshape(8, SEQ, BLK)
    qr[:, lanes(place)] = qs[place]
    in_group(lambda p: qs.at[p], qr.at[:, lanes(place)], s_q)

    for k, buf in enumerate((edb, egb, eub)):
        take(buf.at[0], lsem.at[4 + k])
        remote(buf.at[0], buf.at[1], s_ex.at[k], pair).start()

    take(tb.at[pl.ds(0, 7)], s_ts.at[1])
    take(cb.at[pl.ds(0, 7)], s_cb.at[1])
    sent = cb[...].reshape(128, 128)
    spot_row = jnp.sum(jnp.where(eye, jnp.broadcast_to(sent[:, SEQ : SEQ + 1], (128, 128)), 0.0), axis=0, keepdims=True)
    wanted = (r // 16 * 2 + r % 2).astype(F32)
    regroup = jnp.where(c // 16 == r % 16 // 2, one_hot(wanted == jnp.broadcast_to(spot_row, (128, 128))), 0.0)
    regroup_bf = regroup.astype(BF)
    combs = jnp.dot(regroup, sent, precision=HI, preferred_element_type=F32)
    cs[...] = combs.reshape(8, SEQ, 128)
    cd[group] = cs[group]

    def send_comb(k, carry):
        g = (group + k) % 8
        remote(cs.at[g], cd.at[group], s_cd, chip_of(g, place) * 2 + core).start()
        return carry

    lax.fori_loop(1, 8, send_comb, 0)

    relay(wob, s_wo)
    plant(wup, wub, s_wu)
    over_plane(lambda o: wdp.at[:, lanes((o % 8 // 4 + o // 8) % 2 * 4 + o % 4)], lambda o: wdb.at[chip, core], s_wd)
    own_wd = pltpu.make_async_copy(wdp.at[:, lanes(place)], wdb.at[chip, core], lsem.at[7])
    own_wd.start()

    take(qr.at[:, pl.ds(0, 7 * BLK)], s_q.at[1])
    came = tiles_of(qr[...].astype(F32) * HEAD_DIM**-0.5)
    quarter = iota((SEQ, 128), 1) // 32
    for h in range(HEADS):
        t, g, yl = h // 2, h // 4, h // 2 % 2
        row = jnp.zeros((SEQ, 128), F32)
        for k in range(2):
            p = (yl + g) % 2 * 4 + h % 2 * 2 + k
            at = (2 if t >= 8 else 0) + k
            shift = (at - g % 4) * 32 % 128
            v = came[p * 2 + g // 4]
            row = jnp.where(quarter == at, pltpu.roll(v, shift, 1) if shift else v, row)
        qstack[16 * h : 16 * h + 16, :] = row.astype(BF)
    qb[...] = dot(pq[...], qstack[...]).astype(BF).reshape(SEQ, HEADS, 128)
    local[0].wait()
    local[1].wait()

    def score(t):
        for k in range(2):
            sc[t % 2, k] = dot_nt(qb[2 * t + k], kb[2 * t + k]) + bias

    def weigh(t):
        parts = []
        for k in range(2):
            length = clen[2 * t + k]
            for n in range(4):
                v = sc[t % 2, k, :, n * BLK : (n + 1) * BLK]
                live = iota((HEADS, BLK), 1) < length - n * BLK
                rest = jnp.where(live, -(jnp.maximum(v, 0.0) + jnp.log(1.0 + jnp.exp(-jnp.abs(v)))), 0.0)
                parts.extend(split2(rest))
        sums = dot(jnp.concatenate(parts, axis=0), tri)
        for k in range(2):
            length = clen[2 * t + k]
            run = jnp.zeros((HEADS, 1), F32)
            for n in (3, 2, 1, 0):
                at = (k * 4 + n) * 64
                within = sums[at : at + 32] + sums[at + 32 : at + 64]
                live = iota((HEADS, BLK), 1) < length - n * BLK
                v = sc[t % 2, k, :, n * BLK : (n + 1) * BLK]
                wt[t % 2, k, :, n * BLK : (n + 1) * BLK] = jnp.where(live, jnp.exp(v + within + run), 0.0).astype(BF)
                run = run + within[:, 0:1]

    def mix(t):
        for k in range(2):
            ob[2 * t + k] = dot(wt[t % 2, k], vb[2 * t + k]).astype(BF)

    def hand_out(half):
        rows8 = slice(half * 8, half * 8 + 8)
        heads = dot(po[...], ob[rows8].reshape(256, 128))
        left8 = iota((8, 128), 1) < HEAD_DIM
        for t in range(16):
            a = heads[16 * t : 16 * t + 8, :]
            b = heads[16 * t + 8 : 16 * t + 16, :]
            if t < 8:
                joined = jnp.where(left8, a, pltpu.roll(b, HEAD_DIM, 1))
            else:
                joined = jnp.where(left8, pltpu.roll(a, HEAD_DIM, 1), b)
            xc[place, rows8, t * 128 : (t + 1) * 128] = joined.astype(BF)
        part = xc.at[place, pl.ds(half * 8, 8)]
        in_group(lambda p: part, part, s_xc if half == 0 else s_xc2)

    for t in range(10):
        if t < 8:
            score(t)
        if 1 <= t < 9:
            weigh(t - 1)
        if t >= 2:
            mix(t - 2)
        if t == 5:
            hand_out(0)
    hand_out(1)
    relay(wgb, s_wg)
    finish(wob, s_wo, 1)
    relay(wub, s_wu)

    take(wob.at[:, :, core], s_pair.at[1, 1])
    wot[...] = wob[...].reshape(BLK, D).T
    take(xc.at[pl.ds(0, 7), pl.ds(0, 8)], s_xc.at[1])
    take(xc.at[pl.ds(0, 7), pl.ds(0, 8)], s_xc2.at[1])
    proj = dot(xc[...].reshape(128, D), wot[...]).astype(BF)
    stream = tb[...].reshape(128, BLK).astype(F32) + proj.astype(F32)
    y = (stream * g2b[:, lanes(place)]).astype(BF)
    ys[...] = dot(regroup_bf, y).astype(BF).reshape(8, SEQ, BLK)
    xd[group, :, lanes(place)] = ys[group]
    over_plane(lambda o: ys.at[o // 8], lambda o: xd.at[group, :, lanes(place)], s_y)
    ps[...] = proj.reshape(8, SEQ, BLK)
    pr[:, lanes(place)] = ps[place]
    in_group(lambda p: ps.at[p], pr.at[:, lanes(place)], s_pr)

    finish(wgb, s_wg, 2)
    finish(wub, s_wu, 3)
    own_wd.wait()
    take(wdb.at[pl.ds(0, 63), core], s_wd.at[1])
    remote(wdb.at[:, core], wdb.at[:, core], s_pair.at[4], pair).start()
    take(cd.at[pl.ds(0, 7)], s_cd.at[1])
    lane = iota((128, 128), 1)
    comb = cd[...].reshape(128, 128)
    member0 = chip % 8 * 2 + core
    member1 = chip % 8 * 2 + 1 - core
    comb0 = jnp.sum(jnp.where(lane == member0, comb, 0.0), axis=1, keepdims=True)
    comb1 = jnp.sum(jnp.where(lane == member1, comb, 0.0), axis=1, keepdims=True)

    take(wgb.at[:, :, core], s_pair.at[2, 1])
    wgt[...] = wgb[...].reshape(BLK, D).T
    take(wub.at[:, :, core], s_pair.at[3, 1])
    wut[...] = wub[...].reshape(BLK, D).T

    take(zr.at[pl.ds(0, 63)], s_y.at[1])
    rows_in = xd[...].reshape(128, D)
    plain = rows_in.astype(F32) * (1.0 / g2b[...])
    scale = lax.rsqrt(jnp.mean(plain * plain, axis=1, keepdims=True) + EPS)
    gate = dot(rows_in, wgt[...]) * scale
    upper = dot(rows_in, wut[...]) * scale
    hidden = gate * jax.nn.sigmoid(gate) * upper
    part = jnp.sum(hidden * hidden, axis=1, keepdims=True)
    part_row = jnp.sum(jnp.where(eye, jnp.broadcast_to(part, (128, 128)), 0.0), axis=0, keepdims=True)
    sq[...] = jnp.broadcast_to(part_row, (8, 128))
    sqr[place] = sq[...]
    in_group(lambda p: sq, sqr.at[place], s_sq)

    for e, comb_e in ((0, comb0), (1, comb1)):
        if e == 1:
            take(edb.at[1], s_ex.at[0, 1])
            take(egb.at[1], s_ex.at[1, 1])
            take(eub.at[1], s_ex.at[2, 1])
        gate_e = dot(rows_in, egb[e]) * scale
        upper_e = dot(rows_in, eub[e]) * scale
        hbuf[:, e * 512 : (e + 1) * 512] = (gate_e * jax.nn.sigmoid(gate_e) * upper_e * comb_e).astype(BF)

    def route(k, carry):
        zf[:, lanes(k)] = dot(hbuf[...], edb[:, :, lanes(k)].reshape(1024, BLK))
        return carry

    lax.fori_loop(0, 8, route, 0, unroll=2)
    dense = (hidden * hgb[:, lanes(place)]).astype(BF)
    take(wdb.at[:, core], s_pair.at[4, 1])

    def down(k, carry):
        v = dot_nt(dense, wdb[pl.ds(k * 8, 8)].reshape(BLK, BLK))
        zd[:, lanes(k)] = jax.nn.sigmoid(bl[:, lanes(k)]) * v
        return carry

    lax.fori_loop(0, 8, down, 0, unroll=2)
    spots = dot_nt(one_hot(iota((128, SEQ), 0) % 16 == iota((128, SEQ), 1)), order)
    unfold = dot(spots, one_hot(iota((SEQ, 128), 1) // 8 == iota((SEQ, 128), 0)))
    unfold = jnp.where(r // 16 == c % 8, unfold, 0.0).astype(BF)
    take(pr.at[:, pl.ds(0, 7 * BLK)], s_pr.at[1])
    second = from_block_order(tiles_of(pr[...].astype(F32)))
    take(sqr.at[pl.ds(0, 7)], s_sq.at[1])
    total = jnp.sum(sqr[...], axis=0)[0:1, :]
    total_col = jnp.sum(jnp.where(eye, jnp.broadcast_to(total, (128, 128)), 0.0), axis=1, keepdims=True)
    dense_scale = lax.rsqrt(total_col * (1.0 / D) + EPS)

    def produce(k, carry):
        z = zf[:, lanes(k)] + dense_scale * zd[:, lanes(k)]
        zb[k] = z.astype(BF).reshape(8, SEQ, BLK)
        return carry

    lax.fori_loop(0, 8, produce, 0, unroll=2)

    def give(k, carry):
        g = (group + k) % 8
        zs[g] = dot(fold, zb[:, g].reshape(128, BLK)).astype(BF).reshape(8, SEQ, BLK)

        def send(j, carry):
            p = (place + j) % 8
            remote(zs.at[g, p], zr.at[chip], s_z, chip_of(g, p) * 2 + core).start()
            return carry

        @pl.when(g == group)
        def _():
            zr[chip] = zs[g, place]

        @pl.when(g != group)
        def _():
            send(0, 0)

        lax.fori_loop(1, 8, send, 0)
        return carry

    lax.fori_loop(0, 8, give, 0)

    take(zr.at[pl.ds(0, 63)], s_z.at[1])
    sums = jnp.sum(zr[...].reshape(8, 8, SEQ, BLK).astype(F32), axis=1).reshape(128, BLK)
    high, low = split2(sums)
    branch = dot(unfold, high) + dot(unfold, low)
    for k in range(8):
        s = slice(k * BLK, (k + 1) * BLK)
        own = tok[:, s].astype(F32) + jnp.concatenate(second[2 * k : 2 * k + 2], axis=1)
        out[:, s] = (own + branch[k * 16 : k * 16 + 16]).astype(BF)

    take(wqb.at[pl.ds(0, 7), core, :, near], s_wq.at[0])
    take(wqb.at[pl.ds(0, 7), core, :, far], s_wq2.at[0])
    uproot(wob, s_wo)
    uproot(wgb, s_wg)
    uproot(wub, s_wu)
    take(wdb.at[pl.ds(0, 63), core], s_wd.at[0])
    for k, buf in enumerate((wob, wgb, wub)):
        take(buf.at[:, :, core], s_pair.at[k + 1, 0])
    for k, buf in ((0, wqb.at[:, :, :, near]), (4, wdb), (5, wqb.at[:, :, :, far])):
        take(buf.at[:, core], s_pair.at[k, 0])
    take(edb.at[1], s_ex.at[0, 0])
    take(egb.at[1], s_ex.at[1, 0])
    take(eub.at[1], s_ex.at[2, 0])
    take(xa.at[pl.ds(0, 7)], s_xa.at[0])
    take(xc.at[pl.ds(0, 7), pl.ds(0, 8)], s_xc.at[0])
    take(xc.at[pl.ds(0, 7), pl.ds(0, 8)], s_xc2.at[0])
    take(tb.at[pl.ds(0, 7)], s_ts.at[0])
    take(cb.at[pl.ds(0, 7)], s_cb.at[0])
    take(cd.at[pl.ds(0, 7)], s_cd.at[0])
    take(qr.at[:, pl.ds(0, 7 * BLK)], s_q.at[0])
    take(pr.at[:, pl.ds(0, 7 * BLK)], s_pr.at[0])
    take(zr.at[pl.ds(0, 63)], s_y.at[0])
    take(sqr.at[pl.ds(0, 7)], s_sq.at[0])
    take(zr.at[pl.ds(0, 63)], s_z.at[0])


def write_out(a, b, c, a_out, b_out, c_out, sems):
    copies = [pltpu.make_async_copy(src, dst, sems.at[k]) for k, (src, dst) in enumerate(((a, a_out), (b, b_out), (c, c_out)))]
    for x in copies:
        x.start()
    for x in copies:
        x.wait()


def shards(
    tokens, cache_keys, cache_values, cache_len, norm_gain_first, w_query, w_key, w_value, head_bias,
    w_output, norm_gain_second, group_id, member, group_gate, member_weight, expert_gate_w, expert_up_w,
    expert_down_w, dense_gate_w, dense_up_w, hidden_gain, dense_down_w, branch_logit,
):
    vmem = pl.BlockSpec(memory_space=pltpu.VMEM)
    hbm = pl.BlockSpec(memory_space=pl.ANY)
    V = pltpu.VMEM
    strips = (8, 2, SEQ, D)
    pair_sem = pltpu.SemaphoreType.DMA((2,))
    tree_sem = pltpu.SemaphoreType.DMA((6, 2))
    args = (
        (tokens, hbm),
        (cache_keys, hbm),
        (cache_values, hbm),
        (cache_len, hbm),
        (norm_gain_first.reshape(1, D), hbm),
        (w_query.T, hbm),
        (w_key, hbm),
        (w_value, hbm),
        (head_bias.reshape(1, HEADS), hbm),
        (w_output.T, hbm),
        (norm_gain_second.reshape(1, D), hbm),
        (group_id.reshape(1, SEQ), hbm),
        (member.T, hbm),
        (group_gate.reshape(1, SEQ), hbm),
        (member_weight.T, hbm),
        (expert_gate_w, hbm),
        (expert_up_w, hbm),
        (expert_down_w, hbm),
        (dense_gate_w.T, hbm),
        (dense_up_w.T, hbm),
        (hidden_gain.reshape(1, D), hbm),
        (dense_down_w.T, hbm),
        (branch_logit.reshape(1, D), hbm),
    )
    scratch = [
        V((SEQ, CACHE, 128), BF),
        V((SEQ, CACHE, 128), BF),
        V((2, D, 512), BF),
        V((2, D, 512), BF),
        V((2, 512, D), BF),
        V((D, 128), BF),
        V((D, 128), BF),
        V(strips, BF),
        V((4, 2, 2, SEQ, D), BF),
        V((4, 2, 2, SEQ, D), BF),
        V((4, 2, 2, SEQ, D), BF),
        V((64, 2, SEQ, BLK), BF),
        V((8, SEQ, D), BF),
        V((8, SEQ, D), BF),
        V((8, SEQ, D), BF),
        V((8, SEQ, BLK), BF),
        V((SEQ, D), BF),
        V((8, SEQ, BLK), BF),
        V((8, SEQ, BLK), BF),
        V((SEQ, 128), F32),
        V((8, SEQ, 128), F32),
        V((8, SEQ, 128), F32),
        V((8, SEQ, 128), F32),
        V((512, 512), BF),
        V((256, 256), BF),
        V((512, 128), BF),
        V((SEQ, HEADS, 128), BF),
        V((SEQ, HEADS, 128), BF),
        V((8, SEQ, BLK), BF),
        V((SEQ, D), BF),
        V((8, SEQ, BLK), BF),
        V((8, 128), F32),
        V((8, 8, 128), F32),
        V((8, 8, SEQ, BLK), BF),
        V((8, 8, SEQ, BLK), BF),
        V((64, SEQ, BLK), BF),
        V((128, 1024), BF),
        V((128, D), F32),
        V((128, D), F32),
        V((D, BLK), BF),
        V((D, BLK), BF),
        V((D, BLK), BF),
        V((2, 2, HEADS, CACHE), F32),
        V((2, 2, HEADS, CACHE), BF),
        V((1, D), F32),
        V((1, D), F32),
        V((SEQ, D), BF),
        V((SEQ, D), BF),
        V((SEQ, D), BF),
        pltpu.SemaphoreType.DMA((8,)),
        pair_sem,
        tree_sem,
        tree_sem,
        tree_sem,
        pair_sem,
        pltpu.SemaphoreType.DMA((6, 2)),
        pltpu.SemaphoreType.DMA((3, 2)),
    ] + [pair_sem] * 12
    for a, space in (
        (0, V), (3, pltpu.SMEM), (4, V), (5, V), (8, V), (9, V), (10, V), (11, V),
        (12, V), (13, V), (14, V), (18, V), (19, V), (20, V), (21, V), (22, V),
    ):
        scratch.append(space(args[a][0].shape, args[a][0].dtype))
    scratch.append(pltpu.SemaphoreType.DMA((16,)))
    shapes = (
        jax.ShapeDtypeStruct((SEQ, D), BF),
        jax.ShapeDtypeStruct((SEQ, 128), BF),
        jax.ShapeDtypeStruct((SEQ, 128), BF),
    )
    made = pl.pallas_call(
        kernel,
        out_shape=tuple(pltpu.VMEM(x.shape, x.dtype) for x in shapes),
        in_specs=[spec for _, spec in args],
        out_specs=(vmem, vmem, vmem),
        scratch_shapes=scratch,
        compiler_params=pltpu.CompilerParams(
            collective_id=0, has_side_effects=True, vmem_limit_bytes=62_000_000
        ),
    )(*[a for a, _ in args])
    return pl.pallas_call(
        write_out, out_shape=shapes, in_specs=[vmem] * 3, out_specs=(hbm,) * 3,
        scratch_shapes=[pltpu.SemaphoreType.DMA((3,))],
    )(*[pltpu.with_memory_space_constraint(x, pltpu.VMEM) for x in made])


def solution(mesh):
    in_specs = (
        P("ep", None),
        P("ep", None, None),
        P("ep", None, None),
        P("ep"),
        P(),
        P(None, "ep"),
        P(),
        P(),
        P(),
        P(None, "ep"),
        P(),
        P("ep"),
        P("ep", None),
        P("ep"),
        P("ep", None),
        P("ep", None, None),
        P("ep", None, None),
        P("ep", None, None),
        P(None, "ep"),
        P(None, "ep"),
        P(),
        P(None, "ep"),
        P(),
    )
    out_specs = (P("ep", None), P("ep", None), P("ep", None))
    return jax.shard_map(shards, mesh=mesh, in_specs=in_specs, out_specs=out_specs, check_vma=False)
```

```python
import functools

import jax
import jax.numpy as jnp
from jax import lax
from jax.experimental import pallas as pl
from jax.experimental.pallas import tpu as pltpu
from jax.sharding import PartitionSpec as P

D = 2048
HEADS = 32
HEAD_DIM = 64
SEQ = 16
CACHE = 1024
BLK = 256
EPS = 1e-06
F32 = jnp.float32
BF = jnp.bfloat16
MESH = pl.DeviceIdType.MESH
NT = (((1,), (1,)), ((), ()))
HI = lax.Precision.HIGHEST


def iota(shape, dim):
    return lax.broadcasted_iota(jnp.int32, shape, dim)


def one_hot(mask):
    return jnp.where(mask, 1.0, 0.0)


def dot(a, b):
    return jnp.dot(a, b, preferred_element_type=F32)


def dot_nt(a, b):
    return lax.dot_general(a, b, NT, preferred_element_type=F32)


def split2(v):
    high = v.astype(BF)
    return high, (v - high.astype(F32)).astype(BF)


def remote(src, dst, sems, target):
    return pltpu.make_async_remote_copy(
        src_ref=src,
        dst_ref=dst,
        send_sem=sems.at[0],
        recv_sem=sems.at[1],
        device_id=(target,),
        device_id_type=MESH,
    )


def take(ref, sem):
    pltpu.make_async_copy(ref, ref, sem).wait()


def chip_of(g, p):
    return g * 8 + (p // 4 + g) % 2 * 4 + p % 4


def gather_lanes(tiles, pieces):
    quarter = iota(tiles[0].shape, 1) // 32
    made = None
    for at, (tile, piece) in enumerate(pieces):
        shift = (at - piece) * 32 % 128
        v = pltpu.roll(tiles[tile], shift, 1) if shift else tiles[tile]
        made = v if made is None else jnp.where(quarter == at, v, made)
    return made


def tiles_of(v):
    return [v[:, t * 128 : (t + 1) * 128] for t in range(D // 128)]


def to_block_order(tiles):
    made = []
    for t in range(16):
        p, half = t // 2, t % 2
        chips = [chip_of(half * 4 + k, p) for k in range(4)]
        made.append(gather_lanes(tiles, [(c // 4, c % 4) for c in chips]))
    return made


def from_block_order(tiles):
    made = []
    for v in range(16):
        g, yl = v // 2, v % 2
        places = [(yl + g) % 2 * 4 + x for x in range(4)]
        made.append(gather_lanes(tiles, [(p * 2 + g // 4, g % 4) for p in places]))
    return made


def lanes(k):
    return pl.ds(pl.multiple_of(k * BLK, BLK), BLK)


def kernel(
    tok_h, ck, cv, clen_h, g1_h, wq_h, wk, wv, hb_h, wo_h, g2_h, gid_h, mem_h, gg_h, mw_h, eg, eu, ed, wg_h, wu_h, hg_h, wd_h, bl_h,
    out, nk, nv,
    kb, vb, egb, eub, edb, wkb, wvb,
    wqb, wob, wgb, wub, wdb,
    xa, xc, xd, qs, qr, ts, tb, cs0, cb, cs, cd, pq, po, qstack, qb, ob, ps, pr, ys,
    sq, sqr, zb, zs, zr, hbuf, zf, zd, wot, wgt, wut, sc, wt, g2b, hgb, wgp, wup, wdp,
    lsem, s_wq, s_wo, s_wg, s_wu, s_wd, s_pair, s_ex, s_xa, s_xc, s_ts, s_cb, s_cd, s_q, s_pr, s_y, s_sq, s_z, s_wq2, s_xc2,
    tok, clen, g1, wq, hb, wo, g2, gid, mem, gg, mw, wg, wu, hg, wd, bl, fsem,
):
    me = lax.axis_index("ep")
    chip = me // 2
    core = me % 2
    group = me // 16
    place = (chip % 8 // 4 + group) % 2 * 4 + chip % 4
    pair = chip * 2 + (1 - core)

    fetch = [
        pltpu.make_async_copy(src, dst, fsem.at[k])
        for k, (src, dst) in enumerate(
            (
                (tok_h, tok), (g1_h, g1), (gid_h, gid), (mem_h, mem), (mw_h, mw), (gg_h, gg), (clen_h, clen), (hb_h, hb),
                (wq_h, wq), (wo_h, wo), (g2_h, g2), (hg_h, hg), (wg_h, wg), (wu_h, wu), (wd_h, wd), (bl_h, bl),
            )
        )
    ]
    local = [
        pltpu.make_async_copy(ck, kb, lsem.at[0]),
        pltpu.make_async_copy(cv, vb, lsem.at[1]),
        pltpu.make_async_copy(wk, wkb, lsem.at[2]),
        pltpu.make_async_copy(wv, wvb, lsem.at[3]),
        pltpu.make_async_copy(ed.at[0], edb.at[0], lsem.at[4]),
    ]

    def load_experts(k, carry):
        src = pl.ds(pl.multiple_of(chip_of(k % 8, k // 8) * 32, 32), 32)
        dst = pl.ds(pl.multiple_of(k * 32, 32), 32)
        pltpu.make_async_copy(eg.at[0, src], egb.at[0, dst], lsem.at[5]).start()
        pltpu.make_async_copy(eu.at[0, src], eub.at[0, dst], lsem.at[6]).start()
        return carry

    barrier = pltpu.get_barrier_semaphore()

    def greet(k, carry):
        mate = chip_of(group, (place + k) % 8) * 2 + core
        counterpart = chip_of((group + k) % 8, place) * 2 + core
        pl.semaphore_signal(barrier, inc=1, device_id=(mate,), device_id_type=MESH)
        pl.semaphore_signal(barrier, inc=1, device_id=(counterpart,), device_id_type=MESH)
        return carry

    for c in fetch:
        c.start()
    pl.semaphore_signal(barrier, inc=1, device_id=(pair,), device_id_type=MESH)
    lax.fori_loop(1, 8, greet, 0, unroll=7)
    for c in local:
        c.start()

    for c in fetch:
        c.wait()
    x = tok[...].astype(F32)
    normed = (x * lax.rsqrt(jnp.mean(x * x, axis=-1, keepdims=True) + EPS) * g1[...]).astype(BF)
    xa[place] = normed
    gids = gid[...]
    hits = one_hot(iota((8, SEQ), 0) == gids)
    before = dot(hits, one_hot(iota((SEQ, SEQ), 0) < iota((SEQ, SEQ), 1)))
    rank = jnp.sum(hits * before, axis=0, keepdims=True).astype(jnp.int32)
    spot = gids * 2 + rank
    order = one_hot(iota((SEQ, SEQ), 0) == spot)
    eye16 = iota((SEQ, SEQ), 0) == iota((SEQ, SEQ), 1)
    share = jnp.zeros((128, SEQ), F32)
    for k in range(6):
        share = share + jnp.where(iota((128, SEQ), 0) == mem[k : k + 1, :], mw[k : k + 1, :], 0.0)
    share = share * gg[...] + jnp.where(iota((128, SEQ), 0) == SEQ, spot.astype(F32), 0.0)
    shared = lax.dot_general(one_hot(eye16), share, NT, precision=HI, preferred_element_type=F32)
    cs0[...] = shared
    cb[place] = shared

    pl.semaphore_wait(barrier, 15)

    near, far = pl.ds(0, D // 2), pl.ds(D // 2, D // 2)

    def spread_strip(strip, buf, sems):
        slot = buf.at[group, core]

        pltpu.make_async_copy(strip, slot, sems.at[1]).start()
        for dz, dh in ((2, 1), (2, 0), (1, 1), (3, 1), (1, 0), (3, 0), (0, 1)):
            g = (group // 2 + dz) % 4 * 2 + (group + dh) % 2
            remote(strip, slot, sems, chip_of(g, place) * 2 + core).start()

    def pass_on(buf, sems, k):
        take(buf.at[:, core], sems.at[1])
        remote(buf.at[:, core], buf.at[:, core], s_pair.at[k], pair).start()

    depth, side = group // 2, group % 2
    mirror = chip_of(group + 1 - 2 * side, place) * 2 + core

    def along_z(src, dst, sem):
        for k in (2, 1, 3):
            remote(src, dst, sem, chip_of((depth + k) % 4 * 2 + side, place) * 2 + core).start()

    def plant(strip, buf, sems):
        slot = buf.at[depth, side, core]
        pltpu.make_async_copy(strip, slot, sems.at[5, 1]).start()
        along_z(strip.at[:, near], slot.at[:, near], sems.at[0])
        remote(strip.at[:, far], slot.at[:, far], sems.at[1], mirror).start()
        along_z(strip.at[:, far], slot.at[:, far], sems.at[2])

    def relay(buf, sems):
        take(buf.at[0, 0, core], sems.at[5, 1])
        take(buf.at[0, 0, core, :, far], sems.at[1, 1])
        ahead = buf.at[depth, 1 - side, core, :, far]
        along_z(ahead, ahead, sems.at[3])
        take(buf.at[pl.ds(0, 3), 0, core, :, near], sems.at[0, 1])
        across = buf.at[:, side, core, :, near]
        remote(across, across, sems.at[4], mirror).start()

    def finish(buf, sems, k):
        take(buf.at[pl.ds(0, 3), 0, core, :, far], sems.at[2, 1])
        take(buf.at[pl.ds(0, 3), 0, core, :, far], sems.at[3, 1])
        take(buf.at[:, 0, core, :, near], sems.at[4, 1])
        remote(buf.at[:, :, core], buf.at[:, :, core], s_pair.at[k], pair).start()

    def uproot(buf, sems):
        take(buf.at[pl.ds(0, 3), 0, core, :, near], sems.at[0, 0])
        take(buf.at[0, 0, core, :, far], sems.at[1, 0])
        take(buf.at[pl.ds(0, 3), 0, core, :, far], sems.at[2, 0])
        take(buf.at[pl.ds(0, 3), 0, core, :, far], sems.at[3, 0])
        take(buf.at[:, 0, core, :, near], sems.at[4, 0])

    def in_group(src_of, dst, sems):
        for dy, dx in ((1, 2), (0, 2), (1, 1), (1, 3), (0, 1), (0, 3), (1, 0)):
            p = (place // 4 + dy) % 2 * 4 + (place + dx) % 4
            remote(src_of(p), dst, sems, chip_of(group, p) * 2 + core).start()

    def over_plane(src_of, dst_of, sems):
        def one(dz, dy, dx):
            other = (depth + dz) % 4 * 16 + (chip // 4 + dy) % 4 * 4 + (chip + dx) % 4
            remote(src_of(other), dst_of(other), sems, other * 2 + core).start()

        def far_plane(k, carry):
            m = k * 7 % 16
            one(2, m // 4 + 2, m % 4 + 2)
            return carry

        def next_planes(k, carry):
            m = k * 7 % 16
            one(1, m // 4 + 2, m % 4 + 2)
            one(3, m % 4 + 2, m // 4 + 2)
            return carry

        lax.fori_loop(0, 16, far_plane, 0, unroll=4)
        lax.fori_loop(0, 16, next_planes, 0, unroll=4)
        own = [(y, x) for y in range(4) for x in range(4) if y or x]
        for y, x in sorted(own, key=lambda v: -min(v[0], 4 - v[0]) - min(v[1], 4 - v[1])):
            one(0, y, x)

    spread_strip(wq.at[:, near], wqb.at[:, :, :, near], s_wq)
    spread_strip(wq.at[:, far], wqb.at[:, :, :, far], s_wq2)
    in_group(lambda p: xa.at[place], xa.at[place], s_xa)
    in_group(lambda p: cs0, cb.at[place], s_cb)

    @pl.when(core == 0)
    def _():
        plant(wo, wob, s_wo)

    lax.fori_loop(0, 64, load_experts, 0, unroll=4)
    moved = to_block_order(tiles_of(tok[...].astype(F32)))
    for k in range(8):
        ts[k] = jnp.concatenate(moved[2 * k : 2 * k + 2], axis=1).astype(BF)
    tb[place] = ts[place]
    in_group(lambda p: ts.at[p], tb.at[place], s_ts)
    for src, dst in ((g2, g2b), (hg, hgb), (wg, wgp), (wu, wup), (wd, wdp)):
        for k, tile in enumerate(to_block_order(tiles_of(src[...].astype(F32)))):
            dst[:, k * 128 : (k + 1) * 128] = tile.astype(dst.dtype)

    @pl.when(core == 0)
    def _():
        plant(wgp, wgb, s_wg)

    local[2].wait()
    local[3].wait()
    nk[...] = dot(normed, wkb[...]).astype(BF)
    nv[...] = dot(normed, wvb[...]).astype(BF)
    rows, cols = iota((512, 512), 0), iota((512, 512), 1)
    pq[...] = one_hot(cols == rows % 32 * 16 + rows // 32).astype(BF)
    rows, cols = iota((256, 256), 0), iota((256, 256), 1)
    po[...] = one_hot(cols == rows % 8 * 32 + rows // 8).astype(BF)
    r, c = iota((128, 128), 0), iota((128, 128), 1)
    fold = one_hot(c == r % 8 * 16 + r // 16 * 2 + r % 16 // 8).astype(BF)
    eye = r == c
    eye32 = iota((32, 32), 0) == iota((32, 32), 1)
    bias = jnp.sum(jnp.where(eye32, jnp.broadcast_to(hb[...], (32, 32)), 0.0), axis=1, keepdims=True)
    tri = one_hot(iota((BLK, BLK), 0) >= iota((BLK, BLK), 1)).astype(BF)

    pass_on(wqb.at[:, :, :, near], s_wq, 0)
    pass_on(wqb.at[:, :, :, far], s_wq2, 5)

    @pl.when(core == 1)
    def _():
        plant(wo, wob, s_wo)
        plant(wgp, wgb, s_wg)

    take(xa.at[pl.ds(0, 7)], s_xa.at[1])
    take(wqb.at[:, core, :, near], s_pair.at[0, 1])
    q = dot_nt(xa[:, :, : D // 2].reshape(128, D // 2), wqb[:, :, :, : D // 2].reshape(BLK, D // 2))
    take(wqb.at[:, core, :, far], s_pair.at[5, 1])
    q = q + dot_nt(xa[:, :, D // 2 :].reshape(128, D // 2), wqb[:, :, :, D // 2 :].reshape(BLK, D // 2))
    q = q.astype(BF)
    qs[...] = q.reshape(8, SEQ, BLK)
    qr[:, lanes(place)] = qs[place]
    in_group(lambda p: qs.at[p], qr.at[:, lanes(place)], s_q)

    for k, buf in enumerate((edb, egb, eub)):
        take(buf.at[0], lsem.at[4 + k])
        remote(buf.at[0], buf.at[1], s_ex.at[k], pair).start()

    take(tb.at[pl.ds(0, 7)], s_ts.at[1])
    take(cb.at[pl.ds(0, 7)], s_cb.at[1])
    sent = cb[...].reshape(128, 128)
    spot_row = jnp.sum(jnp.where(eye, jnp.broadcast_to(sent[:, SEQ : SEQ + 1], (128, 128)), 0.0), axis=0, keepdims=True)
    wanted = (r // 16 * 2 + r % 2).astype(F32)
    regroup = jnp.where(c // 16 == r % 16 // 2, one_hot(wanted == jnp.broadcast_to(spot_row, (128, 128))), 0.0)
    regroup_bf = regroup.astype(BF)
    combs = jnp.dot(regroup, sent, precision=HI, preferred_element_type=F32)
    cs[...] = combs.reshape(8, SEQ, 128)
    cd[group] = cs[group]

    def send_comb(k, carry):
        g = (group + k) % 8
        remote(cs.at[g], cd.at[group], s_cd, chip_of(g, place) * 2 + core).start()
        return carry

    lax.fori_loop(1, 8, send_comb, 0)

    relay(wob, s_wo)
    plant(wup, wub, s_wu)
    over_plane(lambda o: wdp.at[:, lanes((o % 8 // 4 + o // 8) % 2 * 4 + o % 4)], lambda o: wdb.at[chip, core], s_wd)
    own_wd = pltpu.make_async_copy(wdp.at[:, lanes(place)], wdb.at[chip, core], lsem.at[7])
    own_wd.start()

    take(qr.at[:, pl.ds(0, 7 * BLK)], s_q.at[1])
    came = tiles_of(qr[...].astype(F32) * HEAD_DIM**-0.5)
    quarter = iota((SEQ, 128), 1) // 32
    for h in range(HEADS):
        t, g, yl = h // 2, h // 4, h // 2 % 2
        row = jnp.zeros((SEQ, 128), F32)
        for k in range(2):
            p = (yl + g) % 2 * 4 + h % 2 * 2 + k
            at = (2 if t >= 8 else 0) + k
            shift = (at - g % 4) * 32 % 128
            v = came[p * 2 + g // 4]
            row = jnp.where(quarter == at, pltpu.roll(v, shift, 1) if shift else v, row)
        qstack[16 * h : 16 * h + 16, :] = row.astype(BF)
    qb[...] = dot(pq[...], qstack[...]).astype(BF).reshape(SEQ, HEADS, 128)
    local[0].wait()
    local[1].wait()

    def score(t):
        for k in range(2):
            sc[t % 2, k] = dot_nt(qb[2 * t + k], kb[2 * t + k]) + bias

    def weigh(t):
        parts = []
        for k in range(2):
            length = clen[2 * t + k]
            for n in range(4):
                v = sc[t % 2, k, :, n * BLK : (n + 1) * BLK]
                live = iota((HEADS, BLK), 1) < length - n * BLK
                rest = jnp.where(live, -(jnp.maximum(v, 0.0) + jnp.log(1.0 + jnp.exp(-jnp.abs(v)))), 0.0)
                parts.extend(split2(rest))
        sums = dot(jnp.concatenate(parts, axis=0), tri)
        for k in range(2):
            length = clen[2 * t + k]
            run = jnp.zeros((HEADS, 1), F32)
            for n in (3, 2, 1, 0):
                at = (k * 4 + n) * 64
                within = sums[at : at + 32] + sums[at + 32 : at + 64]
                live = iota((HEADS, BLK), 1) < length - n * BLK
                v = sc[t % 2, k, :, n * BLK : (n + 1) * BLK]
                wt[t % 2, k, :, n * BLK : (n + 1) * BLK] = jnp.where(live, jnp.exp(v + within + run), 0.0).astype(BF)
                run = run + within[:, 0:1]

    def mix(t):
        for k in range(2):
            ob[2 * t + k] = dot(wt[t % 2, k], vb[2 * t + k]).astype(BF)

    def hand_out(half):
        rows8 = slice(half * 8, half * 8 + 8)
        heads = dot(po[...], ob[rows8].reshape(256, 128))
        left8 = iota((8, 128), 1) < HEAD_DIM
        for t in range(16):
            a = heads[16 * t : 16 * t + 8, :]
            b = heads[16 * t + 8 : 16 * t + 16, :]
            if t < 8:
                joined = jnp.where(left8, a, pltpu.roll(b, HEAD_DIM, 1))
            else:
                joined = jnp.where(left8, pltpu.roll(a, HEAD_DIM, 1), b)
            xc[place, rows8, t * 128 : (t + 1) * 128] = joined.astype(BF)
        part = xc.at[place, pl.ds(half * 8, 8)]
        in_group(lambda p: part, part, s_xc if half == 0 else s_xc2)

    for t in range(10):
        if t < 8:
            score(t)
        if 1 <= t < 9:
            weigh(t - 1)
        if t >= 2:
            mix(t - 2)
        if t == 5:
            hand_out(0)
    hand_out(1)
    relay(wgb, s_wg)
    finish(wob, s_wo, 1)
    relay(wub, s_wu)

    take(wob.at[:, :, core], s_pair.at[1, 1])
    wot[...] = wob[...].reshape(BLK, D).T
    take(xc.at[pl.ds(0, 7), pl.ds(0, 8)], s_xc.at[1])
    take(xc.at[pl.ds(0, 7), pl.ds(0, 8)], s_xc2.at[1])
    proj = dot(xc[...].reshape(128, D), wot[...]).astype(BF)
    stream = tb[...].reshape(128, BLK).astype(F32) + proj.astype(F32)
    y = (stream * g2b[:, lanes(place)]).astype(BF)
    ys[...] = dot(regroup_bf, y).astype(BF).reshape(8, SEQ, BLK)
    xd[group, :, lanes(place)] = ys[group]
    over_plane(lambda o: ys.at[o // 8], lambda o: xd.at[group, :, lanes(place)], s_y)
    ps[...] = proj.reshape(8, SEQ, BLK)
    pr[:, lanes(place)] = ps[place]
    in_group(lambda p: ps.at[p], pr.at[:, lanes(place)], s_pr)

    finish(wgb, s_wg, 2)
    finish(wub, s_wu, 3)
    own_wd.wait()
    take(wdb.at[pl.ds(0, 63), core], s_wd.at[1])
    remote(wdb.at[:, core], wdb.at[:, core], s_pair.at[4], pair).start()
    take(cd.at[pl.ds(0, 7)], s_cd.at[1])
    lane = iota((128, 128), 1)
    comb = cd[...].reshape(128, 128)
    member0 = chip % 8 * 2 + core
    member1 = chip % 8 * 2 + 1 - core
    comb0 = jnp.sum(jnp.where(lane == member0, comb, 0.0), axis=1, keepdims=True)
    comb1 = jnp.sum(jnp.where(lane == member1, comb, 0.0), axis=1, keepdims=True)

    take(wgb.at[:, :, core], s_pair.at[2, 1])
    wgt[...] = wgb[...].reshape(BLK, D).T
    take(wub.at[:, :, core], s_pair.at[3, 1])
    wut[...] = wub[...].reshape(BLK, D).T

    take(zr.at[pl.ds(0, 63)], s_y.at[1])
    rows_in = xd[...].reshape(128, D)
    plain = rows_in.astype(F32) * (1.0 / g2b[...])
    scale = lax.rsqrt(jnp.mean(plain * plain, axis=1, keepdims=True) + EPS)
    gate = dot(rows_in, wgt[...]) * scale
    upper = dot(rows_in, wut[...]) * scale
    hidden = gate * jax.nn.sigmoid(gate) * upper
    part = jnp.sum(hidden * hidden, axis=1, keepdims=True)
    part_row = jnp.sum(jnp.where(eye, jnp.broadcast_to(part, (128, 128)), 0.0), axis=0, keepdims=True)
    sq[...] = jnp.broadcast_to(part_row, (8, 128))
    sqr[place] = sq[...]
    in_group(lambda p: sq, sqr.at[place], s_sq)

    for e, comb_e in ((0, comb0), (1, comb1)):
        if e == 1:
            take(edb.at[1], s_ex.at[0, 1])
            take(egb.at[1], s_ex.at[1, 1])
            take(eub.at[1], s_ex.at[2, 1])
        gate_e = dot(rows_in, egb[e]) * scale
        upper_e = dot(rows_in, eub[e]) * scale
        hbuf[:, e * 512 : (e + 1) * 512] = (gate_e * jax.nn.sigmoid(gate_e) * upper_e * comb_e).astype(BF)

    def route(k, carry):
        zf[:, lanes(k)] = dot(hbuf[...], edb[:, :, lanes(k)].reshape(1024, BLK))
        return carry

    lax.fori_loop(0, 8, route, 0, unroll=2)
    dense = (hidden * hgb[:, lanes(place)]).astype(BF)
    take(wdb.at[:, core], s_pair.at[4, 1])

    def down(k, carry):
        v = dot_nt(dense, wdb[pl.ds(k * 8, 8)].reshape(BLK, BLK))
        zd[:, lanes(k)] = jax.nn.sigmoid(bl[:, lanes(k)]) * v
        return carry

    lax.fori_loop(0, 8, down, 0, unroll=2)
    spots = dot_nt(one_hot(iota((128, SEQ), 0) % 16 == iota((128, SEQ), 1)), order)
    unfold = dot(spots, one_hot(iota((SEQ, 128), 1) // 8 == iota((SEQ, 128), 0)))
    unfold = jnp.where(r // 16 == c % 8, unfold, 0.0).astype(BF)
    take(pr.at[:, pl.ds(0, 7 * BLK)], s_pr.at[1])
    second = from_block_order(tiles_of(pr[...].astype(F32)))
    take(sqr.at[pl.ds(0, 7)], s_sq.at[1])
    total = jnp.sum(sqr[...], axis=0)[0:1, :]
    total_col = jnp.sum(jnp.where(eye, jnp.broadcast_to(total, (128, 128)), 0.0), axis=1, keepdims=True)
    dense_scale = lax.rsqrt(total_col * (1.0 / D) + EPS)

    def produce(k, carry):
        z = zf[:, lanes(k)] + dense_scale * zd[:, lanes(k)]
        zb[k] = z.astype(BF).reshape(8, SEQ, BLK)
        return carry

    lax.fori_loop(0, 8, produce, 0, unroll=2)

    def give(dz, dh):
        g = (depth + dz) % 4 * 2 + (side + dh) % 2
        zs[g] = dot(fold, zb[:, g].reshape(128, BLK)).astype(BF).reshape(8, SEQ, BLK)

        def send(j, carry):
            p = (place + j * 3 + dz) % 8 if dz or dh else (place + j * 3) % 8
            remote(zs.at[g, p], zr.at[chip], s_z, chip_of(g, p) * 2 + core).start()
            return carry

        if dz or dh:
            lax.fori_loop(0, 8, send, 0)
        else:
            zr[chip] = zs[g, place]
            lax.fori_loop(1, 8, send, 0)

    for dz, dh in ((2, 1), (2, 0), (1, 1), (3, 1), (1, 0), (3, 0), (0, 1), (0, 0)):
        give(dz, dh)

    take(zr.at[pl.ds(0, 63)], s_z.at[1])
    sums = jnp.sum(zr[...].reshape(8, 8, SEQ, BLK).astype(F32), axis=1).reshape(128, BLK)
    high, low = split2(sums)
    branch = dot(unfold, high) + dot(unfold, low)
    for k in range(8):
        s = slice(k * BLK, (k + 1) * BLK)
        own = tok[:, s].astype(F32) + jnp.concatenate(second[2 * k : 2 * k + 2], axis=1)
        out[:, s] = (own + branch[k * 16 : k * 16 + 16]).astype(BF)

    take(wqb.at[pl.ds(0, 7), core, :, near], s_wq.at[0])
    take(wqb.at[pl.ds(0, 7), core, :, far], s_wq2.at[0])
    uproot(wob, s_wo)
    uproot(wgb, s_wg)
    uproot(wub, s_wu)
    take(wdb.at[pl.ds(0, 63), core], s_wd.at[0])
    for k, buf in enumerate((wob, wgb, wub)):
        take(buf.at[:, :, core], s_pair.at[k + 1, 0])
    for k, buf in ((0, wqb.at[:, :, :, near]), (4, wdb), (5, wqb.at[:, :, :, far])):
        take(buf.at[:, core], s_pair.at[k, 0])
    take(edb.at[1], s_ex.at[0, 0])
    take(egb.at[1], s_ex.at[1, 0])
    take(eub.at[1], s_ex.at[2, 0])
    take(xa.at[pl.ds(0, 7)], s_xa.at[0])
    take(xc.at[pl.ds(0, 7), pl.ds(0, 8)], s_xc.at[0])
    take(xc.at[pl.ds(0, 7), pl.ds(0, 8)], s_xc2.at[0])
    take(tb.at[pl.ds(0, 7)], s_ts.at[0])
    take(cb.at[pl.ds(0, 7)], s_cb.at[0])
    take(cd.at[pl.ds(0, 7)], s_cd.at[0])
    take(qr.at[:, pl.ds(0, 7 * BLK)], s_q.at[0])
    take(pr.at[:, pl.ds(0, 7 * BLK)], s_pr.at[0])
    take(zr.at[pl.ds(0, 63)], s_y.at[0])
    take(sqr.at[pl.ds(0, 7)], s_sq.at[0])
    take(zr.at[pl.ds(0, 63)], s_z.at[0])


def write_out(a, b, c, a_out, b_out, c_out, sems):
    copies = [pltpu.make_async_copy(src, dst, sems.at[k]) for k, (src, dst) in enumerate(((a, a_out), (b, b_out), (c, c_out)))]
    for x in copies:
        x.start()
    for x in copies:
        x.wait()


def shards(
    tokens, cache_keys, cache_values, cache_len, norm_gain_first, w_query, w_key, w_value, head_bias,
    w_output, norm_gain_second, group_id, member, group_gate, member_weight, expert_gate_w, expert_up_w,
    expert_down_w, dense_gate_w, dense_up_w, hidden_gain, dense_down_w, branch_logit,
):
    vmem = pl.BlockSpec(memory_space=pltpu.VMEM)
    hbm = pl.BlockSpec(memory_space=pl.ANY)
    V = pltpu.VMEM
    strips = (8, 2, SEQ, D)
    pair_sem = pltpu.SemaphoreType.DMA((2,))
    tree_sem = pltpu.SemaphoreType.DMA((6, 2))
    args = (
        (tokens, hbm),
        (cache_keys, hbm),
        (cache_values, hbm),
        (cache_len, hbm),
        (norm_gain_first.reshape(1, D), hbm),
        (w_query.T, hbm),
        (w_key, hbm),
        (w_value, hbm),
        (head_bias.reshape(1, HEADS), hbm),
        (w_output.T, hbm),
        (norm_gain_second.reshape(1, D), hbm),
        (group_id.reshape(1, SEQ), hbm),
        (member.T, hbm),
        (group_gate.reshape(1, SEQ), hbm),
        (member_weight.T, hbm),
        (expert_gate_w, hbm),
        (expert_up_w, hbm),
        (expert_down_w, hbm),
        (dense_gate_w.T, hbm),
        (dense_up_w.T, hbm),
        (hidden_gain.reshape(1, D), hbm),
        (dense_down_w.T, hbm),
        (branch_logit.reshape(1, D), hbm),
    )
    scratch = [
        V((SEQ, CACHE, 128), BF),
        V((SEQ, CACHE, 128), BF),
        V((2, D, 512), BF),
        V((2, D, 512), BF),
        V((2, 512, D), BF),
        V((D, 128), BF),
        V((D, 128), BF),
        V(strips, BF),
        V((4, 2, 2, SEQ, D), BF),
        V((4, 2, 2, SEQ, D), BF),
        V((4, 2, 2, SEQ, D), BF),
        V((64, 2, SEQ, BLK), BF),
        V((8, SEQ, D), BF),
        V((8, SEQ, D), BF),
        V((8, SEQ, D), BF),
        V((8, SEQ, BLK), BF),
        V((SEQ, D), BF),
        V((8, SEQ, BLK), BF),
        V((8, SEQ, BLK), BF),
        V((SEQ, 128), F32),
        V((8, SEQ, 128), F32),
        V((8, SEQ, 128), F32),
        V((8, SEQ, 128), F32),
        V((512, 512), BF),
        V((256, 256), BF),
        V((512, 128), BF),
        V((SEQ, HEADS, 128), BF),
        V((SEQ, HEADS, 128), BF),
        V((8, SEQ, BLK), BF),
        V((SEQ, D), BF),
        V((8, SEQ, BLK), BF),
        V((8, 128), F32),
        V((8, 8, 128), F32),
        V((8, 8, SEQ, BLK), BF),
        V((8, 8, SEQ, BLK), BF),
        V((64, SEQ, BLK), BF),
        V((128, 1024), BF),
        V((128, D), F32),
        V((128, D), F32),
        V((D, BLK), BF),
        V((D, BLK), BF),
        V((D, BLK), BF),
        V((2, 2, HEADS, CACHE), F32),
        V((2, 2, HEADS, CACHE), BF),
        V((1, D), F32),
        V((1, D), F32),
        V((SEQ, D), BF),
        V((SEQ, D), BF),
        V((SEQ, D), BF),
        pltpu.SemaphoreType.DMA((8,)),
        pair_sem,
        tree_sem,
        tree_sem,
        tree_sem,
        pair_sem,
        pltpu.SemaphoreType.DMA((6, 2)),
        pltpu.SemaphoreType.DMA((3, 2)),
    ] + [pair_sem] * 12
    for a, space in (
        (0, V), (3, pltpu.SMEM), (4, V), (5, V), (8, V), (9, V), (10, V), (11, V),
        (12, V), (13, V), (14, V), (18, V), (19, V), (20, V), (21, V), (22, V),
    ):
        scratch.append(space(args[a][0].shape, args[a][0].dtype))
    scratch.append(pltpu.SemaphoreType.DMA((16,)))
    shapes = (
        jax.ShapeDtypeStruct((SEQ, D), BF),
        jax.ShapeDtypeStruct((SEQ, 128), BF),
        jax.ShapeDtypeStruct((SEQ, 128), BF),
    )
    made = pl.pallas_call(
        kernel,
        out_shape=tuple(pltpu.VMEM(x.shape, x.dtype) for x in shapes),
        in_specs=[spec for _, spec in args],
        out_specs=(vmem, vmem, vmem),
        scratch_shapes=scratch,
        compiler_params=pltpu.CompilerParams(
            collective_id=0, has_side_effects=True, vmem_limit_bytes=62_000_000
        ),
    )(*[a for a, _ in args])
    return pl.pallas_call(
        write_out, out_shape=shapes, in_specs=[vmem] * 3, out_specs=(hbm,) * 3,
        scratch_shapes=[pltpu.SemaphoreType.DMA((3,))],
    )(*[pltpu.with_memory_space_constraint(x, pltpu.VMEM) for x in made])


def solution(mesh):
    in_specs = (
        P("ep", None),
        P("ep", None, None),
        P("ep", None, None),
        P("ep"),
        P(),
        P(None, "ep"),
        P(),
        P(),
        P(),
        P(None, "ep"),
        P(),
        P("ep"),
        P("ep", None),
        P("ep"),
        P("ep", None),
        P("ep", None, None),
        P("ep", None, None),
        P("ep", None, None),
        P(None, "ep"),
        P(None, "ep"),
        P(),
        P(None, "ep"),
        P(),
    )
    out_specs = (P("ep", None), P("ep", None), P("ep", None))
    return jax.shard_map(shards, mesh=mesh, in_specs=in_specs, out_specs=out_specs, check_vma=False)
```
